32 devices in a mesh: sp: 16 (over z, y, x), tp: 2 (over core).
Axes of the slice: x: 2, y: 2, z: 4, core: 2. Of those that a mesh axis runs over, the one named last changes fastest.
Arguments:
- queries_narrow: bfloat16 [4096, 1024], P('sp', 'tp'), may hold values from -40 to 40
- keys_narrow: bfloat16 [4096, 256], P('sp', 'tp'), may hold values from -40 to 40
- values_narrow: bfloat16 [4096, 256], P('sp', 'tp'), may hold values from -6 to 6
- queries_wide: bfloat16 [4096, 1024], P('sp', 'tp'), may hold values from -40 to 40
- keys_wide: bfloat16 [4096, 512], P('sp', 'tp'), may hold values from -40 to 40
- values_wide: bfloat16 [4096, 512], P('sp', 'tp'), may hold values from -6 to 6
- lambda_narrow: float32 [8], P('tp'), may hold values from 0.3 to 0.8
- lambda_wide: float32 [4], P('tp'), may hold values from 0.3 to 0.8
- gain_narrow: float32 [128], replicated, may hold values from 0.1 to 1.9
- gain_wide: float32 [256], replicated, may hold values from 0.1 to 1.9
- out_narrow: bfloat16 [1024, 2048], replicated, may hold values from -0.125 to 0.125
- out_wide: bfloat16 [1024, 2048], replicated, may hold values from -0.125 to 0.125
- stream: bfloat16 [4096, 2048], P(('sp', 'tp')), may hold values from -6 to 6
- gain_mix: float32 [2048], replicated, may hold values from 0.1 to 1.9
- gain_ffn: float32 [2048], replicated, may hold values from 0.1 to 1.9
- gain_post: float32 [2048], replicated, may hold values from 0.1 to 1.9
- shared_gate: bfloat16 [2048, 512], replicated, may hold values from -0.125 to 0.125
- shared_up: bfloat16 [2048, 512], replicated, may hold values from -0.125 to 0.125
- shared_down: bfloat16 [512, 2048], replicated, may hold values from -0.25 to 0.25
- expert_gate: bfloat16 [32, 2048, 512], P('sp', None, 'tp'), may hold values from -0.125 to 0.125
- expert_up: bfloat16 [32, 2048, 512], P('sp', None, 'tp'), may hold values from -0.125 to 0.125
- expert_down: bfloat16 [32, 512, 2048], P('sp', 'tp'), may hold values from -0.25 to 0.25
- expert_ids: int32 [4096, 4], P(('sp', 'tp')), may hold values from 0 to 31, all different within a row; in each aligned block of 128 rows (0 to 127, 128 to 255, ...) at most 24 rows name the same one
- route_weights: float32 [4096, 4], P(('sp', 'tp')), may hold values from 0.2 to 1
Outputs:
- layer_out: bfloat16 [4096, 2048], P(('sp', 'tp'))
The draws below stay inside these ranges and needn't reach their ends.
Inputs may be any that keep to these rules, and one draw needn't show every extreme that they name: `expert_ids`: the experts of one token differ. Within the rows that one device holds (aligned blocks of rows in the placement's order), no expert is named more than 24 times, and in every draw some expert is named exactly 24 times there.
All inputs are finite; a program needn't handle non-finite values.
Results may differ from the reference program's by a relative error of at most 0.015.
Values may be sent and summed in bfloat16 or wider, within the bound.
A program may use at most 192 MiB of HBM per device.

```python
import math
import jax
import jax.numpy as jnp
import numpy as np
from jax import lax

D = 2048
HN = 8
DN = 64
VN = 128
KN = 2
HW = 4
DW = 128
VW = 256
KW = 2
FF = 512
SFF = 512
TOPK = 4
TOK_DEV = 256
TOKENS = 4096
EXPERTS = 32
CAP = 24
N_SP = 16
N_TP = 2


def pair_draw(key, heads, groups, key_dim, salt):
    base = jax.random.fold_in(key, salt)
    query_key, keys_key = jax.random.split(base, 2)
    queries = jax.random.normal(query_key, (TOKENS, heads, 2, key_dim), jnp.float32) * 1.4
    keys = jax.random.normal(keys_key, (TOKENS, groups, 2, key_dim), jnp.float32) * 1.3
    queries = jnp.clip(queries, -40.0, 40.0)
    keys = jnp.clip(keys, -40.0, 40.0)
    return (queries.reshape(TOKENS, heads * 2 * key_dim), keys.reshape(TOKENS, groups * 2 * key_dim))


def draw_queries_narrow(key, part):
    return pair_draw(key, HN, KN, DN, 11)[0].astype(jnp.bfloat16)


def draw_keys_narrow(key, part):
    return pair_draw(key, HN, KN, DN, 11)[1].astype(jnp.bfloat16)


def draw_queries_wide(key, part):
    return pair_draw(key, HW, KW, DW, 12)[0].astype(jnp.bfloat16)


def draw_keys_wide(key, part):
    return pair_draw(key, HW, KW, DW, 12)[1].astype(jnp.bfloat16)


def block_levels(rng, dims, pieces, low, high):
    gain, own = 1.0, jax.random.fold_in(rng, 6)
    for axis_at, shards_of in pieces:
        draws = jnp.exp(jax.random.uniform(jax.random.fold_in(own, axis_at), (shards_of,), jnp.float32, low / len(pieces), high / len(pieces)))
        gain = gain * jnp.repeat(draws, dims[axis_at] // shards_of).reshape([-1 if axis == axis_at else 1 for axis in range(len(dims))])
    return gain


def routed_block(rng, own, number, rows, amount, top, bound, slope):
    order = jax.random.permutation(rng, amount)
    crowded, usual = load_shares(amount, rows * top, bound, slope, True), load_shares(amount, rows * top, bound, slope, False)
    places = jnp.arange(amount)

    def named(tallies, rotation):
        used = int((tallies > 0).sum())
        fixed = max(1, used // 4)
        moved = fixed + (places - fixed + rotation * (used - fixed)) % max(1, amount - fixed)
        return jnp.zeros((amount,), jnp.int32).at[order[jnp.where(places < fixed, places, moved)]].set(jnp.asarray(tallies, jnp.int32))

    tallies = jnp.where(number % 4 == 0, named(crowded, number // 4), named(usual, number - number // 4 - 1))
    mixed = jax.random.permutation(jax.random.fold_in(own, 3), amount)
    source_of, sink = mixed[0:amount // 2 * 2:2], mixed[1:amount // 2 * 2:2]
    room = jnp.minimum(tallies[source_of] - 1, bound - tallies[sink]) // 2
    room = jnp.where((source_of == order[0]) | (sink == order[0]) | (tallies[sink] == 0), 0, jnp.maximum(room, 0))
    moved = jax.random.randint(jax.random.fold_in(own, 4), (amount // 2,), 0, 1 << 20) % (room + 1)
    tallies = tallies.at[source_of].add(-moved).at[sink].add(moved)
    items = jnp.searchsorted(jnp.cumsum(tallies), jnp.arange(rows * top), side="right").astype(jnp.int32)
    listing = items.reshape(top, rows).T
    listing = listing[jax.random.permutation(jax.random.fold_in(own, 1), rows)]
    rotation = jax.random.randint(jax.random.fold_in(own, 2), (rows, 1), 0, top)
    return jnp.take_along_axis(listing, (jnp.arange(top)[None, :] + rotation) % top, axis=1)


def load_shares(count, total, reach, lean, full):
    loads = [(1 << 20) // math.isqrt(rank ** lean) + 1 for rank in range(1, count + 1)]
    largest = reach if full else min(reach, max(-(-total // count), total * loads[0] // sum(loads)))
    least = 1 if total - largest >= count - 1 else 0
    given, rest = [largest] + [least] * (count - 1), total - largest - least * (count - 1)
    while rest > 0:
        movable = [i for i in range(1, count) if given[i] < largest] or [i for i in range(1, count) if given[i] < reach]
        whole, budget = sum([loads[i] for i in movable]), rest
        for i in movable:
            extra = min(reach - given[i], max(1, budget * loads[i] // whole), rest)
            given[i] = given[i] + extra
            rest = rest - extra
    return np.array(given)


def normal_values(key, extent, scale, limit, shards=(), kind=jnp.bfloat16):
    values = scale * jax.random.normal(key, extent, jnp.float32)
    if shards:
        values = values * block_levels(key, extent, shards, -0.22, 0.18)
    return jnp.clip(values, -limit, limit).astype(kind)


def setup_inputs(seed: int = 0) -> dict:
    key_list = jax.random.split(jax.random.key(seed), 25)
    queries_narrow = draw_queries_narrow(jax.random.fold_in(key_list[24], 71), 0)
    keys_narrow = draw_keys_narrow(jax.random.fold_in(key_list[24], 71), 0)
    values_narrow = normal_values(key_list[2], (TOKENS, KN * VN), 1.0, 6.0, ((0, 16), (1, 2)))
    queries_wide = draw_queries_wide(jax.random.fold_in(key_list[24], 71), 0)
    keys_wide = draw_keys_wide(jax.random.fold_in(key_list[24], 71), 0)
    values_wide = normal_values(key_list[5], (TOKENS, KW * VW), 1.0, 6.0, ((0, 16), (1, 2)))
    lambda_narrow = jnp.clip(0.3 + 0.5 * jax.random.uniform(key_list[6], (HN,), jnp.float32) ** block_levels(key_list[6], (HN,), ((0, 2),), -0.2, 0.2), 0.3, 0.8)
    lambda_wide = jnp.clip(0.3 + 0.5 * jax.random.uniform(key_list[7], (HW,), jnp.float32) ** block_levels(key_list[7], (HW,), ((0, 2),), -0.2, 0.2), 0.3, 0.8)
    gain_narrow = jnp.clip(1.0 + 0.18 * jax.random.normal(key_list[8], (VN,), jnp.float32), 0.1, 1.9)
    gain_wide = jnp.clip(1.0 + 0.18 * jax.random.normal(key_list[9], (VW,), jnp.float32), 0.1, 1.9)
    out_narrow = normal_values(key_list[10], (HN * VN, D), D ** -0.5, 0.125)
    out_wide = normal_values(key_list[11], (HW * VW, D), D ** -0.5, 0.125)
    stream = normal_values(key_list[12], (TOKENS, D), 1.0, 6.0, ((0, 32),))
    gain_mix = jnp.clip(1.0 + 0.18 * jax.random.normal(key_list[13], (D,), jnp.float32), 0.1, 1.9)
    gain_ffn = jnp.clip(1.0 + 0.18 * jax.random.normal(key_list[14], (D,), jnp.float32), 0.1, 1.9)
    gain_post = jnp.clip(1.0 + 0.18 * jax.random.normal(key_list[15], (D,), jnp.float32), 0.1, 1.9)
    shared_gate = normal_values(key_list[16], (D, SFF), D ** -0.5, 0.125)
    shared_up = normal_values(key_list[17], (D, SFF), D ** -0.5, 0.125)
    shared_down = normal_values(key_list[18], (SFF, D), SFF ** -0.5, 0.25)
    expert_gate = normal_values(key_list[19], (EXPERTS, D, FF), D ** -0.5, 0.125, ((0, 16), (2, 2)))
    expert_up = normal_values(key_list[20], (EXPERTS, D, FF), D ** -0.5, 0.125, ((0, 16), (2, 2)))
    expert_down = normal_values(key_list[21], (EXPERTS, FF, D), FF ** -0.5, 0.25, ((0, 16), (1, 2)))
    expert_ids_keys = jax.random.split(jax.random.fold_in(key_list[22], 1), TOKENS // (TOK_DEV // N_TP))
    expert_ids_turns = jax.random.permutation(jax.random.fold_in(key_list[22], 3), TOKENS // (TOK_DEV // N_TP))
    expert_ids = jax.vmap(lambda own, number: routed_block(jax.random.fold_in(key_list[22], 2), own, number, TOK_DEV // N_TP, EXPERTS, TOPK, CAP, 1))(expert_ids_keys, expert_ids_turns).reshape((TOKENS, TOPK))
    route_weights = jnp.clip(0.2 + 0.8 * jax.random.uniform(key_list[23], (TOKENS, TOPK), jnp.float32) ** block_levels(key_list[23], (TOKENS, TOPK), ((0, 32),), -0.2, 0.2), 0.2, 1.0)
    return {"queries_narrow": queries_narrow, "keys_narrow": keys_narrow, "values_narrow": values_narrow, "queries_wide": queries_wide, "keys_wide": keys_wide, "values_wide": values_wide, "lambda_narrow": lambda_narrow, "lambda_wide": lambda_wide, "gain_narrow": gain_narrow, "gain_wide": gain_wide, "out_narrow": out_narrow, "out_wide": out_wide, "stream": stream, "gain_mix": gain_mix, "gain_ffn": gain_ffn, "gain_post": gain_post, "shared_gate": shared_gate, "shared_up": shared_up, "shared_down": shared_down, "expert_gate": expert_gate, "expert_up": expert_up, "expert_down": expert_down, "expert_ids": expert_ids, "route_weights": route_weights}


EPS = 1e-06

def rms_scale(values, gain_row):
    return values * lax.rsqrt(lax.optimization_barrier(jnp.mean(values * values, axis=-1, keepdims=True)) + EPS) * gain_row

def round_trip(values):
    return lax.optimization_barrier(values.astype(jnp.bfloat16)).astype(jnp.float32)

def group_attention(queries, keys, values, lam_heads, gain_row, heads, groups, key_dim, value_dim):
    per_group = heads // groups
    length = queries.shape[0]
    blocks = length // TOK_DEV
    query_blocks = queries.reshape(blocks, TOK_DEV, groups, per_group, 2, key_dim)
    key_rows = keys.reshape(length, groups, 2, key_dim).astype(jnp.float32)
    value_rows = values.reshape(length, groups, value_dim).astype(jnp.float32)
    key_pos = jnp.arange(length, dtype=jnp.int32)
    lam_grid = lam_heads.reshape(groups, per_group)[:, :, None, None]

    def one_block(inputs):
        query_block, block_index = inputs
        query_pos = block_index * TOK_DEV + jnp.arange(TOK_DEV, dtype=jnp.int32)
        scores = jnp.einsum('qcgmd,kcmd->cgmqk', query_block.astype(jnp.float32), key_rows) * key_dim ** (-0.5)
        causal = key_pos[None, :] <= query_pos[:, None]
        scores = jnp.where(causal, scores, -1e+30)
        row_max = lax.optimization_barrier(jnp.max(scores, axis=-1, keepdims=True))
        weights = jnp.where(causal, jnp.exp(scores - row_max), 0.0)
        row_sum = lax.optimization_barrier(jnp.sum(weights, axis=-1))
        summed_values = jnp.einsum('cgmqk,kcv->cgmqv', round_trip(weights), value_rows)
        mapped = summed_values / row_sum[..., None]
        difference = mapped[:, :, 0] - lam_grid * mapped[:, :, 1]
        normed = rms_scale(difference, gain_row)
        return normed.transpose(2, 0, 1, 3).reshape(TOK_DEV, heads * value_dim).astype(jnp.bfloat16)
    outputs = lax.map(one_block, (query_blocks, jnp.arange(blocks, dtype=jnp.int32)))
    return outputs.reshape(length, heads * value_dim)

def routed_sum(normed, expert_gate, expert_up, expert_down, expert_ids, route_weights):
    assignments = TOKENS * TOPK
    flat_ids = expert_ids.reshape(-1)
    flat_weights = jnp.concatenate([route_weights.reshape(-1), jnp.zeros((1,), jnp.float32)])
    padded = jnp.concatenate([normed, jnp.zeros((1, D), jnp.bfloat16)], axis=0)
    row_bound = N_SP * N_TP * CAP
    half_width = FF // N_TP

    def per_expert(carried, expert):
        matches = jnp.nonzero(flat_ids == expert, size=row_bound, fill_value=assignments)[0].astype(jnp.int32)
        tokens_hit = matches // TOPK
        rows_in = padded[tokens_hit]
        gate_all = lax.dynamic_index_in_dim(expert_gate, expert, 0, keepdims=False)
        up_all = lax.dynamic_index_in_dim(expert_up, expert, 0, keepdims=False)
        down_all = lax.dynamic_index_in_dim(expert_down, expert, 0, keepdims=False)
        summed = jnp.zeros((row_bound, D), jnp.float32)
        for part_index in range(N_TP):
            low = part_index * half_width
            gate_cols = gate_all[:, low:low + half_width]
            up_cols = up_all[:, low:low + half_width]
            down_rows = down_all[low:low + half_width]
            hidden = (jax.nn.silu(jnp.dot(rows_in, gate_cols, preferred_element_type=jnp.float32)) * jnp.dot(rows_in, up_cols, preferred_element_type=jnp.float32)).astype(jnp.bfloat16)
            summed = summed + round_trip(jnp.dot(hidden, down_rows, preferred_element_type=jnp.float32))
        expert_out = round_trip(summed)
        weighted = expert_out * flat_weights[matches][:, None]
        return (carried.at[tokens_hit].add(weighted, mode='drop'), None)
    routed, unused = lax.scan(per_expert, jnp.zeros((TOKENS, D), jnp.float32), jnp.arange(EXPERTS, dtype=jnp.int32))
    return routed

def reference(queries_narrow, keys_narrow, values_narrow, queries_wide, keys_wide, values_wide, lambda_narrow, lambda_wide, gain_narrow, gain_wide, out_narrow, out_wide, stream, gain_mix, gain_ffn, gain_post, shared_gate, shared_up, shared_down, expert_gate, expert_up, expert_down, expert_ids, route_weights):
    narrow = group_attention(queries_narrow, keys_narrow, values_narrow, lambda_narrow, gain_narrow, HN, KN, DN, VN)
    wide = group_attention(queries_wide, keys_wide, values_wide, lambda_wide, gain_wide, HW, KW, DW, VW)
    projected = jnp.dot(narrow, out_narrow, preferred_element_type=jnp.float32) + jnp.dot(wide, out_wide, preferred_element_type=jnp.float32)
    mixed_rows = (stream.astype(jnp.float32) + rms_scale(projected, gain_mix)).astype(jnp.bfloat16)
    normed = rms_scale(mixed_rows.astype(jnp.float32), gain_ffn).astype(jnp.bfloat16)
    shared_hidden = (jax.nn.silu(jnp.dot(normed, shared_gate, preferred_element_type=jnp.float32)) * jnp.dot(normed, shared_up, preferred_element_type=jnp.float32)).astype(jnp.bfloat16)
    shared_out = jnp.dot(shared_hidden, shared_down, preferred_element_type=jnp.float32)
    routed = routed_sum(normed, expert_gate, expert_up, expert_down, expert_ids, route_weights)
    combined = shared_out + routed
    return (mixed_rows.astype(jnp.float32) + rms_scale(combined, gain_post)).astype(jnp.bfloat16)
```

```python
import functools
import math

import jax
import jax.numpy as jnp
from jax import lax
from jax.experimental import pallas as pl
from jax.experimental.pallas import tpu as pltpu
from jax.sharding import PartitionSpec as P

D = 2048
DN = 64
VN = 128
DW = 128
VW = 256
TOPK = 4


EPS = 1e-06


def rms_scale(values, gain_row):
    return values * lax.rsqrt(jnp.mean(values * values, axis=-1, keepdims=True) + EPS) * gain_row


MESH = pl.DeviceIdType.MESH
LOG2E = math.log2(math.e)
MASKED = -1e30


def plane_shape(sp_count):
    bits = sp_count.bit_length() - 1
    if 1 << bits != sp_count:
        return sp_count, 1, 1
    columns = 1 << (bits // 3 if bits % 3 == 0 else (bits - bits // 2) // 2)
    rows = columns
    return sp_count // (rows * columns), rows, columns


def attend_kernel(
    dims,
    qn_ref,
    kn_ref,
    vn_ref,
    qw_ref,
    kw_ref,
    vw_ref,
    lamn_ref,
    lamw_ref,
    gainn_ref,
    gainw_ref,
    out_ref,
    kv,
    att,
    row_max,
    row_sum,
    acc_n,
    acc_w,
    load_sem,
    recv_sem,
    up_sem,
    first_sem,
    second_sem,
    pair_send,
    pair_recv,
    pair_ready,
):
    planes, rows, columns, tp_count = dims
    per_plane = rows * columns
    sp = lax.axis_index("sp")
    tp = lax.axis_index("tp")
    plane = sp // per_plane
    cell = sp % per_plane
    y = cell // columns
    x = cell % columns
    queries = qn_ref.shape[2]
    half_rows = queries // 2

    own = []
    begin = 0
    for index, ref in enumerate((kn_ref, vn_ref, kw_ref, vw_ref)):
        width = ref.shape[1]
        own.append(
            pltpu.make_async_copy(ref, kv.at[0, cell, :, pl.ds(begin, width)], load_sem.at[index])
        )
        begin += width
    for copy in own:
        copy.start()

    def line(axis):
        if axis == 0:
            return [((y + k) % rows) * columns + x for k in range(1, rows)]
        return [y * columns + (x + k) % columns for k in range(1, columns)]

    def crossed(other, axis):
        oy = other // columns
        ox = other % columns
        if axis == 0:
            return [((oy + k) % rows) * columns + ox for k in range(1, rows)]
        return [oy * columns + (ox + k) % columns for k in range(1, columns)]

    barrier = pltpu.get_barrier_semaphore()
    for other in line(0) + line(1):
        pl.semaphore_signal(
            barrier, inc=1, device_id={"sp": plane * per_plane + other}, device_id_type=MESH
        )
    for k in range(1, tp_count):
        pl.semaphore_signal(
            barrier, inc=1, device_id={"tp": (tp + k) % tp_count}, device_id_type=MESH
        )

    @pl.when(plane > 0)
    def _():
        pl.semaphore_signal(barrier, inc=1, device_id={"sp": sp - per_plane}, device_id_type=MESH)

    @pl.when(plane < planes - 1)
    def _():
        pl.semaphore_signal(barrier, inc=1, device_id={"sp": sp + per_plane}, device_id_type=MESH)

    below = (plane > 0).astype(jnp.int32)
    above = (plane < planes - 1).astype(jnp.int32)
    pl.semaphore_wait(barrier, rows - 1 + columns - 1 + tp_count - 1 + below + above)

    for copy in own:
        copy.wait()

    def piece(depth, block, half):
        return kv.at[depth, block, pl.ds(half * half_rows, half_rows), :]

    def remote(depth, to_depth, block, half, target, send):
        return pltpu.make_async_remote_copy(
            src_ref=piece(depth, block, half),
            dst_ref=piece(to_depth, block, half),
            send_sem=send,
            recv_sem=recv_sem.at[to_depth, block, half],
            device_id={"sp": target},
            device_id_type=MESH,
        )

    def arrived(depth, block, half):
        pltpu.make_async_remote_copy(
            src_ref=piece(depth, block, half),
            dst_ref=piece(depth, block, half),
            send_sem=up_sem.at[0, 0],
            recv_sem=recv_sem.at[depth, block, half],
            device_id={"sp": sp},
            device_id_type=MESH,
        ).wait_recv()

    def up_copies(depth):
        return [
            remote(depth, depth + 1, cell, half, sp + per_plane, up_sem.at[depth, half])
            for half in range(2)
        ]

    def direct_copies(depth):
        copies = []
        for half in range(2):
            for k, other in enumerate(line(half)):
                copies.append(
                    remote(
                        depth,
                        depth,
                        cell,
                        half,
                        plane * per_plane + other,
                        first_sem.at[depth, half, k],
                    )
                )
            for k, other in enumerate(line(1 - half)):
                copies.append(
                    remote(
                        depth,
                        depth,
                        cell,
                        half,
                        plane * per_plane + other,
                        second_sem.at[depth, half, 0, k],
                    )
                )
        return copies

    def relay_copies(depth):
        groups = []
        for half in range(2):
            for i, block in enumerate(line(half)):
                copies = [
                    remote(
                        depth,
                        depth,
                        block,
                        half,
                        plane * per_plane + other,
                        second_sem.at[depth, half, i + 1, k],
                    )
                    for k, other in enumerate(line(1 - half))
                ]
                groups.append((block, half, copies))
        return groups

    def issue(depth):
        @pl.when(plane < planes - 1)
        def _():
            for copy in up_copies(depth):
                copy.start()

        for copy in direct_copies(depth):
            copy.start()

    def relay(depth):
        for block, half, copies in relay_copies(depth):
            arrived(depth, block, half)
            for copy in copies:
                copy.start()

    def finish(depth):
        for half in range(2):
            for block in line(1 - half):
                arrived(depth, block, half)
            for first in line(half):
                for block in crossed(first, 1 - half):
                    arrived(depth, block, half)

    row_max[...] = jnp.full_like(row_max, MASKED)
    row_sum[...] = jnp.zeros_like(row_sum)
    acc_n[...] = jnp.zeros_like(acc_n)
    acc_w[...] = jnp.zeros_like(acc_w)
    heads_n = qn_ref.shape[0]
    heads_w = qw_ref.shape[1] // kw_ref.shape[1]
    width_k = kn_ref.shape[1]
    value_n = vn_ref.shape[1]
    begin_kw = width_k + value_n
    map_w = kw_ref.shape[1] // 2
    begin_vw = begin_kw + 2 * map_w
    value_w = vw_ref.shape[1]
    chunk = math.gcd(per_plane, 4)
    key_rows = chunk * queries

    def tile(query, key, value, factor, mask, state, acc, slot):
        scores = lax.dot_general(
            query, key, (((1,), (1,)), ((), ())), preferred_element_type=jnp.float32
        )
        if mask is not None:
            scores = jnp.where(mask, scores, MASKED)
        before = row_max[state][:, :1]
        now = jnp.maximum(before, jnp.max(scores, axis=1, keepdims=True))
        weights = jnp.exp2((scores - now) * factor)
        decay = jnp.exp2((before - now) * factor)
        total = row_sum[state][:, :1] * decay + jnp.sum(weights, axis=1, keepdims=True)
        acc[slot] = acc[slot] * decay + jnp.dot(
            weights.astype(jnp.bfloat16), value, preferred_element_type=jnp.float32
        )
        row_max[state] = jnp.broadcast_to(now, row_max.shape[1:])
        row_sum[state] = jnp.broadcast_to(total, row_sum.shape[1:])

    def attend(depth, masked):
        def part(at):
            def columns_of(begin, width):
                return kv[depth, pl.ds(at, chunk), :, begin : begin + width].reshape(
                    key_rows, width
                )

            mask = None
            if masked:
                query_pos = cell * queries + lax.broadcasted_iota(
                    jnp.int32, (queries, key_rows), 0
                )
                key_pos = at * queries + lax.broadcasted_iota(jnp.int32, (queries, key_rows), 1)
                mask = key_pos <= query_pos

            def narrow(head, carry):
                key = columns_of(0, width_k)
                value = columns_of(width_k, value_n)
                for which in range(2):
                    index = head * 2 + which
                    tile(
                        qn_ref[head, which],
                        key,
                        value,
                        DN**-0.5 * LOG2E,
                        mask,
                        index,
                        acc_n,
                        index,
                    )
                return carry

            def wide(head, carry):
                value = columns_of(begin_vw, value_w)
                for which in range(2):
                    index = head * 2 + which
                    tile(
                        qw_ref[:, pl.ds(pl.multiple_of(index * map_w, map_w), map_w)],
                        columns_of(begin_kw + which * map_w, map_w),
                        value,
                        DW**-0.5 * LOG2E,
                        mask,
                        2 * heads_n + index,
                        acc_w,
                        index,
                    )
                return carry

            lax.fori_loop(0, heads_n, narrow, 0)
            lax.fori_loop(0, heads_w, wide, 0)

        if per_plane == chunk:
            part(0)
        else:

            def step(at, carry):
                part(at * chunk)
                return carry

            lax.fori_loop(0, per_plane // chunk, step, 0)

    def advance(depth):
        @pl.when(depth < plane)
        def _():
            for half in range(2):
                arrived(depth + 1, cell, half)
            issue(depth + 1)

    def relay_next(depth):
        @pl.when(depth < plane)
        def _():
            relay(depth + 1)

    issue(0)
    relay(0)
    advance(0)
    finish(0)
    attend(0, True)
    relay_next(0)

    def depth_step(depth, carry):
        advance(depth)
        finish(depth)
        attend(depth, False)
        relay_next(depth)
        return carry

    lax.fori_loop(1, plane + 1, depth_step, 0)

    def close(first, second, lam, gain):
        head = first - lam * second
        scale = lax.rsqrt(jnp.mean(head * head, axis=1, keepdims=True) + EPS)
        return (head * scale * gain).astype(jnp.bfloat16)

    for head in range(heads_n):
        maps = [acc_n[2 * head + k] / row_sum[2 * head + k][:, :1] for k in range(2)]
        att[:, head * value_n : (head + 1) * value_n] = close(
            maps[0], maps[1], lamn_ref[head], gainn_ref[...]
        )
    begin_w = heads_n * value_n
    for head in range(heads_w):
        maps = [
            acc_w[2 * head + k] / row_sum[2 * (heads_n + head) + k][:, :1] for k in range(2)
        ]
        att[:, begin_w + head * value_w : begin_w + (head + 1) * value_w] = close(
            maps[0], maps[1], lamw_ref[head], gainw_ref[...]
        )

    def drain(depth, carry):
        @pl.when(plane < planes - 1)
        def _():
            for copy in up_copies(depth):
                copy.wait_send()

        for copy in direct_copies(depth):
            copy.wait_send()
        for _block, _half, copies in relay_copies(depth):
            for copy in copies:
                copy.wait_send()
        return carry

    lax.fori_loop(0, plane + 1, drain, 0)
    for k in range(1, tp_count):
        pl.semaphore_signal(
            pair_ready, inc=1, device_id={"tp": (tp + k) % tp_count}, device_id_type=MESH
        )
    pl.semaphore_wait(pair_ready, tp_count - 1)
    share = out_ref.shape[1]
    copies = []
    for k in range(1, tp_count):
        other = (tp + k) % tp_count
        copies.append(
            pltpu.make_async_remote_copy(
                src_ref=att.at[pl.ds(pl.multiple_of(other * share, share), share), :],
                dst_ref=out_ref.at[tp],
                send_sem=pair_send.at[k - 1],
                recv_sem=pair_recv.at[k - 1],
                device_id={"tp": other},
                device_id_type=MESH,
            )
        )
    for copy in copies:
        copy.start()
    out_ref[tp] = att[pl.ds(pl.multiple_of(tp * share, share), share), :]
    for copy in copies:
        copy.wait()


def attended_rows(
    sp_count,
    tp_count,
    queries_narrow,
    keys_narrow,
    values_narrow,
    queries_wide,
    keys_wide,
    values_wide,
    lambda_narrow,
    lambda_wide,
    gain_narrow,
    gain_wide,
):
    planes, rows, columns = plane_shape(sp_count)
    count = queries_narrow.shape[0]
    heads_n = queries_narrow.shape[1] // (2 * DN)
    heads_w = queries_wide.shape[1] // (2 * DW)
    maps = queries_narrow.reshape(count, heads_n, 2, DN).transpose(1, 2, 0, 3)
    padded = jnp.stack(
        [
            jnp.pad(maps[:, 0], ((0, 0), (0, 0), (0, DN))),
            jnp.pad(maps[:, 1], ((0, 0), (0, 0), (DN, 0))),
        ],
        axis=1,
    )
    width = (
        keys_narrow.shape[1] + values_narrow.shape[1] + keys_wide.shape[1] + values_wide.shape[1]
    )
    per_plane = rows * columns
    features = heads_n * VN + heads_w * VW
    longest = max(rows, columns)
    tiles = 2 * (heads_n + heads_w)
    vmem = pl.BlockSpec(memory_space=pltpu.VMEM)
    smem = pl.BlockSpec(memory_space=pltpu.SMEM)
    hbm = pl.BlockSpec(memory_space=pl.ANY)
    return pl.pallas_call(
        functools.partial(attend_kernel, (planes, rows, columns, tp_count)),
        out_shape=jax.ShapeDtypeStruct((tp_count, count // tp_count, features), jnp.bfloat16),
        in_specs=[vmem, hbm, hbm, vmem, hbm, hbm, smem, smem, vmem, vmem],
        out_specs=vmem,
        scratch_shapes=[
            pltpu.VMEM((planes, per_plane, count, width), jnp.bfloat16),
            pltpu.VMEM((count, features), jnp.bfloat16),
            pltpu.VMEM((tiles, count, 128), jnp.float32),
            pltpu.VMEM((tiles, count, 128), jnp.float32),
            pltpu.VMEM((2 * heads_n, count, VN), jnp.float32),
            pltpu.VMEM((2 * heads_w, count, VW), jnp.float32),
            pltpu.SemaphoreType.DMA((4,)),
            pltpu.SemaphoreType.DMA((planes, per_plane, 2)),
            pltpu.SemaphoreType.DMA((planes, 2)),
            pltpu.SemaphoreType.DMA((planes, 2, longest)),
            pltpu.SemaphoreType.DMA((planes, 2, longest, longest)),
            pltpu.SemaphoreType.DMA((max(1, tp_count - 1),)),
            pltpu.SemaphoreType.DMA((max(1, tp_count - 1),)),
            pltpu.SemaphoreType.REGULAR,
        ],
        compiler_params=pltpu.CompilerParams(
            collective_id=0, has_side_effects=True, vmem_limit_bytes=56 * 1024 * 1024
        ),
        name="gather_attend",
    )(
        padded,
        keys_narrow,
        values_narrow,
        queries_wide,
        keys_wide,
        values_wide,
        lambda_narrow,
        lambda_wide,
        gain_narrow.reshape(1, -1),
        gain_wide.reshape(1, -1),
    )


def plane_greeting(planes, rows, columns, tp_count):
    per_plane = rows * columns
    sp = lax.axis_index("sp")
    tp = lax.axis_index("tp")
    plane = sp // per_plane
    cell = sp % per_plane
    barrier = pltpu.get_barrier_semaphore()
    for k in range(1, per_plane):
        pl.semaphore_signal(
            barrier,
            inc=1,
            device_id={"sp": plane * per_plane + (cell + k) % per_plane},
            device_id_type=MESH,
        )
    for k in range(1, planes):
        pl.semaphore_signal(
            barrier,
            inc=1,
            device_id={"sp": (plane + k) % planes * per_plane + cell},
            device_id_type=MESH,
        )
    for k in range(1, tp_count):
        pl.semaphore_signal(
            barrier, inc=1, device_id={"tp": (tp + k) % tp_count}, device_id_type=MESH
        )
    pl.semaphore_wait(barrier, per_plane - 1 + planes - 1 + tp_count - 1)
    return plane, cell, sp, tp


def dispatch_kernel(
    dims,
    group,
    normed_ref,
    slots_ref,
    inbox,
    marks,
    held,
    stage,
    load_sem,
    row_recv,
    mark_recv,
    row_send,
    mark_send,
    cell_recv,
    cell_send,
    pair_recv,
    pair_send,
):
    planes, rows, columns, tp_count = dims
    per_plane = rows * columns
    sp_now = lax.axis_index("sp")
    mine = sp_now // per_plane
    loads = [
        pltpu.make_async_copy(normed_ref, held.at[mine], load_sem.at[0]),
        pltpu.make_async_copy(slots_ref, marks.at[mine], load_sem.at[1]),
    ]
    for copy in loads:
        copy.start()
    plane, cell, sp, tp = plane_greeting(planes, rows, columns, tp_count)
    for copy in loads:
        copy.wait()
    padded = stage.shape[2]
    token_count = held.shape[1]

    def hops(source, way):
        target = {"sp": (sp + per_plane * (1 if way == 0 else planes - 1)) % (planes * per_plane)}
        return [
            pltpu.make_async_remote_copy(
                src_ref=marks.at[source],
                dst_ref=marks.at[source],
                send_sem=mark_send.at[source, way],
                recv_sem=mark_recv.at[source],
                device_id=target,
                device_id_type=MESH,
            ),
            pltpu.make_async_remote_copy(
                src_ref=held.at[source],
                dst_ref=held.at[source],
                send_sem=row_send.at[source, way],
                recv_sem=row_recv.at[source],
                device_id=target,
                device_id_type=MESH,
            ),
        ]

    def to_cell(source, k):
        other = (cell + k) % per_plane
        return pltpu.make_async_remote_copy(
            src_ref=stage.at[source, other],
            dst_ref=inbox.at[tp, source * per_plane + cell],
            send_sem=cell_send.at[source, k],
            recv_sem=cell_recv.at[source, (per_plane - k) % per_plane],
            device_id={"sp": plane * per_plane + other},
            device_id_type=MESH,
        )

    def to_pair(source, k):
        block = inbox.at[tp, pl.ds(source * per_plane, per_plane)]
        return pltpu.make_async_remote_copy(
            src_ref=block,
            dst_ref=block,
            send_sem=pair_send.at[source, k - 1],
            recv_sem=pair_recv.at[source, k - 1],
            device_id={"tp": (tp + k) % tp_count},
            device_id_type=MESH,
        )

    steps = [(0, 0)] + [(d, way) for d in range(1, planes) for way in range(2)]

    def of_step(d, way):
        source = plane - d if way == 0 else plane + d
        exists = source >= 0 if way == 0 else source < planes
        return source, exists

    def onward(source, d, way, act):
        for side in ((0, 1) if d == 0 else (way,)):

            @pl.when(plane < planes - 1 if side == 0 else plane > 0)
            def _(side=side):
                for copy in hops(source, side):
                    act(copy)

    def start(copy):
        copy.start()

    def wait_send(copy):
        copy.wait_send()

    def body(d, way):
        source, exists = of_step(d, way)

        @pl.when(exists)
        def _():
            if d > 0:
                for copy in hops(source, way):
                    copy.wait_recv()
            onward(source, d, way, start)
            tokens = held[source]
            slots = marks[source]
            row = lax.broadcasted_iota(jnp.int32, (padded, token_count), 0)
            for k in list(range(1, per_plane)) + [0]:
                other = (cell + k) % per_plane
                base = (plane * per_plane + other) * group
                wanted = jnp.where(row < group, row + base, -1).astype(jnp.float32)
                hit = slots[0:1, :] == wanted
                for choice in range(1, TOPK):
                    hit = hit | (slots[choice : choice + 1, :] == wanted)
                chosen = jnp.dot(
                    jnp.where(hit, 1.0, 0.0).astype(jnp.bfloat16),
                    tokens,
                    preferred_element_type=jnp.float32,
                ).astype(jnp.bfloat16)
                if k == 0:
                    inbox[tp, source * per_plane + cell] = chosen
                else:
                    stage[source, other] = chosen
            for k in range(1, per_plane):
                to_cell(source, k).start()

    def finish(d, way):
        source, exists = of_step(d, way)

        @pl.when(exists)
        def _():
            for k in range(1, per_plane):
                pltpu.make_async_remote_copy(
                    src_ref=stage.at[source, cell],
                    dst_ref=inbox.at[tp, source * per_plane + (cell + k) % per_plane],
                    send_sem=cell_send.at[source, k],
                    recv_sem=cell_recv.at[source, k],
                    device_id={"sp": sp},
                    device_id_type=MESH,
                ).wait_recv()
            for k in range(1, tp_count):
                to_pair(source, k).start()

    for index, step in enumerate(steps):
        body(*step)
        if index > 0:
            finish(*steps[index - 1])
    finish(*steps[-1])
    for d, way in steps:
        source, exists = of_step(d, way)

        @pl.when(exists)
        def _(source=source, d=d, way=way):
            onward(source, d, way, wait_send)
            for k in range(1, per_plane):
                to_cell(source, k).wait_send()
            for k in range(1, tp_count):
                to_pair(source, k).wait()


def dispatched_rows(dims, group, normed, slot_index, route_weights):
    planes, rows, columns, tp_count = dims
    per_plane = rows * columns
    token_count, width = normed.shape
    padded = -(-group // 16) * 16
    slots = slot_index.reshape(token_count, TOPK).astype(jnp.float32)
    slots = jnp.concatenate([slots, route_weights], axis=1).T
    hbm = pl.BlockSpec(memory_space=pl.ANY)
    dma = pltpu.SemaphoreType.DMA
    return pl.pallas_call(
        functools.partial(dispatch_kernel, dims, group),
        out_shape=[
            jax.ShapeDtypeStruct((tp_count, planes * per_plane, padded, width), jnp.bfloat16),
            jax.ShapeDtypeStruct((planes, 2 * TOPK, token_count), jnp.float32),
        ],
        in_specs=[hbm, hbm],
        out_specs=[pl.BlockSpec(memory_space=pltpu.VMEM)] * 2,
        scratch_shapes=[
            pltpu.VMEM((planes, token_count, width), jnp.bfloat16),
            pltpu.VMEM((planes, per_plane, padded, width), jnp.bfloat16),
            dma((2,)),
            dma((planes,)),
            dma((planes,)),
            dma((planes, 2)),
            dma((planes, 2)),
            dma((planes, per_plane)),
            dma((planes, per_plane)),
            dma((planes, max(1, tp_count - 1))),
            dma((planes, max(1, tp_count - 1))),
        ],
        compiler_params=pltpu.CompilerParams(
            collective_id=1, has_side_effects=True, vmem_limit_bytes=56 * 1024 * 1024
        ),
        name="dispatch",
    )(normed, slots)


def combine_kernel(
    dims,
    group,
    chunks,
    parts_ref,
    marks_ref,
    out_ref,
    mine,
    theirs,
    stage,
    back,
    leaving,
    landed,
    load_sem,
    pair_recv,
    pair_send,
    cell_recv,
    cell_send,
    far_recv,
    far_send,
):
    planes, rows, columns, tp_count = dims
    per_plane = rows * columns
    plane, cell, sp, tp = plane_greeting(planes, rows, columns, tp_count)
    padded = stage.shape[2]
    token_count = out_ref.shape[0]

    order = []
    low, high = jnp.int32(0), jnp.int32(planes - 1)
    for _ in range(planes - 1):
        use_high = high - plane >= plane - low
        order.append(jnp.where(use_high, high, low))
        high = jnp.where(use_high, high - 1, high)
        low = jnp.where(use_high, low, low + 1)
    order.append(plane)

    wide = out_ref.shape[1] // chunks

    def span(chunk):
        return pl.ds(chunk * wide, wide)

    def load(source, chunk):
        return pltpu.make_async_copy(
            parts_ref.at[tp, pl.ds(source * per_plane, per_plane), :, span(chunk)],
            mine.at[source, :, :, span(chunk)],
            load_sem.at[source, chunk],
        )

    def to_pair(source, chunk, k):
        other = (tp + k) % tp_count
        return pltpu.make_async_remote_copy(
            src_ref=parts_ref.at[other, pl.ds(source * per_plane, per_plane), :, span(chunk)],
            dst_ref=theirs.at[k - 1, source, :, :, span(chunk)],
            send_sem=pair_send.at[source, chunk, k - 1],
            recv_sem=pair_recv.at[source, chunk, k - 1],
            device_id={"tp": other},
            device_id_type=MESH,
        )

    def to_cell(source, chunk, k):
        other = (cell + k) % per_plane
        return pltpu.make_async_remote_copy(
            src_ref=stage.at[source, other, :, span(chunk)],
            dst_ref=back.at[source, cell, :, span(chunk)],
            send_sem=cell_send.at[source, chunk, k],
            recv_sem=cell_recv.at[source, chunk, (per_plane - k) % per_plane],
            device_id={"sp": plane * per_plane + other},
            device_id_type=MESH,
        )

    def from_cell(source, chunk, k):
        return pltpu.make_async_remote_copy(
            src_ref=stage.at[source, cell, :, span(chunk)],
            dst_ref=back.at[source, (cell + k) % per_plane, :, span(chunk)],
            send_sem=cell_send.at[source, chunk, k],
            recv_sem=cell_recv.at[source, chunk, k],
            device_id={"sp": sp},
            device_id_type=MESH,
        )

    def onward(source, chunk, way, target):
        return pltpu.make_async_remote_copy(
            src_ref=leaving.at[source, :, span(chunk)],
            dst_ref=landed.at[way, source, :, span(chunk)],
            send_sem=far_send.at[source, chunk],
            recv_sem=far_recv.at[way, source, chunk],
            device_id={"sp": target},
            device_id_type=MESH,
        )

    items = [(source, chunk) for source in order for chunk in range(chunks)]
    for item in items:
        load(*item).start()
        for k in range(1, tp_count):
            to_pair(*item, k).start()

    def body(source, chunk):
        load(source, chunk).wait()
        for k in range(1, tp_count):
            to_pair(source, chunk, k).wait_recv()
        for k in list(range(1, per_plane)) + [0]:
            other = (cell + k) % per_plane
            total = mine[source, other, :, span(chunk)].astype(jnp.float32)
            for i in range(tp_count - 1):
                total += theirs[i, source, other, :, span(chunk)].astype(jnp.float32)
            if k == 0:
                back[source, cell, :, span(chunk)] = total.astype(jnp.bfloat16)
            else:
                stage[source, other, :, span(chunk)] = total.astype(jnp.bfloat16)
                to_cell(source, chunk, k).start()

    def shares(source):
        marks = marks_ref[source]
        row = lax.broadcasted_iota(jnp.int32, (per_plane * padded, token_count), 0)
        block = lax.div(row, padded)
        inner = row - block * padded
        wanted = jnp.where(
            inner < group, inner + (plane * per_plane + block) * group, -1
        ).astype(jnp.float32)
        share = jnp.zeros(wanted.shape, jnp.float32)
        for choice in range(TOPK):
            share += jnp.where(
                marks[choice : choice + 1, :] == wanted,
                marks[TOPK + choice : TOPK + choice + 1, :],
                0.0,
            )
        high = share.astype(jnp.bfloat16)
        low = (share - high.astype(jnp.float32)).astype(jnp.bfloat16)
        return jnp.concatenate([high, low], axis=1)

    def finish(source, chunk, both, last):
        for k in range(1, per_plane):
            from_cell(source, chunk, k).wait_recv()
        begin = chunk * wide
        for at in range(begin, begin + wide, 512):
            values = back[source, :, :, at : at + 512].reshape(per_plane * padded, 512)
            pieces = lax.dot_general(
                both, values, (((0,), (0,)), ((), ())), preferred_element_type=jnp.float32
            )
            out_ref[:, at : at + 512] = pieces[:token_count] + pieces[token_count:]
        if last:
            comes = [(0, plane > 0), (1, plane < planes - 1)]
        else:
            up = source > plane
            comes = [
                (0, up & (plane > 0)),
                (1, jnp.logical_not(up) & (plane < planes - 1)),
            ]
        for way, exists in comes:

            @pl.when(exists)
            def _(way=way):
                onward(source, chunk, way, sp).wait_recv()
                out_ref[:, span(chunk)] += landed[way, source, :, span(chunk)].astype(jnp.float32)

        if not last:
            leaving[source, :, span(chunk)] = out_ref[:, span(chunk)].astype(jnp.bfloat16)

            @pl.when(up)
            def _():
                onward(source, chunk, 0, sp + per_plane).start()

            @pl.when(jnp.logical_not(up))
            def _():
                onward(source, chunk, 1, sp - per_plane).start()

    for item in items:
        body(*item)
    for index, source in enumerate(order):
        both = shares(source)
        for chunk in range(chunks):
            finish(source, chunk, both, index == planes - 1)
    for index, source in enumerate(order):
        for chunk in range(chunks):
            for k in range(1, tp_count):
                to_pair(source, chunk, k).wait_send()
            for k in range(1, per_plane):
                to_cell(source, chunk, k).wait_send()
            if index < planes - 1:
                onward(source, chunk, 0, sp).wait_send()


def combined_rows(dims, group, parts, marks):
    planes, rows, columns, tp_count = dims
    per_plane = rows * columns
    padded, width = parts.shape[2:]
    token_count = marks.shape[2]
    dma = pltpu.SemaphoreType.DMA
    block = (planes, per_plane, padded, width)
    pairs = max(1, tp_count - 1)
    chunks = math.gcd(width // 512, 2)
    return pl.pallas_call(
        functools.partial(combine_kernel, dims, group, chunks),
        out_shape=jax.ShapeDtypeStruct((token_count, width), jnp.float32),
        in_specs=[pl.BlockSpec(memory_space=pl.ANY), pl.BlockSpec(memory_space=pltpu.VMEM)],
        out_specs=pl.BlockSpec(memory_space=pltpu.VMEM),
        scratch_shapes=[
            pltpu.VMEM(block, jnp.bfloat16),
            pltpu.VMEM((pairs,) + block, jnp.bfloat16),
            pltpu.VMEM(block, jnp.bfloat16),
            pltpu.VMEM(block, jnp.bfloat16),
            pltpu.VMEM((planes, token_count, width), jnp.bfloat16),
            pltpu.VMEM((2, planes, token_count, width), jnp.bfloat16),
            dma((planes, chunks)),
            dma((planes, chunks, pairs)),
            dma((planes, chunks, pairs)),
            dma((planes, chunks, per_plane)),
            dma((planes, chunks, per_plane)),
            dma((2, planes, chunks)),
            dma((planes, chunks)),
        ],
        compiler_params=pltpu.CompilerParams(
            collective_id=2, has_side_effects=True, vmem_limit_bytes=56 * 1024 * 1024
        ),
        name="combine",
    )(parts, marks)


def run_experts(incoming, expert_gate, expert_up, expert_down, capacity):
    sources = incoming.shape[0]
    local_experts = expert_gate.shape[0]
    grouped = incoming.reshape(sources, local_experts, capacity, D)
    gate_part = jnp.einsum(
        "rjcd,jdf->rjcf", grouped, expert_gate, preferred_element_type=jnp.float32
    )
    up_part = jnp.einsum("rjcd,jdf->rjcf", grouped, expert_up, preferred_element_type=jnp.float32)
    hidden = (jax.nn.silu(gate_part) * up_part).astype(jnp.bfloat16)
    result = jnp.stack(
        [
            jnp.einsum(
                "rcf,fd->rcd", hidden[:, j], expert_down[j], preferred_element_type=jnp.float32
            ).astype(jnp.bfloat16)
            for j in range(local_experts)
        ],
        axis=1,
    )
    return result.reshape(sources, local_experts * capacity, D)


def shards(
    queries_narrow,
    keys_narrow,
    values_narrow,
    queries_wide,
    keys_wide,
    values_wide,
    lambda_narrow,
    lambda_wide,
    gain_narrow,
    gain_wide,
    out_narrow,
    out_wide,
    stream,
    gain_mix,
    gain_ffn,
    gain_post,
    shared_gate,
    shared_up,
    shared_down,
    expert_gate,
    expert_up,
    expert_down,
    expert_ids,
    route_weights,
):
    sp_count = lax.axis_size("sp")
    attended = attended_rows(
        sp_count,
        lax.axis_size("tp"),
        queries_narrow,
        keys_narrow,
        values_narrow,
        queries_wide,
        keys_wide,
        values_wide,
        lambda_narrow,
        lambda_wide,
        gain_narrow,
        gain_wide,
    )
    narrow_width = out_narrow.shape[0] // attended.shape[0]
    attended = attended.transpose(1, 0, 2)
    narrow_rows = attended[:, :, :narrow_width].reshape(attended.shape[0], -1)
    wide_rows = attended[:, :, narrow_width:].reshape(attended.shape[0], -1)
    projected = jnp.dot(narrow_rows, out_narrow, preferred_element_type=jnp.float32) + jnp.dot(
        wide_rows, out_wide, preferred_element_type=jnp.float32
    )
    mixed_rows = (stream.astype(jnp.float32) + rms_scale(projected, gain_mix)).astype(jnp.bfloat16)
    normed = rms_scale(mixed_rows.astype(jnp.float32), gain_ffn).astype(jnp.bfloat16)
    row_count = normed.shape[0]
    tp_count = lax.axis_size("tp")
    local_experts = expert_gate.shape[0]
    experts_all = local_experts * sp_count
    capacity = max(2, 3 * row_count * TOPK // (2 * experts_all))
    flat_ids = expert_ids.reshape(-1)
    onehot = (flat_ids[:, None] == jnp.arange(experts_all, dtype=jnp.int32)[None, :]).astype(
        jnp.int32
    )
    earlier = jnp.cumsum(onehot, axis=0) - onehot
    slot_rank = jnp.sum(earlier * onehot, axis=1)
    slot_index = flat_ids * capacity + slot_rank
    group = local_experts * capacity
    dims = plane_shape(sp_count) + (tp_count,)
    all_rows, marks = dispatched_rows(dims, group, normed, slot_index, route_weights)
    padded = all_rows.shape[2]
    partials = run_experts(
        all_rows[:, :, :group].reshape(tp_count * sp_count, group, D),
        expert_gate,
        expert_up,
        expert_down,
        capacity,
    )
    partials = partials.astype(jnp.bfloat16).reshape(tp_count, sp_count, group, D)
    if padded > group:
        partials = jnp.pad(partials, ((0, 0), (0, 0), (0, padded - group), (0, 0)))
    routed = combined_rows(dims, group, partials, marks)
    shared_hidden = (
        jax.nn.silu(jnp.dot(normed, shared_gate, preferred_element_type=jnp.float32))
        * jnp.dot(normed, shared_up, preferred_element_type=jnp.float32)
    ).astype(jnp.bfloat16)
    shared_out = jnp.dot(shared_hidden, shared_down, preferred_element_type=jnp.float32)
    combined = shared_out + routed
    return (mixed_rows.astype(jnp.float32) + rms_scale(combined, gain_post)).astype(jnp.bfloat16)


def solution(mesh):
    return jax.shard_map(
        shards,
        mesh=mesh,
        in_specs=(
            P("sp", "tp"),
            P("sp", "tp"),
            P("sp", "tp"),
            P("sp", "tp"),
            P("sp", "tp"),
            P("sp", "tp"),
            P("tp"),
            P("tp"),
            P(),
            P(),
            P(),
            P(),
            P(("sp", "tp"), None),
            P(),
            P(),
            P(),
            P(),
            P(),
            P(),
            P("sp", None, "tp"),
            P("sp", None, "tp"),
            P("sp", "tp", None),
            P(("sp", "tp"), None),
            P(("sp", "tp"), None),
        ),
        out_specs=P(("sp", "tp"), None),
        check_vma=False,
    )
```

```python
import functools
import math

import jax
import jax.numpy as jnp
from jax import lax
from jax.experimental import pallas as pl
from jax.experimental.pallas import tpu as pltpu
from jax.sharding import PartitionSpec as P

D = 2048
DN = 64
VN = 128
DW = 128
VW = 256
TOPK = 4


EPS = 1e-06


def rms_scale(values, gain_row):
    return values * lax.rsqrt(jnp.mean(values * values, axis=-1, keepdims=True) + EPS) * gain_row


MESH = pl.DeviceIdType.MESH
LOG2E = math.log2(math.e)
MASKED = -1e30


def plane_shape(sp_count):
    bits = sp_count.bit_length() - 1
    if 1 << bits != sp_count:
        return sp_count, 1, 1
    columns = 1 << (bits // 3 if bits % 3 == 0 else (bits - bits // 2) // 2)
    rows = columns
    return sp_count // (rows * columns), rows, columns


def attend_kernel(
    dims,
    qn_ref,
    kn_ref,
    vn_ref,
    qw_ref,
    kw_ref,
    vw_ref,
    lam_ref,
    gainn_ref,
    gainw_ref,
    outn_ref,
    outw_ref,
    kv,
    own,
    raw_n,
    raw_w,
    maps_n,
    att_n,
    att_w,
    row_max,
    row_sum,
    acc_n,
    acc_w,
    lam,
    load_sem,
    query_sem,
    query_recv,
    recv_sem,
    swap_sem,
    whole_sem,
    up_sem,
    peer_sem,
    pair_sem,
    relay_sem,
    out_send,
    out_recv,
    lam_sem,
):
    planes, rows, columns, _tp_count = dims
    per_plane = rows * columns
    pairs = columns // 2
    grid = rows * pairs
    sp = lax.axis_index("sp")
    tp = lax.axis_index("tp")
    plane = sp // per_plane
    cell = sp % per_plane
    y = cell // columns
    x = cell % columns
    side = x % 2
    across = cell + 1 - 2 * side
    across_sp = plane * per_plane + across
    query_cell = cell - side + tp
    queries = qn_ref.shape[0]
    half_rows = queries // 2
    at_home = side == tp
    away = side != tp

    def loads(into):
        copies = []
        begin = 0
        for index, ref in enumerate((kn_ref, vn_ref, kw_ref, vw_ref)):
            width = ref.shape[1]
            copies.append(
                pltpu.make_async_copy(ref, into.at[:, pl.ds(begin, width)], load_sem.at[index])
            )
            begin += width
        return copies

    def query_loads():
        return [
            pltpu.make_async_copy(qn_ref, raw_n, query_sem.at[0]),
            pltpu.make_async_copy(qw_ref, raw_w, query_sem.at[1]),
        ]

    def query_swaps():
        return [
            pltpu.make_async_remote_copy(
                src_ref=source,
                dst_ref=target,
                send_sem=query_sem.at[index],
                recv_sem=query_recv.at[index],
                device_id={"sp": across_sp, "tp": 1 - tp},
                device_id_type=MESH,
            )
            for index, (source, target) in enumerate(((qn_ref, raw_n), (qw_ref, raw_w)))
        ]

    @pl.when(at_home)
    def _():
        for copy in loads(kv.at[0, cell]) + query_loads():
            copy.start()

    @pl.when(away)
    def _():
        for copy in loads(own):
            copy.start()

    def peer(k):
        place = (y * pairs + x // 2 + k) % grid
        return place // pairs * columns + place % pairs * 2 + side

    barrier = pltpu.get_barrier_semaphore()

    def greet(device):
        pl.semaphore_signal(barrier, inc=1, device_id=device, device_id_type=MESH)

    for k in range(1, grid):
        greet({"sp": plane * per_plane + peer(k)})
    greet({"tp": 1 - tp})
    for core in range(2):
        greet({"sp": across_sp, "tp": core})

    @pl.when(plane > 0)
    def _():
        greet({"sp": sp - per_plane})

    @pl.when(plane < planes - 1)
    def _():
        greet({"sp": sp + per_plane})

    below = (plane > 0).astype(jnp.int32)
    above = (plane < planes - 1).astype(jnp.int32)
    pl.semaphore_wait(barrier, grid - 1 + 3 + below + above)

    def piece(depth, block, half):
        return kv.at[depth, block, pl.ds(pl.multiple_of(half * half_rows, half_rows), half_rows), :]

    def remote(source, depth, block, half, device, send):
        return pltpu.make_async_remote_copy(
            src_ref=source,
            dst_ref=piece(depth, block, half),
            send_sem=send,
            recv_sem=recv_sem.at[depth, block, half],
            device_id=device,
            device_id_type=MESH,
        )

    def arrived(depth, block, half):
        remote(
            piece(depth, block, half), depth, block, half, {"sp": sp}, up_sem.at[0, 0]
        ).wait_recv()

    def swap_copies():
        return [
            remote(
                own.at[pl.ds(core * half_rows, half_rows), :],
                0,
                cell,
                core,
                {"sp": across_sp, "tp": core},
                swap_sem.at[core],
            )
            for core in range(2)
        ]

    def whole_copies():
        return [
            remote(piece(0, cell, half), 0, cell, half, {"tp": 1 - tp}, whole_sem.at[half])
            for half in range(2)
        ]

    def up_copy(depth, which):
        block = cell if which == 0 else across
        return remote(
            piece(depth, block, tp),
            depth + 1,
            block,
            tp,
            {"sp": sp + per_plane},
            up_sem.at[depth, which],
        )

    def peer_copies(depth, which):
        block = cell if which == 0 else across
        return [
            remote(
                piece(depth, block, tp),
                depth,
                block,
                tp,
                {"sp": plane * per_plane + peer(k)},
                peer_sem.at[depth, which, k],
            )
            for k in range(1, grid)
        ]

    def pair_copy(depth, which):
        block = cell if which == 0 else across
        return remote(
            piece(depth, block, tp), depth, block, tp, {"tp": 1 - tp}, pair_sem.at[depth, which]
        )

    def relay_copy(depth, which, k):
        block = peer(k)
        if which == 1:
            block = block + 1 - 2 * side
        return remote(
            piece(depth, block, tp), depth, block, tp, {"tp": 1 - tp}, relay_sem.at[depth, which, k]
        )

    def spread(depth, which):
        @pl.when(plane < planes - 1)
        def _():
            up_copy(depth, which).start()

        for copy in peer_copies(depth, which):
            copy.start()

    def line(depth):
        for which, block in enumerate((cell, across)):
            arrived(depth, block, tp)
            spread(depth, which)
            pair_copy(depth, which).start()

    def relay(depth):
        for which in range(2):
            for k in range(1, grid):
                block = peer(k) if which == 0 else peer(k) + 1 - 2 * side
                arrived(depth, block, tp)
                relay_copy(depth, which, k).start()

    def finish(depth):
        for k in range(1, grid):
            arrived(depth, peer(k), 1 - tp)
            arrived(depth, peer(k) + 1 - 2 * side, 1 - tp)

    lam_copy = pltpu.make_async_remote_copy(
        src_ref=lam_ref,
        dst_ref=lam,
        send_sem=lam_sem.at[0],
        recv_sem=lam_sem.at[1],
        device_id={"tp": 1 - tp},
        device_id_type=MESH,
    )

    @pl.when(at_home)
    def _():
        for copy in loads(kv.at[0, cell]):
            copy.wait()
        for copy in whole_copies():
            copy.start()
        lam_copy.start()
        lam[...] = lam_ref[...]

    @pl.when(away)
    def _():
        for copy in loads(own):
            copy.wait()
        for copy in swap_copies() + query_swaps():
            copy.start()
        arrived(0, cell, tp)

    spread(0, 0)
    row_max[...] = jnp.full_like(row_max, MASKED)
    row_sum[...] = jnp.zeros_like(row_sum)
    acc_n[...] = jnp.zeros_like(acc_n)
    acc_w[...] = jnp.zeros_like(acc_w)
    heads_n = maps_n.shape[0]
    width_k = kn_ref.shape[1]
    heads_w = qw_ref.shape[1] // kw_ref.shape[1]
    value_n = vn_ref.shape[1]
    begin_kw = width_k + value_n
    map_w = kw_ref.shape[1] // 2
    begin_vw = begin_kw + 2 * map_w
    value_w = vw_ref.shape[1]
    chunk = math.gcd(per_plane, 4)
    key_rows = chunk * queries

    def tile(query, key, value, factor, mask, state, acc, slot):
        scores = lax.dot_general(
            query, key, (((1,), (1,)), ((), ())), preferred_element_type=jnp.float32
        )
        if mask is not None:
            scores = jnp.where(mask, scores, MASKED)
        before = row_max[state][:, :1]
        now = jnp.maximum(before, jnp.max(scores, axis=1, keepdims=True))
        weights = jnp.exp2((scores - now) * factor)
        decay = jnp.exp2((before - now) * factor)
        total = row_sum[state][:, :1] * decay + jnp.sum(weights, axis=1, keepdims=True)
        acc[slot] = acc[slot] * decay + jnp.dot(
            weights.astype(jnp.bfloat16), value, preferred_element_type=jnp.float32
        )
        row_max[state] = jnp.broadcast_to(now, row_max.shape[1:])
        row_sum[state] = jnp.broadcast_to(total, row_sum.shape[1:])

    def attend(depth, masked):
        def part(at):
            def columns_of(begin, width):
                return kv[depth, pl.ds(at, chunk), :, begin : begin + width].reshape(
                    key_rows, width
                )

            mask = None
            if masked:
                query_pos = query_cell * queries + lax.broadcasted_iota(
                    jnp.int32, (queries, key_rows), 0
                )
                key_pos = at * queries + lax.broadcasted_iota(jnp.int32, (queries, key_rows), 1)
                mask = key_pos <= query_pos

            def narrow(head, carry):
                key = columns_of(0, width_k)
                value = columns_of(width_k, value_n)
                for which in range(2):
                    index = head * 2 + which
                    tile(
                        maps_n[head, which],
                        key,
                        value,
                        DN**-0.5 * LOG2E,
                        mask,
                        index,
                        acc_n,
                        index,
                    )
                return carry

            def wide(head, carry):
                value = columns_of(begin_vw, value_w)
                for which in range(2):
                    index = head * 2 + which
                    tile(
                        raw_w[:, pl.ds(pl.multiple_of(index * map_w, map_w), map_w)],
                        columns_of(begin_kw + which * map_w, map_w),
                        value,
                        DW**-0.5 * LOG2E,
                        mask,
                        2 * heads_n + index,
                        acc_w,
                        index,
                    )
                return carry

            lax.fori_loop(0, heads_n, narrow, 0)
            lax.fori_loop(0, heads_w, wide, 0)

        if per_plane == chunk:
            part(0)
        else:

            def step(at, carry):
                part(at * chunk)
                return carry

            lax.fori_loop(0, per_plane // chunk, step, 0)

    arrived(0, across, tp)
    spread(0, 1)
    pair_copy(0, 1).start()
    relay(0)

    @pl.when(plane > 0)
    def _():
        line(1)

    @pl.when(at_home)
    def _():
        for copy in query_loads():
            copy.wait()

    @pl.when(away)
    def _():
        for copy in query_swaps():
            copy.wait()

    for head in range(heads_n):
        both = raw_n[:, head * width_k : (head + 1) * width_k]
        lane = lax.broadcasted_iota(jnp.int32, both.shape, 1)
        zero = jnp.zeros_like(both)
        maps_n[head, 0] = jnp.where(lane < DN, both, zero)
        maps_n[head, 1] = jnp.where(lane < DN, zero, both)

    @pl.when(away)
    def _():
        arrived(0, cell, 1 - tp)
        lam_copy.wait_recv()

    arrived(0, across, 1 - tp)
    finish(0)
    attend(0, True)

    def depth_step(depth, carry):
        relay(depth)

        @pl.when(depth < plane)
        def _():
            line(depth + 1)

        arrived(depth, cell, 1 - tp)
        arrived(depth, across, 1 - tp)
        finish(depth)
        attend(depth, False)
        return carry

    lax.fori_loop(1, plane + 1, depth_step, 0)

    def close(first, second, weight, gain):
        head = first - weight * second
        scale = lax.rsqrt(jnp.mean(head * head, axis=1, keepdims=True) + EPS)
        return (head * scale * gain).astype(jnp.bfloat16)

    for head in range(heads_n):
        maps = [acc_n[2 * head + k] / row_sum[2 * head + k][:, :1] for k in range(2)]
        att_n[:, head * value_n : (head + 1) * value_n] = close(
            maps[0], maps[1], lam[head : head + 1, :1], gainn_ref[...]
        )
    share = outn_ref.shape[0]
    home_sp = plane * per_plane + query_cell

    def out_copies(kind, core):
        att, out = ((att_n, outn_ref), (att_w, outw_ref))[kind]
        width = att.shape[1]
        return pltpu.make_async_remote_copy(
            src_ref=att.at[pl.ds(pl.multiple_of(core * share, share), share), :],
            dst_ref=out.at[:, pl.ds(pl.multiple_of(side * width, width), width)],
            send_sem=out_send.at[kind, core],
            recv_sem=out_recv.at[kind, side],
            device_id={"sp": home_sp, "tp": core},
            device_id_type=MESH,
        )

    def send_out(kind, act):
        @pl.when(at_home)
        def _():
            act(out_copies(kind, 1 - tp))

        @pl.when(away)
        def _():
            for core in range(2):
                act(out_copies(kind, core))

    def keep(kind):
        att, out = ((att_n, outn_ref), (att_w, outw_ref))[kind]
        width = att.shape[1]

        @pl.when(at_home)
        def _():
            out[:, pl.ds(pl.multiple_of(side * width, width), width)] = att[
                pl.ds(pl.multiple_of(tp * share, share), share), :
            ]

    def start(copy):
        copy.start()

    def wait_send(copy):
        copy.wait_send()

    def out_arrived(kind, group):
        att, out = ((att_n, outn_ref), (att_w, outw_ref))[kind]
        width = att.shape[1]
        block = out.at[:, pl.ds(pl.multiple_of(group * width, width), width)]
        pltpu.make_async_remote_copy(
            src_ref=block,
            dst_ref=block,
            send_sem=out_send.at[kind, 0],
            recv_sem=out_recv.at[kind, group],
            device_id={"sp": sp},
            device_id_type=MESH,
        ).wait_recv()

    send_out(0, start)
    for head in range(heads_w):
        maps = [
            acc_w[2 * head + k] / row_sum[2 * (heads_n + head) + k][:, :1] for k in range(2)
        ]
        att_w[:, head * value_w : (head + 1) * value_w] = close(
            maps[0], maps[1], lam[heads_n + head : heads_n + head + 1, :1], gainw_ref[...]
        )
    send_out(1, start)
    keep(0)
    keep(1)

    @pl.when(at_home)
    def _():
        for copy in whole_copies():
            copy.wait_send()
        lam_copy.wait_send()

    @pl.when(away)
    def _():
        for copy in swap_copies():
            copy.wait_send()

    def drain_line(depth, which):
        @pl.when(plane < planes - 1)
        def _():
            up_copy(depth, which).wait_send()

        for copy in peer_copies(depth, which):
            copy.wait_send()
        for k in range(1, grid):
            relay_copy(depth, which, k).wait_send()

    def drain(depth, carry):
        for which in range(2):
            drain_line(depth, which)
            pair_copy(depth, which).wait_send()
        return carry

    drain_line(0, 0)
    drain_line(0, 1)
    pair_copy(0, 1).wait_send()
    lax.fori_loop(1, plane + 1, drain, 0)
    for kind in range(2):
        out_arrived(kind, 1 - side)

        @pl.when(away)
        def _(kind=kind):
            out_arrived(kind, side)

        send_out(kind, wait_send)


def attended_rows(
    sp_count,
    tp_count,
    queries_narrow,
    keys_narrow,
    values_narrow,
    queries_wide,
    keys_wide,
    values_wide,
    lambda_narrow,
    lambda_wide,
    gain_narrow,
    gain_wide,
):
    planes, rows, columns = plane_shape(sp_count)
    count = queries_narrow.shape[0]
    heads_n = queries_narrow.shape[1] // (2 * DN)
    heads_w = queries_wide.shape[1] // (2 * DW)
    width = (
        keys_narrow.shape[1] + values_narrow.shape[1] + keys_wide.shape[1] + values_wide.shape[1]
    )
    per_plane = rows * columns
    grid = per_plane // 2
    tiles = 2 * (heads_n + heads_w)
    share = count // tp_count
    vmem = pl.BlockSpec(memory_space=pltpu.VMEM)
    lambdas = jnp.concatenate([lambda_narrow, lambda_wide])
    lambdas = jnp.pad(lambdas, (0, -lambdas.shape[0] % 8))
    lambdas = jnp.broadcast_to(lambdas[:, None], (lambdas.shape[0], 128))
    hbm = pl.BlockSpec(memory_space=pl.ANY)
    dma = pltpu.SemaphoreType.DMA
    return pl.pallas_call(
        functools.partial(attend_kernel, (planes, rows, columns, tp_count)),
        out_shape=[
            jax.ShapeDtypeStruct((share, tp_count * heads_n * VN), jnp.bfloat16),
            jax.ShapeDtypeStruct((share, tp_count * heads_w * VW), jnp.bfloat16),
        ],
        in_specs=[hbm, hbm, hbm, hbm, hbm, hbm, vmem, vmem, vmem],
        out_specs=[vmem, vmem],
        scratch_shapes=[
            pltpu.VMEM((planes, per_plane, count, width), jnp.bfloat16),
            pltpu.VMEM((count, width), jnp.bfloat16),
            pltpu.VMEM(queries_narrow.shape, jnp.bfloat16),
            pltpu.VMEM(queries_wide.shape, jnp.bfloat16),
            pltpu.VMEM((heads_n, 2, count, 2 * DN), jnp.bfloat16),
            pltpu.VMEM((count, heads_n * VN), jnp.bfloat16),
            pltpu.VMEM((count, heads_w * VW), jnp.bfloat16),
            pltpu.VMEM((tiles, count, 128), jnp.float32),
            pltpu.VMEM((tiles, count, 128), jnp.float32),
            pltpu.VMEM((2 * heads_n, count, VN), jnp.float32),
            pltpu.VMEM((2 * heads_w, count, VW), jnp.float32),
            pltpu.VMEM(lambdas.shape, jnp.float32),
            dma((4,)),
            dma((2,)),
            dma((2,)),
            dma((planes, per_plane, 2)),
            dma((2,)),
            dma((2,)),
            dma((planes, 2)),
            dma((planes, 2, grid)),
            dma((planes, 2)),
            dma((planes, 2, grid)),
            dma((2, 2)),
            dma((2, 2)),
            dma((2,)),
        ],
        compiler_params=pltpu.CompilerParams(
            collective_id=0, has_side_effects=True, vmem_limit_bytes=56 * 1024 * 1024
        ),
        name="gather_attend",
    )(
        queries_narrow,
        keys_narrow,
        values_narrow,
        queries_wide,
        keys_wide,
        values_wide,
        lambdas,
        gain_narrow.reshape(1, -1),
        gain_wide.reshape(1, -1),
    )


def plane_greeting(planes, rows, columns, tp_count):
    per_plane = rows * columns
    sp = lax.axis_index("sp")
    tp = lax.axis_index("tp")
    plane = sp // per_plane
    cell = sp % per_plane
    barrier = pltpu.get_barrier_semaphore()
    for k in range(1, per_plane):
        pl.semaphore_signal(
            barrier,
            inc=1,
            device_id={"sp": plane * per_plane + (cell + k) % per_plane},
            device_id_type=MESH,
        )
    for k in range(1, planes):
        pl.semaphore_signal(
            barrier,
            inc=1,
            device_id={"sp": (plane + k) % planes * per_plane + cell},
            device_id_type=MESH,
        )
    for k in range(1, tp_count):
        pl.semaphore_signal(
            barrier, inc=1, device_id={"tp": (tp + k) % tp_count}, device_id_type=MESH
        )
    pl.semaphore_wait(barrier, per_plane - 1 + planes - 1 + tp_count - 1)
    return plane, cell, sp, tp


def dispatch_kernel(
    dims,
    group,
    normed_ref,
    slots_ref,
    inbox,
    marks,
    held,
    stage,
    load_sem,
    row_recv,
    mark_recv,
    row_send,
    mark_send,
    cell_recv,
    cell_send,
    pair_recv,
    pair_send,
):
    planes, rows, columns, tp_count = dims
    per_plane = rows * columns
    sp_now = lax.axis_index("sp")
    mine = sp_now // per_plane
    loads = [
        pltpu.make_async_copy(normed_ref, held.at[mine], load_sem.at[0]),
        pltpu.make_async_copy(slots_ref, marks.at[mine], load_sem.at[1]),
    ]
    for copy in loads:
        copy.start()
    plane, cell, sp, tp = plane_greeting(planes, rows, columns, tp_count)
    for copy in loads:
        copy.wait()
    padded = stage.shape[2]
    token_count = held.shape[1]

    def hops(source, way):
        target = {"sp": (sp + per_plane * (1 if way == 0 else planes - 1)) % (planes * per_plane)}
        return [
            pltpu.make_async_remote_copy(
                src_ref=marks.at[source],
                dst_ref=marks.at[source],
                send_sem=mark_send.at[source, way],
                recv_sem=mark_recv.at[source],
                device_id=target,
                device_id_type=MESH,
            ),
            pltpu.make_async_remote_copy(
                src_ref=held.at[source],
                dst_ref=held.at[source],
                send_sem=row_send.at[source, way],
                recv_sem=row_recv.at[source],
                device_id=target,
                device_id_type=MESH,
            ),
        ]

    def to_cell(source, k):
        other = (cell + k) % per_plane
        return pltpu.make_async_remote_copy(
            src_ref=stage.at[source, other],
            dst_ref=inbox.at[tp, source * per_plane + cell],
            send_sem=cell_send.at[source, k],
            recv_sem=cell_recv.at[source, (per_plane - k) % per_plane],
            device_id={"sp": plane * per_plane + other},
            device_id_type=MESH,
        )

    def to_pair(source, k):
        block = inbox.at[tp, pl.ds(source * per_plane, per_plane)]
        return pltpu.make_async_remote_copy(
            src_ref=block,
            dst_ref=block,
            send_sem=pair_send.at[source, k - 1],
            recv_sem=pair_recv.at[source, k - 1],
            device_id={"tp": (tp + k) % tp_count},
            device_id_type=MESH,
        )

    steps = [(0, 0)] + [(d, way) for d in range(1, planes) for way in range(2)]

    def of_step(d, way):
        source = plane - d if way == 0 else plane + d
        exists = source >= 0 if way == 0 else source < planes
        return source, exists

    def onward(source, d, way, act):
        for side in ((0, 1) if d == 0 else (way,)):

            @pl.when(plane < planes - 1 if side == 0 else plane > 0)
            def _(side=side):
                for copy in hops(source, side):
                    act(copy)

    def start(copy):
        copy.start()

    def wait_send(copy):
        copy.wait_send()

    def body(d, way):
        source, exists = of_step(d, way)

        @pl.when(exists)
        def _():
            if d > 0:
                for copy in hops(source, way):
                    copy.wait_recv()
            onward(source, d, way, start)
            tokens = held[source]
            slots = marks[source]
            row = lax.broadcasted_iota(jnp.int32, (padded, token_count), 0)
            for k in list(range(1, per_plane)) + [0]:
                other = (cell + k) % per_plane
                base = (plane * per_plane + other) * group
                wanted = jnp.where(row < group, row + base, -1).astype(jnp.float32)
                hit = slots[0:1, :] == wanted
                for choice in range(1, TOPK):
                    hit = hit | (slots[choice : choice + 1, :] == wanted)
                chosen = jnp.dot(
                    jnp.where(hit, 1.0, 0.0).astype(jnp.bfloat16),
                    tokens,
                    preferred_element_type=jnp.float32,
                ).astype(jnp.bfloat16)
                if k == 0:
                    inbox[tp, source * per_plane + cell] = chosen
                else:
                    stage[source, other] = chosen
            for k in range(1, per_plane):
                to_cell(source, k).start()

    def finish(d, way):
        source, exists = of_step(d, way)

        @pl.when(exists)
        def _():
            for k in range(1, per_plane):
                pltpu.make_async_remote_copy(
                    src_ref=stage.at[source, cell],
                    dst_ref=inbox.at[tp, source * per_plane + (cell + k) % per_plane],
                    send_sem=cell_send.at[source, k],
                    recv_sem=cell_recv.at[source, k],
                    device_id={"sp": sp},
                    device_id_type=MESH,
                ).wait_recv()
            for k in range(1, tp_count):
                to_pair(source, k).start()

    for index, step in enumerate(steps):
        body(*step)
        if index > 0:
            finish(*steps[index - 1])
    finish(*steps[-1])
    for d, way in steps:
        source, exists = of_step(d, way)

        @pl.when(exists)
        def _(source=source, d=d, way=way):
            onward(source, d, way, wait_send)
            for k in range(1, per_plane):
                to_cell(source, k).wait_send()
            for k in range(1, tp_count):
                to_pair(source, k).wait()


def dispatched_rows(dims, group, normed, slot_index, route_weights):
    planes, rows, columns, tp_count = dims
    per_plane = rows * columns
    token_count, width = normed.shape
    padded = -(-group // 16) * 16
    slots = slot_index.reshape(token_count, TOPK).astype(jnp.float32)
    slots = jnp.concatenate([slots, route_weights], axis=1).T
    hbm = pl.BlockSpec(memory_space=pl.ANY)
    dma = pltpu.SemaphoreType.DMA
    return pl.pallas_call(
        functools.partial(dispatch_kernel, dims, group),
        out_shape=[
            jax.ShapeDtypeStruct((tp_count, planes * per_plane, padded, width), jnp.bfloat16),
            jax.ShapeDtypeStruct((planes, 2 * TOPK, token_count), jnp.float32),
        ],
        in_specs=[hbm, hbm],
        out_specs=[pl.BlockSpec(memory_space=pltpu.VMEM)] * 2,
        scratch_shapes=[
            pltpu.VMEM((planes, token_count, width), jnp.bfloat16),
            pltpu.VMEM((planes, per_plane, padded, width), jnp.bfloat16),
            dma((2,)),
            dma((planes,)),
            dma((planes,)),
            dma((planes, 2)),
            dma((planes, 2)),
            dma((planes, per_plane)),
            dma((planes, per_plane)),
            dma((planes, max(1, tp_count - 1))),
            dma((planes, max(1, tp_count - 1))),
        ],
        compiler_params=pltpu.CompilerParams(
            collective_id=1, has_side_effects=True, vmem_limit_bytes=56 * 1024 * 1024
        ),
        name="dispatch",
    )(normed, slots)


def combine_kernel(
    dims,
    group,
    chunks,
    parts_ref,
    marks_ref,
    out_ref,
    mine,
    theirs,
    stage,
    back,
    leaving,
    landed,
    load_sem,
    pair_recv,
    pair_send,
    cell_recv,
    cell_send,
    far_recv,
    far_send,
):
    planes, rows, columns, tp_count = dims
    per_plane = rows * columns
    plane, cell, sp, tp = plane_greeting(planes, rows, columns, tp_count)
    padded = stage.shape[2]
    token_count = out_ref.shape[0]

    order = []
    low, high = jnp.int32(0), jnp.int32(planes - 1)
    for _ in range(planes - 1):
        use_high = high - plane >= plane - low
        order.append(jnp.where(use_high, high, low))
        high = jnp.where(use_high, high - 1, high)
        low = jnp.where(use_high, low, low + 1)
    order.append(plane)

    wide = out_ref.shape[1] // chunks

    def span(chunk):
        return pl.ds(chunk * wide, wide)

    def load(source, chunk):
        return pltpu.make_async_copy(
            parts_ref.at[tp, pl.ds(source * per_plane, per_plane), :, span(chunk)],
            mine.at[source, :, :, span(chunk)],
            load_sem.at[source, chunk],
        )

    def to_pair(source, chunk, k):
        other = (tp + k) % tp_count
        return pltpu.make_async_remote_copy(
            src_ref=parts_ref.at[other, pl.ds(source * per_plane, per_plane), :, span(chunk)],
            dst_ref=theirs.at[k - 1, source, :, :, span(chunk)],
            send_sem=pair_send.at[source, chunk, k - 1],
            recv_sem=pair_recv.at[source, chunk, k - 1],
            device_id={"tp": other},
            device_id_type=MESH,
        )

    def to_cell(source, chunk, k):
        other = (cell + k) % per_plane
        return pltpu.make_async_remote_copy(
            src_ref=stage.at[source, other, :, span(chunk)],
            dst_ref=back.at[source, cell, :, span(chunk)],
            send_sem=cell_send.at[source, chunk, k],
            recv_sem=cell_recv.at[source, chunk, (per_plane - k) % per_plane],
            device_id={"sp": plane * per_plane + other},
            device_id_type=MESH,
        )

    def from_cell(source, chunk, k):
        return pltpu.make_async_remote_copy(
            src_ref=stage.at[source, cell, :, span(chunk)],
            dst_ref=back.at[source, (cell + k) % per_plane, :, span(chunk)],
            send_sem=cell_send.at[source, chunk, k],
            recv_sem=cell_recv.at[source, chunk, k],
            device_id={"sp": sp},
            device_id_type=MESH,
        )

    def onward(source, chunk, way, target):
        return pltpu.make_async_remote_copy(
            src_ref=leaving.at[source, :, span(chunk)],
            dst_ref=landed.at[way, source, :, span(chunk)],
            send_sem=far_send.at[source, chunk],
            recv_sem=far_recv.at[way, source, chunk],
            device_id={"sp": target},
            device_id_type=MESH,
        )

    items = [(source, chunk) for source in order for chunk in range(chunks)]
    for item in items:
        load(*item).start()
        for k in range(1, tp_count):
            to_pair(*item, k).start()

    def body(source, chunk):
        load(source, chunk).wait()
        for k in range(1, tp_count):
            to_pair(source, chunk, k).wait_recv()
        for k in list(range(1, per_plane)) + [0]:
            other = (cell + k) % per_plane
            total = mine[source, other, :, span(chunk)].astype(jnp.float32)
            for i in range(tp_count - 1):
                total += theirs[i, source, other, :, span(chunk)].astype(jnp.float32)
            if k == 0:
                back[source, cell, :, span(chunk)] = total.astype(jnp.bfloat16)
            else:
                stage[source, other, :, span(chunk)] = total.astype(jnp.bfloat16)
                to_cell(source, chunk, k).start()

    def shares(source):
        marks = marks_ref[source]
        row = lax.broadcasted_iota(jnp.int32, (per_plane * padded, token_count), 0)
        block = lax.div(row, padded)
        inner = row - block * padded
        wanted = jnp.where(
            inner < group, inner + (plane * per_plane + block) * group, -1
        ).astype(jnp.float32)
        share = jnp.zeros(wanted.shape, jnp.float32)
        for choice in range(TOPK):
            share += jnp.where(
                marks[choice : choice + 1, :] == wanted,
                marks[TOPK + choice : TOPK + choice + 1, :],
                0.0,
            )
        high = share.astype(jnp.bfloat16)
        low = (share - high.astype(jnp.float32)).astype(jnp.bfloat16)
        return jnp.concatenate([high, low], axis=1)

    def finish(source, chunk, both, last):
        for k in range(1, per_plane):
            from_cell(source, chunk, k).wait_recv()
        begin = chunk * wide
        for at in range(begin, begin + wide, 512):
            values = back[source, :, :, at : at + 512].reshape(per_plane * padded, 512)
            pieces = lax.dot_general(
                both, values, (((0,), (0,)), ((), ())), preferred_element_type=jnp.float32
            )
            out_ref[:, at : at + 512] = pieces[:token_count] + pieces[token_count:]
        if last:
            comes = [(0, plane > 0), (1, plane < planes - 1)]
        else:
            up = source > plane
            comes = [
                (0, up & (plane > 0)),
                (1, jnp.logical_not(up) & (plane < planes - 1)),
            ]
        for way, exists in comes:

            @pl.when(exists)
            def _(way=way):
                onward(source, chunk, way, sp).wait_recv()
                out_ref[:, span(chunk)] += landed[way, source, :, span(chunk)].astype(jnp.float32)

        if not last:
            leaving[source, :, span(chunk)] = out_ref[:, span(chunk)].astype(jnp.bfloat16)

            @pl.when(up)
            def _():
                onward(source, chunk, 0, sp + per_plane).start()

            @pl.when(jnp.logical_not(up))
            def _():
                onward(source, chunk, 1, sp - per_plane).start()

    for item in items:
        body(*item)
    for index, source in enumerate(order):
        both = shares(source)
        for chunk in range(chunks):
            finish(source, chunk, both, index == planes - 1)
    for index, source in enumerate(order):
        for chunk in range(chunks):
            for k in range(1, tp_count):
                to_pair(source, chunk, k).wait_send()
            for k in range(1, per_plane):
                to_cell(source, chunk, k).wait_send()
            if index < planes - 1:
                onward(source, chunk, 0, sp).wait_send()


def combined_rows(dims, group, parts, marks):
    planes, rows, columns, tp_count = dims
    per_plane = rows * columns
    padded, width = parts.shape[2:]
    token_count = marks.shape[2]
    dma = pltpu.SemaphoreType.DMA
    block = (planes, per_plane, padded, width)
    pairs = max(1, tp_count - 1)
    chunks = math.gcd(width // 512, 2)
    return pl.pallas_call(
        functools.partial(combine_kernel, dims, group, chunks),
        out_shape=jax.ShapeDtypeStruct((token_count, width), jnp.float32),
        in_specs=[pl.BlockSpec(memory_space=pl.ANY), pl.BlockSpec(memory_space=pltpu.VMEM)],
        out_specs=pl.BlockSpec(memory_space=pltpu.VMEM),
        scratch_shapes=[
            pltpu.VMEM(block, jnp.bfloat16),
            pltpu.VMEM((pairs,) + block, jnp.bfloat16),
            pltpu.VMEM(block, jnp.bfloat16),
            pltpu.VMEM(block, jnp.bfloat16),
            pltpu.VMEM((planes, token_count, width), jnp.bfloat16),
            pltpu.VMEM((2, planes, token_count, width), jnp.bfloat16),
            dma((planes, chunks)),
            dma((planes, chunks, pairs)),
            dma((planes, chunks, pairs)),
            dma((planes, chunks, per_plane)),
            dma((planes, chunks, per_plane)),
            dma((2, planes, chunks)),
            dma((planes, chunks)),
        ],
        compiler_params=pltpu.CompilerParams(
            collective_id=2, has_side_effects=True, vmem_limit_bytes=56 * 1024 * 1024
        ),
        name="combine",
    )(parts, marks)


def run_experts(incoming, expert_gate, expert_up, expert_down, capacity):
    sources = incoming.shape[0]
    local_experts = expert_gate.shape[0]
    grouped = incoming.reshape(sources, local_experts, capacity, D)
    gate_part = jnp.einsum(
        "rjcd,jdf->rjcf", grouped, expert_gate, preferred_element_type=jnp.float32
    )
    up_part = jnp.einsum("rjcd,jdf->rjcf", grouped, expert_up, preferred_element_type=jnp.float32)
    hidden = (jax.nn.silu(gate_part) * up_part).astype(jnp.bfloat16)
    result = jnp.stack(
        [
            jnp.einsum(
                "rcf,fd->rcd", hidden[:, j], expert_down[j], preferred_element_type=jnp.float32
            ).astype(jnp.bfloat16)
            for j in range(local_experts)
        ],
        axis=1,
    )
    return result.reshape(sources, local_experts * capacity, D)


def shards(
    queries_narrow,
    keys_narrow,
    values_narrow,
    queries_wide,
    keys_wide,
    values_wide,
    lambda_narrow,
    lambda_wide,
    gain_narrow,
    gain_wide,
    out_narrow,
    out_wide,
    stream,
    gain_mix,
    gain_ffn,
    gain_post,
    shared_gate,
    shared_up,
    shared_down,
    expert_gate,
    expert_up,
    expert_down,
    expert_ids,
    route_weights,
):
    sp_count = lax.axis_size("sp")
    narrow_rows, wide_rows = attended_rows(
        sp_count,
        lax.axis_size("tp"),
        queries_narrow,
        keys_narrow,
        values_narrow,
        queries_wide,
        keys_wide,
        values_wide,
        lambda_narrow,
        lambda_wide,
        gain_narrow,
        gain_wide,
    )
    projected = jnp.dot(narrow_rows, out_narrow, preferred_element_type=jnp.float32) + jnp.dot(
        wide_rows, out_wide, preferred_element_type=jnp.float32
    )
    mixed_rows = (stream.astype(jnp.float32) + rms_scale(projected, gain_mix)).astype(jnp.bfloat16)
    normed = rms_scale(mixed_rows.astype(jnp.float32), gain_ffn).astype(jnp.bfloat16)
    row_count = normed.shape[0]
    tp_count = lax.axis_size("tp")
    local_experts = expert_gate.shape[0]
    experts_all = local_experts * sp_count
    capacity = max(2, 3 * row_count * TOPK // (2 * experts_all))
    flat_ids = expert_ids.reshape(-1)
    onehot = (flat_ids[:, None] == jnp.arange(experts_all, dtype=jnp.int32)[None, :]).astype(
        jnp.int32
    )
    earlier = jnp.cumsum(onehot, axis=0) - onehot
    slot_rank = jnp.sum(earlier * onehot, axis=1)
    slot_index = flat_ids * capacity + slot_rank
    group = local_experts * capacity
    dims = plane_shape(sp_count) + (tp_count,)
    all_rows, marks = dispatched_rows(dims, group, normed, slot_index, route_weights)
    padded = all_rows.shape[2]
    partials = run_experts(
        all_rows[:, :, :group].reshape(tp_count * sp_count, group, D),
        expert_gate,
        expert_up,
        expert_down,
        capacity,
    )
    partials = partials.astype(jnp.bfloat16).reshape(tp_count, sp_count, group, D)
    if padded > group:
        partials = jnp.pad(partials, ((0, 0), (0, 0), (0, padded - group), (0, 0)))
    routed = combined_rows(dims, group, partials, marks)
    shared_hidden = (
        jax.nn.silu(jnp.dot(normed, shared_gate, preferred_element_type=jnp.float32))
        * jnp.dot(normed, shared_up, preferred_element_type=jnp.float32)
    ).astype(jnp.bfloat16)
    shared_out = jnp.dot(shared_hidden, shared_down, preferred_element_type=jnp.float32)
    combined = shared_out + routed
    return (mixed_rows.astype(jnp.float32) + rms_scale(combined, gain_post)).astype(jnp.bfloat16)


def solution(mesh):
    return jax.shard_map(
        shards,
        mesh=mesh,
        in_specs=(
            P("sp", "tp"),
            P("sp", "tp"),
            P("sp", "tp"),
            P("sp", "tp"),
            P("sp", "tp"),
            P("sp", "tp"),
            P("tp"),
            P("tp"),
            P(),
            P(),
            P(),
            P(),
            P(("sp", "tp"), None),
            P(),
            P(),
            P(),
            P(),
            P(),
            P(),
            P("sp", None, "tp"),
            P("sp", None, "tp"),
            P("sp", "tp", None),
            P(("sp", "tp"), None),
            P(("sp", "tp"), None),
        ),
        out_specs=P(("sp", "tp"), None),
        check_vma=False,
    )
```

```python
import functools
import math

import jax
import jax.numpy as jnp
from jax import lax
from jax.experimental import pallas as pl
from jax.experimental.pallas import tpu as pltpu
from jax.sharding import PartitionSpec as P

D = 2048
DN = 64
VN = 128
DW = 128
VW = 256
TOPK = 4


EPS = 1e-06


def rms_scale(values, gain_row):
    return values * lax.rsqrt(jnp.mean(values * values, axis=-1, keepdims=True) + EPS) * gain_row


MESH = pl.DeviceIdType.MESH
LOG2E = math.log2(math.e)
MASKED = -1e30


def plane_shape(sp_count):
    bits = sp_count.bit_length() - 1
    if 1 << bits != sp_count:
        return sp_count, 1, 1
    columns = 1 << (bits // 3 if bits % 3 == 0 else (bits - bits // 2) // 2)
    rows = columns
    return sp_count // (rows * columns), rows, columns


def attend_kernel(
    dims,
    qn_ref,
    kn_ref,
    vn_ref,
    qw_ref,
    kw_ref,
    vw_ref,
    lam_ref,
    gainn_ref,
    gainw_ref,
    outn_ref,
    outw_ref,
    kv,
    own,
    raw_n,
    raw_w,
    maps_n,
    att_n,
    att_w,
    row_max,
    row_sum,
    acc_n,
    acc_w,
    lam,
    load_sem,
    query_sem,
    query_recv,
    recv_sem,
    swap_sem,
    whole_sem,
    up_sem,
    peer_sem,
    pair_sem,
    relay_sem,
    out_send,
    out_recv,
    lam_sem,
):
    planes, rows, columns, _tp_count = dims
    per_plane = rows * columns
    pairs = columns // 2
    grid = rows * pairs
    sp = lax.axis_index("sp")
    tp = lax.axis_index("tp")
    plane = sp // per_plane
    cell = sp % per_plane
    y = cell // columns
    x = cell % columns
    side = x % 2
    across = cell + 1 - 2 * side
    across_sp = plane * per_plane + across
    query_cell = cell - side + tp
    queries = qn_ref.shape[0]
    half_rows = queries // 2
    at_home = side == tp
    away = side != tp

    def loads(into):
        copies = []
        begin = 0
        for index, ref in enumerate((kn_ref, vn_ref, kw_ref, vw_ref)):
            width = ref.shape[1]
            copies.append(
                pltpu.make_async_copy(ref, into.at[:, pl.ds(begin, width)], load_sem.at[index])
            )
            begin += width
        return copies

    def query_loads():
        return [
            pltpu.make_async_copy(qn_ref, raw_n, query_sem.at[0]),
            pltpu.make_async_copy(qw_ref, raw_w, query_sem.at[1]),
        ]

    def query_swaps():
        return [
            pltpu.make_async_remote_copy(
                src_ref=source,
                dst_ref=target,
                send_sem=query_sem.at[index],
                recv_sem=query_recv.at[index],
                device_id={"sp": across_sp, "tp": 1 - tp},
                device_id_type=MESH,
            )
            for index, (source, target) in enumerate(((qn_ref, raw_n), (qw_ref, raw_w)))
        ]

    @pl.when(at_home)
    def _():
        for copy in loads(kv.at[0, cell]) + query_loads():
            copy.start()

    @pl.when(away)
    def _():
        for copy in loads(own):
            copy.start()

    def peer(k):
        place = (y * pairs + x // 2 + k) % grid
        return place // pairs * columns + place % pairs * 2 + side

    barrier = pltpu.get_barrier_semaphore()

    def greet(device):
        pl.semaphore_signal(barrier, inc=1, device_id=device, device_id_type=MESH)

    for k in range(1, grid):
        greet({"sp": plane * per_plane + peer(k)})
    greet({"tp": 1 - tp})
    for core in range(2):
        greet({"sp": across_sp, "tp": core})

    @pl.when(plane > 0)
    def _():
        greet({"sp": sp - per_plane})

    @pl.when(plane < planes - 1)
    def _():
        greet({"sp": sp + per_plane})

    below = (plane > 0).astype(jnp.int32)
    above = (plane < planes - 1).astype(jnp.int32)
    pl.semaphore_wait(barrier, grid - 1 + 3 + below + above)

    def piece(depth, block, half):
        return kv.at[depth, block, pl.ds(pl.multiple_of(half * half_rows, half_rows), half_rows), :]

    def remote(source, depth, block, half, device, send):
        return pltpu.make_async_remote_copy(
            src_ref=source,
            dst_ref=piece(depth, block, half),
            send_sem=send,
            recv_sem=recv_sem.at[depth, block, half],
            device_id=device,
            device_id_type=MESH,
        )

    def arrived(depth, block, half):
        remote(
            piece(depth, block, half), depth, block, half, {"sp": sp}, up_sem.at[0, 0]
        ).wait_recv()

    def swap_copies():
        return [
            remote(
                own.at[pl.ds(core * half_rows, half_rows), :],
                0,
                cell,
                core,
                {"sp": across_sp, "tp": core},
                swap_sem.at[core],
            )
            for core in range(2)
        ]

    def whole_copies():
        return [
            remote(piece(0, cell, half), 0, cell, half, {"tp": 1 - tp}, whole_sem.at[half])
            for half in range(2)
        ]

    def up_copy(depth, which):
        block = cell if which == 0 else across
        return remote(
            piece(depth, block, tp),
            depth + 1,
            block,
            tp,
            {"sp": sp + per_plane},
            up_sem.at[depth, which],
        )

    def peer_copies(depth, which):
        block = cell if which == 0 else across
        return [
            remote(
                piece(depth, block, tp),
                depth,
                block,
                tp,
                {"sp": plane * per_plane + peer(k)},
                peer_sem.at[depth, which, k],
            )
            for k in range(1, grid)
        ]

    def pair_copy(depth, which):
        block = cell if which == 0 else across
        return remote(
            piece(depth, block, tp), depth, block, tp, {"tp": 1 - tp}, pair_sem.at[depth, which]
        )

    def relay_copy(depth, which, k):
        block = peer(k)
        if which == 1:
            block = block + 1 - 2 * side
        return remote(
            piece(depth, block, tp), depth, block, tp, {"tp": 1 - tp}, relay_sem.at[depth, which, k]
        )

    def spread(depth, which):
        @pl.when(plane < planes - 1)
        def _():
            up_copy(depth, which).start()

        for copy in peer_copies(depth, which):
            copy.start()

    def line(depth):
        for which, block in enumerate((cell, across)):
            arrived(depth, block, tp)
            spread(depth, which)
            pair_copy(depth, which).start()

    def relay(depth):
        for which in range(2):
            for k in range(1, grid):
                block = peer(k) if which == 0 else peer(k) + 1 - 2 * side
                arrived(depth, block, tp)
                relay_copy(depth, which, k).start()

    def finish(depth):
        for k in range(1, grid):
            arrived(depth, peer(k), 1 - tp)
            arrived(depth, peer(k) + 1 - 2 * side, 1 - tp)

    lam_copy = pltpu.make_async_remote_copy(
        src_ref=lam_ref,
        dst_ref=lam,
        send_sem=lam_sem.at[0],
        recv_sem=lam_sem.at[1],
        device_id={"tp": 1 - tp},
        device_id_type=MESH,
    )

    @pl.when(at_home)
    def _():
        for copy in loads(kv.at[0, cell]):
            copy.wait()
        for copy in whole_copies():
            copy.start()
        lam_copy.start()
        lam[...] = lam_ref[...]

    @pl.when(away)
    def _():
        for copy in loads(own):
            copy.wait()
        for copy in swap_copies() + query_swaps():
            copy.start()
        arrived(0, cell, tp)

    spread(0, 0)
    row_max[...] = jnp.full_like(row_max, MASKED)
    row_sum[...] = jnp.zeros_like(row_sum)
    acc_n[...] = jnp.zeros_like(acc_n)
    acc_w[...] = jnp.zeros_like(acc_w)
    heads_n = maps_n.shape[0]
    width_k = kn_ref.shape[1]
    heads_w = qw_ref.shape[1] // kw_ref.shape[1]
    value_n = vn_ref.shape[1]
    begin_kw = width_k + value_n
    map_w = kw_ref.shape[1] // 2
    begin_vw = begin_kw + 2 * map_w
    value_w = vw_ref.shape[1]
    chunk = math.gcd(per_plane, 4)
    key_rows = chunk * queries

    def tile(query, key, value, factor, mask, state, acc, slot):
        scores = lax.dot_general(
            query, key, (((1,), (1,)), ((), ())), preferred_element_type=jnp.float32
        )
        if mask is not None:
            scores = jnp.where(mask, scores, MASKED)
        before = row_max[state][:, :1]
        now = jnp.maximum(before, jnp.max(scores, axis=1, keepdims=True))
        weights = jnp.exp2((scores - now) * factor)
        decay = jnp.exp2((before - now) * factor)
        total = row_sum[state][:, :1] * decay + jnp.sum(weights, axis=1, keepdims=True)
        acc[slot] = acc[slot] * decay + jnp.dot(
            weights.astype(jnp.bfloat16), value, preferred_element_type=jnp.float32
        )
        row_max[state] = jnp.broadcast_to(now, row_max.shape[1:])
        row_sum[state] = jnp.broadcast_to(total, row_sum.shape[1:])

    def attend(depth, masked):
        def part(at):
            def columns_of(begin, width):
                return kv[depth, pl.ds(at, chunk), :, begin : begin + width].reshape(
                    key_rows, width
                )

            mask = None
            if masked:
                query_pos = query_cell * queries + lax.broadcasted_iota(
                    jnp.int32, (queries, key_rows), 0
                )
                key_pos = at * queries + lax.broadcasted_iota(jnp.int32, (queries, key_rows), 1)
                mask = key_pos <= query_pos

            def narrow(head, carry):
                key = columns_of(0, width_k)
                value = columns_of(width_k, value_n)
                for which in range(2):
                    index = head * 2 + which
                    tile(
                        maps_n[head, which],
                        key,
                        value,
                        DN**-0.5 * LOG2E,
                        mask,
                        index,
                        acc_n,
                        index,
                    )
                return carry

            def wide(head, carry):
                value = columns_of(begin_vw, value_w)
                for which in range(2):
                    index = head * 2 + which
                    tile(
                        raw_w[:, pl.ds(pl.multiple_of(index * map_w, map_w), map_w)],
                        columns_of(begin_kw + which * map_w, map_w),
                        value,
                        DW**-0.5 * LOG2E,
                        mask,
                        2 * heads_n + index,
                        acc_w,
                        index,
                    )
                return carry

            lax.fori_loop(0, heads_n, narrow, 0)
            lax.fori_loop(0, heads_w, wide, 0)

        if per_plane == chunk:
            part(0)
        else:

            def step(at, carry):
                part(at * chunk)
                return carry

            lax.fori_loop(0, per_plane // chunk, step, 0)

    arrived(0, across, tp)
    spread(0, 1)
    pair_copy(0, 1).start()
    relay(0)

    @pl.when(plane > 0)
    def _():
        line(1)

    @pl.when(at_home)
    def _():
        for copy in query_loads():
            copy.wait()

    @pl.when(away)
    def _():
        for copy in query_swaps():
            copy.wait()

    for head in range(heads_n):
        both = raw_n[:, head * width_k : (head + 1) * width_k]
        lane = lax.broadcasted_iota(jnp.int32, both.shape, 1)
        zero = jnp.zeros_like(both)
        maps_n[head, 0] = jnp.where(lane < DN, both, zero)
        maps_n[head, 1] = jnp.where(lane < DN, zero, both)

    @pl.when(away)
    def _():
        arrived(0, cell, 1 - tp)
        lam_copy.wait_recv()

    arrived(0, across, 1 - tp)
    finish(0)
    attend(0, True)

    def depth_step(depth, carry):
        relay(depth)

        @pl.when(depth < plane)
        def _():
            line(depth + 1)

        arrived(depth, cell, 1 - tp)
        arrived(depth, across, 1 - tp)
        finish(depth)
        attend(depth, False)
        return carry

    lax.fori_loop(1, plane + 1, depth_step, 0)

    def close(first, second, weight, gain):
        head = first - weight * second
        scale = lax.rsqrt(jnp.mean(head * head, axis=1, keepdims=True) + EPS)
        return (head * scale * gain).astype(jnp.bfloat16)

    for head in range(heads_n):
        maps = [acc_n[2 * head + k] / row_sum[2 * head + k][:, :1] for k in range(2)]
        att_n[:, head * value_n : (head + 1) * value_n] = close(
            maps[0], maps[1], lam[head : head + 1, :1], gainn_ref[...]
        )
    share = outn_ref.shape[0]
    home_sp = plane * per_plane + query_cell

    def out_copies(kind, core):
        att, out = ((att_n, outn_ref), (att_w, outw_ref))[kind]
        width = att.shape[1]
        return pltpu.make_async_remote_copy(
            src_ref=att.at[pl.ds(pl.multiple_of(core * share, share), share), :],
            dst_ref=out.at[:, pl.ds(pl.multiple_of(side * width, width), width)],
            send_sem=out_send.at[kind, core],
            recv_sem=out_recv.at[kind, side],
            device_id={"sp": home_sp, "tp": core},
            device_id_type=MESH,
        )

    def send_out(kind, act):
        @pl.when(at_home)
        def _():
            act(out_copies(kind, 1 - tp))

        @pl.when(away)
        def _():
            for core in range(2):
                act(out_copies(kind, core))

    def keep(kind):
        att, out = ((att_n, outn_ref), (att_w, outw_ref))[kind]
        width = att.shape[1]

        @pl.when(at_home)
        def _():
            out[:, pl.ds(pl.multiple_of(side * width, width), width)] = att[
                pl.ds(pl.multiple_of(tp * share, share), share), :
            ]

    def start(copy):
        copy.start()

    def wait_send(copy):
        copy.wait_send()

    def out_arrived(kind, group):
        att, out = ((att_n, outn_ref), (att_w, outw_ref))[kind]
        width = att.shape[1]
        block = out.at[:, pl.ds(pl.multiple_of(group * width, width), width)]
        pltpu.make_async_remote_copy(
            src_ref=block,
            dst_ref=block,
            send_sem=out_send.at[kind, 0],
            recv_sem=out_recv.at[kind, group],
            device_id={"sp": sp},
            device_id_type=MESH,
        ).wait_recv()

    send_out(0, start)
    for head in range(heads_w):
        maps = [
            acc_w[2 * head + k] / row_sum[2 * (heads_n + head) + k][:, :1] for k in range(2)
        ]
        att_w[:, head * value_w : (head + 1) * value_w] = close(
            maps[0], maps[1], lam[heads_n + head : heads_n + head + 1, :1], gainw_ref[...]
        )
    send_out(1, start)
    keep(0)
    keep(1)

    @pl.when(at_home)
    def _():
        for copy in whole_copies():
            copy.wait_send()
        lam_copy.wait_send()

    @pl.when(away)
    def _():
        for copy in swap_copies():
            copy.wait_send()

    def drain_line(depth, which):
        @pl.when(plane < planes - 1)
        def _():
            up_copy(depth, which).wait_send()

        for copy in peer_copies(depth, which):
            copy.wait_send()
        for k in range(1, grid):
            relay_copy(depth, which, k).wait_send()

    def drain(depth, carry):
        for which in range(2):
            drain_line(depth, which)
            pair_copy(depth, which).wait_send()
        return carry

    drain_line(0, 0)
    drain_line(0, 1)
    pair_copy(0, 1).wait_send()
    lax.fori_loop(1, plane + 1, drain, 0)
    for kind in range(2):
        out_arrived(kind, 1 - side)

        @pl.when(away)
        def _(kind=kind):
            out_arrived(kind, side)

        send_out(kind, wait_send)


def attended_rows(
    sp_count,
    tp_count,
    queries_narrow,
    keys_narrow,
    values_narrow,
    queries_wide,
    keys_wide,
    values_wide,
    lambda_narrow,
    lambda_wide,
    gain_narrow,
    gain_wide,
):
    planes, rows, columns = plane_shape(sp_count)
    count = queries_narrow.shape[0]
    heads_n = queries_narrow.shape[1] // (2 * DN)
    heads_w = queries_wide.shape[1] // (2 * DW)
    width = (
        keys_narrow.shape[1] + values_narrow.shape[1] + keys_wide.shape[1] + values_wide.shape[1]
    )
    per_plane = rows * columns
    grid = per_plane // 2
    tiles = 2 * (heads_n + heads_w)
    share = count // tp_count
    vmem = pl.BlockSpec(memory_space=pltpu.VMEM)
    lambdas = jnp.concatenate([lambda_narrow, lambda_wide])
    lambdas = jnp.pad(lambdas, (0, -lambdas.shape[0] % 8))
    lambdas = jnp.broadcast_to(lambdas[:, None], (lambdas.shape[0], 128))
    hbm = pl.BlockSpec(memory_space=pl.ANY)
    dma = pltpu.SemaphoreType.DMA
    return pl.pallas_call(
        functools.partial(attend_kernel, (planes, rows, columns, tp_count)),
        out_shape=[
            jax.ShapeDtypeStruct((share, tp_count * heads_n * VN), jnp.bfloat16),
            jax.ShapeDtypeStruct((share, tp_count * heads_w * VW), jnp.bfloat16),
        ],
        in_specs=[hbm, hbm, hbm, hbm, hbm, hbm, vmem, vmem, vmem],
        out_specs=[vmem, vmem],
        scratch_shapes=[
            pltpu.VMEM((planes, per_plane, count, width), jnp.bfloat16),
            pltpu.VMEM((count, width), jnp.bfloat16),
            pltpu.VMEM(queries_narrow.shape, jnp.bfloat16),
            pltpu.VMEM(queries_wide.shape, jnp.bfloat16),
            pltpu.VMEM((heads_n, 2, count, 2 * DN), jnp.bfloat16),
            pltpu.VMEM((count, heads_n * VN), jnp.bfloat16),
            pltpu.VMEM((count, heads_w * VW), jnp.bfloat16),
            pltpu.VMEM((tiles, count, 128), jnp.float32),
            pltpu.VMEM((tiles, count, 128), jnp.float32),
            pltpu.VMEM((2 * heads_n, count, VN), jnp.float32),
            pltpu.VMEM((2 * heads_w, count, VW), jnp.float32),
            pltpu.VMEM(lambdas.shape, jnp.float32),
            dma((4,)),
            dma((2,)),
            dma((2,)),
            dma((planes, per_plane, 2)),
            dma((2,)),
            dma((2,)),
            dma((planes, 2)),
            dma((planes, 2, grid)),
            dma((planes, 2)),
            dma((planes, 2, grid)),
            dma((2, 2)),
            dma((2, 2)),
            dma((2,)),
        ],
        compiler_params=pltpu.CompilerParams(
            collective_id=0, has_side_effects=True, vmem_limit_bytes=56 * 1024 * 1024
        ),
        name="gather_attend",
    )(
        queries_narrow,
        keys_narrow,
        values_narrow,
        queries_wide,
        keys_wide,
        values_wide,
        lambdas,
        gain_narrow.reshape(1, -1),
        gain_wide.reshape(1, -1),
    )


def plane_greeting(planes, rows, columns, tp_count):
    per_plane = rows * columns
    sp = lax.axis_index("sp")
    tp = lax.axis_index("tp")
    plane = sp // per_plane
    cell = sp % per_plane
    barrier = pltpu.get_barrier_semaphore()
    for k in range(1, per_plane):
        pl.semaphore_signal(
            barrier,
            inc=1,
            device_id={"sp": plane * per_plane + (cell + k) % per_plane},
            device_id_type=MESH,
        )
    for k in range(1, planes):
        pl.semaphore_signal(
            barrier,
            inc=1,
            device_id={"sp": (plane + k) % planes * per_plane + cell},
            device_id_type=MESH,
        )
    for k in range(1, tp_count):
        pl.semaphore_signal(
            barrier, inc=1, device_id={"tp": (tp + k) % tp_count}, device_id_type=MESH
        )
    pl.semaphore_wait(barrier, per_plane - 1 + planes - 1 + tp_count - 1)
    return plane, cell, sp, tp


def silu(values):
    return values / (1.0 + jnp.exp(-values))


def dispatch_kernel(
    dims,
    group,
    chunks,
    normed_ref,
    slots_ref,
    gate_ref,
    up_ref,
    down_ref,
    shared_gate_ref,
    shared_up_ref,
    shared_down_ref,
    parts,
    marks,
    shared_out,
    held,
    stage,
    inbox,
    result,
    gate,
    up,
    down,
    shared_gate,
    shared_up,
    shared_down,
    load_sem,
    weight_sem,
    row_recv,
    mark_recv,
    row_send,
    mark_send,
    cell_recv,
    cell_send,
    pair_recv,
    pair_send,
    store_sem,
):
    planes, rows, columns, tp_count = dims
    per_plane = rows * columns
    mine = lax.axis_index("sp") // per_plane
    loads = [
        pltpu.make_async_copy(normed_ref, held.at[mine], load_sem.at[0]),
        pltpu.make_async_copy(slots_ref, marks.at[mine], load_sem.at[1]),
    ]
    weights = [
        pltpu.make_async_copy(source, target, weight_sem.at[index])
        for index, (source, target) in enumerate(
            (
                (shared_gate_ref, shared_gate),
                (shared_up_ref, shared_up),
                (shared_down_ref, shared_down),
                (gate_ref, gate),
                (up_ref, up),
                (down_ref, down),
            )
        )
    ]
    for copy in loads + weights:
        copy.start()
    plane, cell, sp, tp = plane_greeting(planes, rows, columns, tp_count)
    for copy in loads:
        copy.wait()
    padded = stage.shape[2]
    token_count = held.shape[1]
    width = held.shape[2]
    wide = width // chunks
    local_experts = gate.shape[0]
    capacity = group // local_experts

    def span(chunk):
        return pl.ds(chunk * wide, wide)

    def mark_hop(source, way, target):
        return pltpu.make_async_remote_copy(
            src_ref=marks.at[source],
            dst_ref=marks.at[source],
            send_sem=mark_send.at[source, way],
            recv_sem=mark_recv.at[source],
            device_id={"sp": target},
            device_id_type=MESH,
        )

    def row_hop(source, chunk, way, target):
        block = held.at[source, :, span(chunk)]
        return pltpu.make_async_remote_copy(
            src_ref=block,
            dst_ref=block,
            send_sem=row_send.at[source, chunk, way],
            recv_sem=row_recv.at[source, chunk],
            device_id={"sp": target},
            device_id_type=MESH,
        )

    def to_cell(source, chunk, k):
        other = (cell + k) % per_plane
        return pltpu.make_async_remote_copy(
            src_ref=stage.at[source, other, :, span(chunk)],
            dst_ref=inbox.at[source, tp, cell, :, span(chunk)],
            send_sem=cell_send.at[source, chunk, k],
            recv_sem=cell_recv.at[source, chunk, (per_plane - k) % per_plane],
            device_id={"sp": plane * per_plane + other},
            device_id_type=MESH,
        )

    def from_cell(source, chunk, k):
        return pltpu.make_async_remote_copy(
            src_ref=stage.at[source, cell, :, span(chunk)],
            dst_ref=inbox.at[source, tp, (cell + k) % per_plane, :, span(chunk)],
            send_sem=cell_send.at[source, chunk, k],
            recv_sem=cell_recv.at[source, chunk, k],
            device_id={"sp": sp},
            device_id_type=MESH,
        )

    def to_pair(source, chunk, k):
        block = inbox.at[source, tp, :, :, span(chunk)]
        return pltpu.make_async_remote_copy(
            src_ref=block,
            dst_ref=block,
            send_sem=pair_send.at[source, chunk, k - 1],
            recv_sem=pair_recv.at[source, chunk, k - 1],
            device_id={"tp": (tp + k) % tp_count},
            device_id_type=MESH,
        )

    def store(source):
        return pltpu.make_async_copy(result.at[source], parts.at[source], store_sem.at[source])

    def onward(source, act):
        @pl.when((source <= plane) & (plane < planes - 1))
        def _():
            act(0, sp + per_plane)

        @pl.when((source >= plane) & (plane > 0))
        def _():
            act(1, sp - per_plane)

    def body(source, first):
        if not first:
            mark_hop(source, 0, sp).wait_recv()
        onward(source, lambda way, target: mark_hop(source, way, target).start())
        slots = marks[source]
        row = lax.broadcasted_iota(jnp.int32, (padded, token_count), 0)
        for chunk in range(chunks):
            if not first:
                row_hop(source, chunk, 0, sp).wait_recv()
            onward(
                source, lambda way, target: row_hop(source, chunk, way, target).start()
            )
            tokens = held[source, :, span(chunk)]
            for k in list(range(1, per_plane)) + [0]:
                other = (cell + k) % per_plane
                base = (plane * per_plane + other) * group
                wanted = jnp.where(row < group, row + base, -1).astype(jnp.float32)
                hit = slots[0:1, :] == wanted
                for choice in range(1, TOPK):
                    hit = hit | (slots[choice : choice + 1, :] == wanted)
                chosen = jnp.dot(
                    jnp.where(hit, 1.0, 0.0).astype(jnp.bfloat16),
                    tokens,
                    preferred_element_type=jnp.float32,
                ).astype(jnp.bfloat16)
                if k == 0:
                    inbox[source, tp, cell, :, span(chunk)] = chosen
                else:
                    stage[source, other, :, span(chunk)] = chosen
                    to_cell(source, chunk, k).start()

    def finish(source):
        for chunk in range(chunks):
            for k in range(1, per_plane):
                from_cell(source, chunk, k).wait_recv()
            for k in range(1, tp_count):
                to_pair(source, chunk, k).start()

    def experts(source):
        for chunk in range(chunks):
            for k in range(1, tp_count):
                to_pair(source, chunk, k).wait_recv()
        done = 0
        for index in range(local_experts):
            begin = index * capacity // 16 * 16
            end = -(-((index + 1) * capacity) // 16) * 16
            block = (tp_count, per_plane, end - begin, width)
            tokens = inbox[source, :, :, begin:end, :].reshape(-1, width)
            gated = jnp.dot(tokens, gate[index], preferred_element_type=jnp.float32)
            hidden = silu(gated) * jnp.dot(
                tokens, up[index], preferred_element_type=jnp.float32
            )
            out = (
                jnp.dot(
                    hidden.astype(jnp.bfloat16), down[index], preferred_element_type=jnp.float32
                )
                .astype(jnp.bfloat16)
                .reshape(block)
            )
            both = max(0, done - begin)
            if both > 0:
                shape = (tp_count, per_plane, both, width)
                row = lax.broadcasted_iota(jnp.int32, shape, 2) + begin
                result[source, :, :, begin:done, :] = jnp.where(
                    row < index * capacity, result[source, :, :, begin:done, :], out[:, :, :both]
                )
            if end > begin + both:
                result[source, :, :, begin + both : end, :] = out[:, :, both:]
            done = max(done, end)
        store(source).start()

    body(plane, True)
    for copy in weights[:3]:
        copy.wait()
    normed = held[plane]
    shared_hidden = silu(
        jnp.dot(normed, shared_gate[...], preferred_element_type=jnp.float32)
    ) * jnp.dot(normed, shared_up[...], preferred_element_type=jnp.float32)
    shared_out[...] = jnp.dot(
        shared_hidden.astype(jnp.bfloat16), shared_down[...], preferred_element_type=jnp.float32
    )
    for copy in weights[3:]:
        copy.wait()

    def step(_, carry):
        low, high, before = carry
        use_high = (low < 0) | ((high < planes) & (high - plane <= plane - low))
        source = jnp.where(use_high, high, low)
        body(source, False)
        finish(before)
        experts(before)
        return jnp.where(use_high, low, low - 1), jnp.where(use_high, high + 1, high), source

    last = lax.fori_loop(0, planes - 1, step, (plane - 1, plane + 1, plane))[2]
    finish(last)
    experts(last)

    def drain(source, carry):
        onward(source, lambda way, target: mark_hop(source, way, target).wait_send())
        for chunk in range(chunks):
            onward(
                source, lambda way, target: row_hop(source, chunk, way, target).wait_send()
            )
            for k in range(1, per_plane):
                to_cell(source, chunk, k).wait_send()
            for k in range(1, tp_count):
                to_pair(source, chunk, k).wait_send()
        store(source).wait()
        return carry

    lax.fori_loop(0, planes, drain, 0)


def dispatched_rows(
    dims, group, normed, slot_index, route_weights, routed_weights, shared_weights
):
    planes, rows, columns, tp_count = dims
    per_plane = rows * columns
    token_count, width = normed.shape
    padded = -(-group // 16) * 16
    slots = slot_index.reshape(token_count, TOPK).astype(jnp.float32)
    slots = jnp.concatenate([slots, route_weights], axis=1).T
    hbm = pl.BlockSpec(memory_space=pl.ANY)
    vmem = pl.BlockSpec(memory_space=pltpu.VMEM)
    dma = pltpu.SemaphoreType.DMA
    chunks = math.gcd(width // 512, 2)
    pairs = max(1, tp_count - 1)
    weights = list(routed_weights) + list(shared_weights)
    inbox = (planes, tp_count, per_plane, padded, width)
    return pl.pallas_call(
        functools.partial(dispatch_kernel, dims, group, chunks),
        out_shape=[
            jax.ShapeDtypeStruct(inbox, jnp.bfloat16),
            jax.ShapeDtypeStruct((planes, 2 * TOPK, token_count), jnp.float32),
            jax.ShapeDtypeStruct((token_count, width), jnp.float32),
        ],
        in_specs=[hbm] * (2 + len(weights)),
        out_specs=[hbm, vmem, vmem],
        scratch_shapes=[
            pltpu.VMEM((planes, token_count, width), jnp.bfloat16),
            pltpu.VMEM((planes, per_plane, padded, width), jnp.bfloat16),
            pltpu.VMEM(inbox, jnp.bfloat16),
            pltpu.VMEM(inbox, jnp.bfloat16),
        ]
        + [pltpu.VMEM(weight.shape, jnp.bfloat16) for weight in weights]
        + [
            dma((2,)),
            dma((len(weights),)),
            dma((planes, chunks)),
            dma((planes,)),
            dma((planes, chunks, 2)),
            dma((planes, 2)),
            dma((planes, chunks, per_plane)),
            dma((planes, chunks, per_plane)),
            dma((planes, chunks, pairs)),
            dma((planes, chunks, pairs)),
            dma((planes,)),
        ],
        compiler_params=pltpu.CompilerParams(
            collective_id=1, has_side_effects=True, vmem_limit_bytes=60 * 1024 * 1024
        ),
        name="dispatch",
    )(normed, slots, *weights)


def combine_kernel(
    dims,
    group,
    chunks,
    parts_ref,
    marks_ref,
    mixed_ref,
    shared_ref,
    gain_ref,
    layer_ref,
    out_ref,
    mine,
    theirs,
    stage,
    back,
    leaving,
    landed,
    load_sem,
    pair_recv,
    pair_send,
    cell_recv,
    cell_send,
    far_recv,
    far_send,
):
    planes, rows, columns, tp_count = dims
    per_plane = rows * columns
    plane, cell, sp, tp = plane_greeting(planes, rows, columns, tp_count)
    padded = stage.shape[2]
    token_count = out_ref.shape[0]

    order = []
    low, high = jnp.int32(0), jnp.int32(planes - 1)
    for _ in range(planes - 1):
        use_high = high - plane >= plane - low
        order.append(jnp.where(use_high, high, low))
        high = jnp.where(use_high, high - 1, high)
        low = jnp.where(use_high, low, low + 1)
    order.append(plane)

    wide = out_ref.shape[1] // chunks

    def span(chunk):
        return pl.ds(chunk * wide, wide)

    def load(source, chunk):
        return pltpu.make_async_copy(
            parts_ref.at[source, tp, :, :, span(chunk)],
            mine.at[source, :, :, span(chunk)],
            load_sem.at[source, chunk],
        )

    def to_pair(source, chunk, k):
        other = (tp + k) % tp_count
        return pltpu.make_async_remote_copy(
            src_ref=parts_ref.at[source, other, :, :, span(chunk)],
            dst_ref=theirs.at[k - 1, source, :, :, span(chunk)],
            send_sem=pair_send.at[source, chunk, k - 1],
            recv_sem=pair_recv.at[source, chunk, k - 1],
            device_id={"tp": other},
            device_id_type=MESH,
        )

    def to_cell(source, chunk, k):
        other = (cell + k) % per_plane
        return pltpu.make_async_remote_copy(
            src_ref=stage.at[source, other, :, span(chunk)],
            dst_ref=back.at[source, cell, :, span(chunk)],
            send_sem=cell_send.at[source, chunk, k],
            recv_sem=cell_recv.at[source, chunk, (per_plane - k) % per_plane],
            device_id={"sp": plane * per_plane + other},
            device_id_type=MESH,
        )

    def from_cell(source, chunk, k):
        return pltpu.make_async_remote_copy(
            src_ref=stage.at[source, cell, :, span(chunk)],
            dst_ref=back.at[source, (cell + k) % per_plane, :, span(chunk)],
            send_sem=cell_send.at[source, chunk, k],
            recv_sem=cell_recv.at[source, chunk, k],
            device_id={"sp": sp},
            device_id_type=MESH,
        )

    def onward(source, chunk, way, target):
        return pltpu.make_async_remote_copy(
            src_ref=leaving.at[source, :, span(chunk)],
            dst_ref=landed.at[way, source, :, span(chunk)],
            send_sem=far_send.at[source, chunk],
            recv_sem=far_recv.at[way, source, chunk],
            device_id={"sp": target},
            device_id_type=MESH,
        )

    items = [(source, chunk) for source in order for chunk in range(chunks)]
    for item in items:
        load(*item).start()
        for k in range(1, tp_count):
            to_pair(*item, k).start()

    def body(source, chunk):
        load(source, chunk).wait()
        for k in range(1, tp_count):
            to_pair(source, chunk, k).wait_recv()
        for k in list(range(1, per_plane)) + [0]:
            other = (cell + k) % per_plane
            total = mine[source, other, :, span(chunk)].astype(jnp.float32)
            for i in range(tp_count - 1):
                total += theirs[i, source, other, :, span(chunk)].astype(jnp.float32)
            if k == 0:
                back[source, cell, :, span(chunk)] = total.astype(jnp.bfloat16)
            else:
                stage[source, other, :, span(chunk)] = total.astype(jnp.bfloat16)
                to_cell(source, chunk, k).start()

    def shares(source):
        marks = marks_ref[source]
        row = lax.broadcasted_iota(jnp.int32, (per_plane * padded, token_count), 0)
        block = lax.div(row, padded)
        inner = row - block * padded
        wanted = jnp.where(
            inner < group, inner + (plane * per_plane + block) * group, -1
        ).astype(jnp.float32)
        share = jnp.zeros(wanted.shape, jnp.float32)
        for choice in range(TOPK):
            share += jnp.where(
                marks[choice : choice + 1, :] == wanted,
                marks[TOPK + choice : TOPK + choice + 1, :],
                0.0,
            )
        high = share.astype(jnp.bfloat16)
        low = (share - high.astype(jnp.float32)).astype(jnp.bfloat16)
        return jnp.concatenate([high, low], axis=1)

    def finish(source, chunk, both, last):
        for k in range(1, per_plane):
            from_cell(source, chunk, k).wait_recv()
        begin = chunk * wide
        for at in range(begin, begin + wide, 512):
            values = back[source, :, :, at : at + 512].reshape(per_plane * padded, 512)
            pieces = lax.dot_general(
                both, values, (((0,), (0,)), ((), ())), preferred_element_type=jnp.float32
            )
            out_ref[:, at : at + 512] = pieces[:token_count] + pieces[token_count:]
        if last:
            comes = [(0, plane > 0), (1, plane < planes - 1)]
        else:
            up = source > plane
            comes = [
                (0, up & (plane > 0)),
                (1, jnp.logical_not(up) & (plane < planes - 1)),
            ]
        for way, exists in comes:

            @pl.when(exists)
            def _(way=way):
                onward(source, chunk, way, sp).wait_recv()
                out_ref[:, span(chunk)] += landed[way, source, :, span(chunk)].astype(jnp.float32)

        if not last:
            leaving[source, :, span(chunk)] = out_ref[:, span(chunk)].astype(jnp.bfloat16)

            @pl.when(up)
            def _():
                onward(source, chunk, 0, sp + per_plane).start()

            @pl.when(jnp.logical_not(up))
            def _():
                onward(source, chunk, 1, sp - per_plane).start()

    for item in items:
        body(*item)
    for index, source in enumerate(order):
        both = shares(source)
        for chunk in range(chunks):
            finish(source, chunk, both, index == planes - 1)
    layer_ref[...] = (
        mixed_ref[...].astype(jnp.float32)
        + rms_scale(shared_ref[...] + out_ref[...], gain_ref[...])
    ).astype(jnp.bfloat16)
    for index, source in enumerate(order):
        for chunk in range(chunks):
            for k in range(1, tp_count):
                to_pair(source, chunk, k).wait_send()
            for k in range(1, per_plane):
                to_cell(source, chunk, k).wait_send()
            if index < planes - 1:
                onward(source, chunk, 0, sp).wait_send()


def combined_rows(dims, group, parts, marks, mixed, shared, gain):
    planes, rows, columns, tp_count = dims
    per_plane = rows * columns
    padded, width = parts.shape[3:]
    token_count = marks.shape[2]
    dma = pltpu.SemaphoreType.DMA
    block = (planes, per_plane, padded, width)
    pairs = max(1, tp_count - 1)
    chunks = math.gcd(width // 512, 2)
    return pl.pallas_call(
        functools.partial(combine_kernel, dims, group, chunks),
        out_shape=jax.ShapeDtypeStruct((token_count, width), jnp.bfloat16),
        in_specs=[pl.BlockSpec(memory_space=pl.ANY)] + [pl.BlockSpec(memory_space=pltpu.VMEM)] * 4,
        out_specs=pl.BlockSpec(memory_space=pltpu.VMEM),
        scratch_shapes=[
            pltpu.VMEM((token_count, width), jnp.float32),
            pltpu.VMEM(block, jnp.bfloat16),
            pltpu.VMEM((pairs,) + block, jnp.bfloat16),
            pltpu.VMEM(block, jnp.bfloat16),
            pltpu.VMEM(block, jnp.bfloat16),
            pltpu.VMEM((planes, token_count, width), jnp.bfloat16),
            pltpu.VMEM((2, planes, token_count, width), jnp.bfloat16),
            dma((planes, chunks)),
            dma((planes, chunks, pairs)),
            dma((planes, chunks, pairs)),
            dma((planes, chunks, per_plane)),
            dma((planes, chunks, per_plane)),
            dma((2, planes, chunks)),
            dma((planes, chunks)),
        ],
        compiler_params=pltpu.CompilerParams(
            collective_id=2, has_side_effects=True, vmem_limit_bytes=56 * 1024 * 1024
        ),
        name="combine",
    )(parts, marks, mixed, shared, gain.reshape(1, -1))


def shards(
    queries_narrow,
    keys_narrow,
    values_narrow,
    queries_wide,
    keys_wide,
    values_wide,
    lambda_narrow,
    lambda_wide,
    gain_narrow,
    gain_wide,
    out_narrow,
    out_wide,
    stream,
    gain_mix,
    gain_ffn,
    gain_post,
    shared_gate,
    shared_up,
    shared_down,
    expert_gate,
    expert_up,
    expert_down,
    expert_ids,
    route_weights,
):
    sp_count = lax.axis_size("sp")
    narrow_rows, wide_rows = attended_rows(
        sp_count,
        lax.axis_size("tp"),
        queries_narrow,
        keys_narrow,
        values_narrow,
        queries_wide,
        keys_wide,
        values_wide,
        lambda_narrow,
        lambda_wide,
        gain_narrow,
        gain_wide,
    )
    projected = jnp.dot(narrow_rows, out_narrow, preferred_element_type=jnp.float32) + jnp.dot(
        wide_rows, out_wide, preferred_element_type=jnp.float32
    )
    mixed_rows = (stream.astype(jnp.float32) + rms_scale(projected, gain_mix)).astype(jnp.bfloat16)
    normed = rms_scale(mixed_rows.astype(jnp.float32), gain_ffn).astype(jnp.bfloat16)
    row_count = normed.shape[0]
    tp_count = lax.axis_size("tp")
    local_experts = expert_gate.shape[0]
    experts_all = local_experts * sp_count
    capacity = max(2, 3 * row_count * TOPK // (2 * experts_all))
    chosen = (
        expert_ids[:, :, None] == jnp.arange(experts_all, dtype=jnp.int32)[None, None, :]
    ).astype(jnp.float32)
    named = jnp.sum(chosen, axis=1)
    order = jnp.arange(row_count, dtype=jnp.int32)
    earlier = jnp.dot(
        (order[None, :] < order[:, None]).astype(jnp.bfloat16),
        named.astype(jnp.bfloat16),
        preferred_element_type=jnp.float32,
    )
    slot_rank = jnp.sum(chosen * earlier[:, None, :], axis=2).astype(jnp.int32)
    slot_index = expert_ids * capacity + slot_rank
    group = local_experts * capacity
    dims = plane_shape(sp_count) + (tp_count,)
    parts, marks, shared_out = dispatched_rows(
        dims,
        group,
        normed,
        slot_index,
        route_weights,
        (expert_gate, expert_up, expert_down),
        (shared_gate, shared_up, shared_down),
    )
    return combined_rows(dims, group, parts, marks, mixed_rows, shared_out, gain_post)


def solution(mesh):
    return jax.shard_map(
        shards,
        mesh=mesh,
        in_specs=(
            P("sp", "tp"),
            P("sp", "tp"),
            P("sp", "tp"),
            P("sp", "tp"),
            P("sp", "tp"),
            P("sp", "tp"),
            P("tp"),
            P("tp"),
            P(),
            P(),
            P(),
            P(),
            P(("sp", "tp"), None),
            P(),
            P(),
            P(),
            P(),
            P(),
            P(),
            P("sp", None, "tp"),
            P("sp", None, "tp"),
            P("sp", "tp", None),
            P(("sp", "tp"), None),
            P(("sp", "tp"), None),
        ),
        out_specs=P(("sp", "tp"), None),
        check_vma=False,
    )
```

```python
import functools
import math

import jax
import jax.numpy as jnp
from jax import lax
from jax.experimental import pallas as pl
from jax.experimental.pallas import tpu as pltpu
from jax.sharding import PartitionSpec as P

D = 2048
DN = 64
VN = 128
DW = 128
VW = 256
TOPK = 4


EPS = 1e-06


def rms_scale(values, gain_row):
    return values * lax.rsqrt(jnp.mean(values * values, axis=-1, keepdims=True) + EPS) * gain_row


MESH = pl.DeviceIdType.MESH
LOG2E = math.log2(math.e)
MASKED = -1e30


def plane_shape(sp_count):
    bits = sp_count.bit_length() - 1
    if 1 << bits != sp_count:
        return sp_count, 1, 1
    columns = 1 << (bits // 3 if bits % 3 == 0 else (bits - bits // 2) // 2)
    rows = columns
    return sp_count // (rows * columns), rows, columns


def attend_kernel(
    dims,
    qn_ref,
    kn_ref,
    vn_ref,
    qw_ref,
    kw_ref,
    vw_ref,
    lamn_ref,
    lamw_ref,
    gainn_ref,
    gainw_ref,
    outn_ref,
    outw_ref,
    kv,
    own,
    raw_n,
    raw_w,
    maps_n,
    att_n,
    att_w,
    row_max,
    row_sum,
    acc_n,
    acc_w,
    lam,
    lam_own,
    load_sem,
    query_sem,
    query_recv,
    recv_sem,
    swap_sem,
    whole_sem,
    up_sem,
    peer_sem,
    pair_sem,
    relay_sem,
    out_send,
    out_recv,
    lam_sem,
):
    planes, rows, columns, _tp_count = dims
    per_plane = rows * columns
    pairs = columns // 2
    grid = rows * pairs
    sp = lax.axis_index("sp")
    tp = lax.axis_index("tp")
    plane = sp // per_plane
    cell = sp % per_plane
    y = cell // columns
    x = cell % columns
    side = x % 2
    across = cell + 1 - 2 * side
    across_sp = plane * per_plane + across
    query_cell = cell - side + tp
    queries = qn_ref.shape[0]
    half_rows = queries // 2
    at_home = side == tp
    away = side != tp

    weights = [lamn_ref[head] for head in range(lamn_ref.shape[0])]
    weights += [lamw_ref[head] for head in range(lamw_ref.shape[0])]
    lam_own[...] = jnp.zeros_like(lam_own)
    for index, weight in enumerate(weights):
        lam_own[index : index + 1, :] = jnp.full((1, lam_own.shape[1]), weight)

    def loads(into):
        copies = []
        begin = 0
        for index, ref in enumerate((kn_ref, vn_ref, kw_ref, vw_ref)):
            width = ref.shape[1]
            copies.append(
                pltpu.make_async_copy(ref, into.at[:, pl.ds(begin, width)], load_sem.at[index])
            )
            begin += width
        return copies

    moved = ((qn_ref, raw_n), (qw_ref, raw_w))

    def query_load(index):
        source, target = moved[index]
        return pltpu.make_async_copy(source, target, query_sem.at[index])

    def query_swap(index):
        source, target = moved[index]
        return pltpu.make_async_remote_copy(
            src_ref=source,
            dst_ref=target,
            send_sem=query_sem.at[index],
            recv_sem=query_recv.at[index],
            device_id={"sp": across_sp, "tp": 1 - tp},
            device_id_type=MESH,
        )

    @pl.when(at_home)
    def _():
        for copy in loads(kv.at[0, cell]) + [query_load(0), query_load(1)]:
            copy.start()

    @pl.when(away)
    def _():
        for copy in loads(own):
            copy.start()

    def peer(k):
        place = (y * pairs + x // 2 + k) % grid
        return place // pairs * columns + place % pairs * 2 + side

    barrier = pltpu.get_barrier_semaphore()

    def greet(device):
        pl.semaphore_signal(barrier, inc=1, device_id=device, device_id_type=MESH)

    for k in range(1, grid):
        greet({"sp": plane * per_plane + peer(k)})
    greet({"tp": 1 - tp})
    for core in range(2):
        greet({"sp": across_sp, "tp": core})

    @pl.when(plane > 0)
    def _():
        greet({"sp": sp - per_plane})

    @pl.when(plane < planes - 1)
    def _():
        greet({"sp": sp + per_plane})

    below = (plane > 0).astype(jnp.int32)
    above = (plane < planes - 1).astype(jnp.int32)
    pl.semaphore_wait(barrier, grid - 1 + 3 + below + above)

    def piece(depth, block, half):
        return kv.at[depth, block, pl.ds(pl.multiple_of(half * half_rows, half_rows), half_rows), :]

    def remote(source, depth, block, half, device, send):
        return pltpu.make_async_remote_copy(
            src_ref=source,
            dst_ref=piece(depth, block, half),
            send_sem=send,
            recv_sem=recv_sem.at[depth, block, half],
            device_id=device,
            device_id_type=MESH,
        )

    def arrived(depth, block, half):
        remote(
            piece(depth, block, half), depth, block, half, {"sp": sp}, up_sem.at[0, 0]
        ).wait_recv()

    def swap_copies():
        return [
            remote(
                own.at[pl.ds(core * half_rows, half_rows), :],
                0,
                cell,
                core,
                {"sp": across_sp, "tp": core},
                swap_sem.at[core],
            )
            for core in range(2)
        ]

    def whole_copies():
        return [
            remote(piece(0, cell, half), 0, cell, half, {"tp": 1 - tp}, whole_sem.at[half])
            for half in range(2)
        ]

    def up_copy(depth, which):
        block = cell if which == 0 else across
        return remote(
            piece(depth, block, tp),
            depth + 1,
            block,
            tp,
            {"sp": sp + per_plane},
            up_sem.at[depth, which],
        )

    def peer_copies(depth, which):
        block = cell if which == 0 else across
        return [
            remote(
                piece(depth, block, tp),
                depth,
                block,
                tp,
                {"sp": plane * per_plane + peer(k)},
                peer_sem.at[depth, which, k],
            )
            for k in range(1, grid)
        ]

    def pair_copy(depth, which):
        block = cell if which == 0 else across
        return remote(
            piece(depth, block, tp), depth, block, tp, {"tp": 1 - tp}, pair_sem.at[depth, which]
        )

    def relay_copy(depth, which, k):
        block = peer(k)
        if which == 1:
            block = block + 1 - 2 * side
        return remote(
            piece(depth, block, tp), depth, block, tp, {"tp": 1 - tp}, relay_sem.at[depth, which, k]
        )

    def spread(depth, which):
        @pl.when(plane < planes - 1)
        def _():
            up_copy(depth, which).start()

        for copy in peer_copies(depth, which):
            copy.start()

    def line(depth):
        for which, block in enumerate((cell, across)):
            arrived(depth, block, tp)
            spread(depth, which)
            pair_copy(depth, which).start()

    def relay(depth):
        for which in range(2):
            for k in range(1, grid):
                block = peer(k) if which == 0 else peer(k) + 1 - 2 * side
                arrived(depth, block, tp)
                relay_copy(depth, which, k).start()

    def finish(depth):
        for k in range(1, grid):
            arrived(depth, peer(k), 1 - tp)
            arrived(depth, peer(k) + 1 - 2 * side, 1 - tp)

    lam_copy = pltpu.make_async_remote_copy(
        src_ref=lam_own,
        dst_ref=lam,
        send_sem=lam_sem.at[0],
        recv_sem=lam_sem.at[1],
        device_id={"tp": 1 - tp},
        device_id_type=MESH,
    )

    @pl.when(at_home)
    def _():
        for copy in loads(kv.at[0, cell]):
            copy.wait()
        for copy in whole_copies():
            copy.start()
        lam_copy.start()
        lam[...] = lam_own[...]

    @pl.when(away)
    def _():
        for copy in loads(own):
            copy.wait()
        for copy in swap_copies() + [query_swap(0), query_swap(1)]:
            copy.start()
        arrived(0, cell, tp)

    spread(0, 0)
    row_max[...] = jnp.full_like(row_max, MASKED)
    row_sum[...] = jnp.zeros_like(row_sum)
    acc_n[...] = jnp.zeros_like(acc_n)
    acc_w[...] = jnp.zeros_like(acc_w)
    heads_n = maps_n.shape[0]
    width_k = kn_ref.shape[1]
    heads_w = qw_ref.shape[1] // kw_ref.shape[1]
    value_n = vn_ref.shape[1]
    begin_kw = width_k + value_n
    map_w = kw_ref.shape[1] // 2
    begin_vw = begin_kw + 2 * map_w
    value_w = vw_ref.shape[1]
    chunk = math.gcd(per_plane, 4)
    key_rows = chunk * queries

    def tile(query, key, value, factor, mask, state, acc, slot):
        scores = lax.dot_general(
            query, key, (((1,), (1,)), ((), ())), preferred_element_type=jnp.float32
        )
        if mask is not None:
            scores = jnp.where(mask, scores, MASKED)
        before = row_max[state][:, :1]
        now = jnp.maximum(before, jnp.max(scores, axis=1, keepdims=True))
        weights = jnp.exp2((scores - now) * factor)
        decay = jnp.exp2((before - now) * factor)
        total = row_sum[state][:, :1] * decay + jnp.sum(weights, axis=1, keepdims=True)
        acc[slot] = acc[slot] * decay + jnp.dot(
            weights.astype(jnp.bfloat16), value, preferred_element_type=jnp.float32
        )
        row_max[state] = jnp.broadcast_to(now, row_max.shape[1:])
        row_sum[state] = jnp.broadcast_to(total, row_sum.shape[1:])

    def attend(depth, masked, group):
        def part(at):
            def columns_of(begin, width):
                return kv[depth, pl.ds(at, chunk), :, begin : begin + width].reshape(
                    key_rows, width
                )

            mask = None
            if masked:
                query_pos = query_cell * queries + lax.broadcasted_iota(
                    jnp.int32, (queries, key_rows), 0
                )
                key_pos = at * queries + lax.broadcasted_iota(jnp.int32, (queries, key_rows), 1)
                mask = key_pos <= query_pos

            def narrow(head, carry):
                key = columns_of(0, width_k)
                value = columns_of(width_k, value_n)
                for which in range(2):
                    index = head * 2 + which
                    tile(
                        maps_n[head, which],
                        key,
                        value,
                        DN**-0.5 * LOG2E,
                        mask,
                        index,
                        acc_n,
                        index,
                    )
                return carry

            def wide(head, carry):
                value = columns_of(begin_vw, value_w)
                for which in range(2):
                    index = head * 2 + which
                    tile(
                        raw_w[:, pl.ds(pl.multiple_of(index * map_w, map_w), map_w)],
                        columns_of(begin_kw + which * map_w, map_w),
                        value,
                        DW**-0.5 * LOG2E,
                        mask,
                        2 * heads_n + index,
                        acc_w,
                        index,
                    )
                return carry

            if group == 0:
                lax.fori_loop(0, heads_n, narrow, 0)
            else:
                lax.fori_loop(0, heads_w, wide, 0)

        if per_plane == chunk:
            part(0)
        else:

            def step(at, carry):
                part(at * chunk)
                return carry

            lax.fori_loop(0, per_plane // chunk, step, 0)

    def close(first, second, weight, gain):
        head = first - weight * second
        scale = lax.rsqrt(jnp.mean(head * head, axis=1, keepdims=True) + EPS)
        return (head * scale * gain).astype(jnp.bfloat16)

    share = outn_ref.shape[0]
    home_sp = plane * per_plane + query_cell

    def out_copies(kind, core):
        att, out = ((att_n, outn_ref), (att_w, outw_ref))[kind]
        width = att.shape[1]
        return pltpu.make_async_remote_copy(
            src_ref=att.at[pl.ds(pl.multiple_of(core * share, share), share), :],
            dst_ref=out.at[:, pl.ds(pl.multiple_of(side * width, width), width)],
            send_sem=out_send.at[kind, core],
            recv_sem=out_recv.at[kind, side],
            device_id={"sp": home_sp, "tp": core},
            device_id_type=MESH,
        )

    def send_out(kind, act):
        @pl.when(at_home)
        def _():
            act(out_copies(kind, 1 - tp))

        @pl.when(away)
        def _():
            for core in range(2):
                act(out_copies(kind, core))

    def keep(kind):
        att, out = ((att_n, outn_ref), (att_w, outw_ref))[kind]
        width = att.shape[1]

        @pl.when(at_home)
        def _():
            out[:, pl.ds(pl.multiple_of(side * width, width), width)] = att[
                pl.ds(pl.multiple_of(tp * share, share), share), :
            ]

    def start(copy):
        copy.start()

    def wait_send(copy):
        copy.wait_send()

    def out_arrived(kind, group):
        att, out = ((att_n, outn_ref), (att_w, outw_ref))[kind]
        width = att.shape[1]
        block = out.at[:, pl.ds(pl.multiple_of(group * width, width), width)]
        pltpu.make_async_remote_copy(
            src_ref=block,
            dst_ref=block,
            send_sem=out_send.at[kind, 0],
            recv_sem=out_recv.at[kind, group],
            device_id={"sp": sp},
            device_id_type=MESH,
        ).wait_recv()

    def close_narrow():
        for head in range(heads_n):
            maps = [acc_n[2 * head + k] / row_sum[2 * head + k][:, :1] for k in range(2)]
            att_n[:, head * value_n : (head + 1) * value_n] = close(
                maps[0], maps[1], lam[head : head + 1, :1], gainn_ref[...]
            )
        send_out(0, start)

    arrived(0, across, tp)
    spread(0, 1)
    pair_copy(0, 1).start()
    relay(0)

    @pl.when(plane > 0)
    def _():
        line(1)

    def query_wait(index):
        @pl.when(at_home)
        def _():
            query_load(index).wait()

        @pl.when(away)
        def _():
            query_swap(index).wait()

    query_wait(0)

    for head in range(heads_n):
        both = raw_n[:, head * width_k : (head + 1) * width_k]
        lane = lax.broadcasted_iota(jnp.int32, both.shape, 1)
        zero = jnp.zeros_like(both)
        maps_n[head, 0] = jnp.where(lane < DN, both, zero)
        maps_n[head, 1] = jnp.where(lane < DN, zero, both)

    @pl.when(away)
    def _():
        arrived(0, cell, 1 - tp)
        lam_copy.wait_recv()

    arrived(0, across, 1 - tp)
    finish(0)
    attend(0, True, 0)

    @pl.when(plane == 0)
    def _():
        close_narrow()

    query_wait(1)
    attend(0, True, 1)

    def depth_step(depth, carry):
        relay(depth)

        @pl.when(depth < plane)
        def _():
            line(depth + 1)

        arrived(depth, cell, 1 - tp)
        arrived(depth, across, 1 - tp)
        finish(depth)
        attend(depth, False, 0)

        @pl.when(depth == plane)
        def _():
            close_narrow()

        attend(depth, False, 1)
        return carry

    lax.fori_loop(1, plane + 1, depth_step, 0)

    for head in range(heads_w):
        maps = [
            acc_w[2 * head + k] / row_sum[2 * (heads_n + head) + k][:, :1] for k in range(2)
        ]
        att_w[:, head * value_w : (head + 1) * value_w] = close(
            maps[0], maps[1], lam[heads_n + head : heads_n + head + 1, :1], gainw_ref[...]
        )
    send_out(1, start)
    keep(0)
    keep(1)

    @pl.when(at_home)
    def _():
        for copy in whole_copies():
            copy.wait_send()
        lam_copy.wait_send()

    @pl.when(away)
    def _():
        for copy in swap_copies():
            copy.wait_send()

    def drain_line(depth, which):
        @pl.when(plane < planes - 1)
        def _():
            up_copy(depth, which).wait_send()

        for copy in peer_copies(depth, which):
            copy.wait_send()
        for k in range(1, grid):
            relay_copy(depth, which, k).wait_send()

    def drain(depth, carry):
        for which in range(2):
            drain_line(depth, which)
            pair_copy(depth, which).wait_send()
        return carry

    drain_line(0, 0)
    drain_line(0, 1)
    pair_copy(0, 1).wait_send()
    lax.fori_loop(1, plane + 1, drain, 0)
    for kind in range(2):
        out_arrived(kind, 1 - side)

        @pl.when(away)
        def _(kind=kind):
            out_arrived(kind, side)

        send_out(kind, wait_send)


def attended_rows(
    sp_count,
    tp_count,
    queries_narrow,
    keys_narrow,
    values_narrow,
    queries_wide,
    keys_wide,
    values_wide,
    lambda_narrow,
    lambda_wide,
    gain_narrow,
    gain_wide,
):
    planes, rows, columns = plane_shape(sp_count)
    count = queries_narrow.shape[0]
    heads_n = queries_narrow.shape[1] // (2 * DN)
    heads_w = queries_wide.shape[1] // (2 * DW)
    width = (
        keys_narrow.shape[1] + values_narrow.shape[1] + keys_wide.shape[1] + values_wide.shape[1]
    )
    per_plane = rows * columns
    grid = per_plane // 2
    tiles = 2 * (heads_n + heads_w)
    share = count // tp_count
    vmem = pl.BlockSpec(memory_space=pltpu.VMEM)
    smem = pl.BlockSpec(memory_space=pltpu.SMEM)
    lambdas = (-(-(heads_n + heads_w) // 8) * 8, 128)
    hbm = pl.BlockSpec(memory_space=pl.ANY)
    dma = pltpu.SemaphoreType.DMA
    return pl.pallas_call(
        functools.partial(attend_kernel, (planes, rows, columns, tp_count)),
        out_shape=[
            jax.ShapeDtypeStruct((share, tp_count * heads_n * VN), jnp.bfloat16),
            jax.ShapeDtypeStruct((share, tp_count * heads_w * VW), jnp.bfloat16),
        ],
        in_specs=[hbm, hbm, hbm, hbm, hbm, hbm, smem, smem, vmem, vmem],
        out_specs=[vmem, vmem],
        scratch_shapes=[
            pltpu.VMEM((planes, per_plane, count, width), jnp.bfloat16),
            pltpu.VMEM((count, width), jnp.bfloat16),
            pltpu.VMEM(queries_narrow.shape, jnp.bfloat16),
            pltpu.VMEM(queries_wide.shape, jnp.bfloat16),
            pltpu.VMEM((heads_n, 2, count, 2 * DN), jnp.bfloat16),
            pltpu.VMEM((count, heads_n * VN), jnp.bfloat16),
            pltpu.VMEM((count, heads_w * VW), jnp.bfloat16),
            pltpu.VMEM((tiles, count, 128), jnp.float32),
            pltpu.VMEM((tiles, count, 128), jnp.float32),
            pltpu.VMEM((2 * heads_n, count, VN), jnp.float32),
            pltpu.VMEM((2 * heads_w, count, VW), jnp.float32),
            pltpu.VMEM(lambdas, jnp.float32),
            pltpu.VMEM(lambdas, jnp.float32),
            dma((4,)),
            dma((2,)),
            dma((2,)),
            dma((planes, per_plane, 2)),
            dma((2,)),
            dma((2,)),
            dma((planes, 2)),
            dma((planes, 2, grid)),
            dma((planes, 2)),
            dma((planes, 2, grid)),
            dma((2, 2)),
            dma((2, 2)),
            dma((2,)),
        ],
        compiler_params=pltpu.CompilerParams(
            collective_id=0, has_side_effects=True, vmem_limit_bytes=56 * 1024 * 1024
        ),
        name="gather_attend",
    )(
        queries_narrow,
        keys_narrow,
        values_narrow,
        queries_wide,
        keys_wide,
        values_wide,
        lambda_narrow,
        lambda_wide,
        gain_narrow.reshape(1, -1),
        gain_wide.reshape(1, -1),
    )


def plane_greeting(planes, rows, columns, tp_count):
    per_plane = rows * columns
    sp = lax.axis_index("sp")
    tp = lax.axis_index("tp")
    plane = sp // per_plane
    cell = sp % per_plane
    barrier = pltpu.get_barrier_semaphore()
    for k in range(1, per_plane):
        pl.semaphore_signal(
            barrier,
            inc=1,
            device_id={"sp": plane * per_plane + (cell + k) % per_plane},
            device_id_type=MESH,
        )
    for k in range(1, planes):
        pl.semaphore_signal(
            barrier,
            inc=1,
            device_id={"sp": (plane + k) % planes * per_plane + cell},
            device_id_type=MESH,
        )
    for k in range(1, tp_count):
        pl.semaphore_signal(
            barrier, inc=1, device_id={"tp": (tp + k) % tp_count}, device_id_type=MESH
        )
    pl.semaphore_wait(barrier, per_plane - 1 + planes - 1 + tp_count - 1)
    return plane, cell, sp, tp


def silu(values):
    return values / (1.0 + jnp.exp(-values))


def expert_kernel(
    dims,
    group,
    chunks,
    normed_ref,
    slots_ref,
    gate_ref,
    up_ref,
    down_ref,
    shared_gate_ref,
    shared_up_ref,
    shared_down_ref,
    mixed_ref,
    gain_ref,
    layer_ref,
    marks,
    shared_out,
    summed,
    held,
    stage,
    inbox,
    result,
    theirs,
    back,
    leaving,
    landed,
    gate,
    up,
    down,
    shared_gate,
    shared_up,
    shared_down,
    load_sem,
    weight_sem,
    row_recv,
    mark_recv,
    row_send,
    mark_send,
    cell_recv,
    cell_send,
    pair_recv,
    pair_send,
    part_recv,
    part_send,
    back_recv,
    back_send,
    far_recv,
    far_send,
):
    planes, rows, columns, tp_count = dims
    per_plane = rows * columns
    mine = lax.axis_index("sp") // per_plane
    loads = [
        pltpu.make_async_copy(normed_ref, held.at[mine], load_sem.at[0]),
        pltpu.make_async_copy(slots_ref, marks.at[mine], load_sem.at[1]),
    ]
    weights = [
        pltpu.make_async_copy(source, target, weight_sem.at[index])
        for index, (source, target) in enumerate(
            (
                (shared_gate_ref, shared_gate),
                (shared_up_ref, shared_up),
                (shared_down_ref, shared_down),
                (gate_ref, gate),
                (up_ref, up),
                (down_ref, down),
            )
        )
    ]
    for copy in loads + weights:
        copy.start()
    plane, cell, sp, tp = plane_greeting(planes, rows, columns, tp_count)
    for copy in loads:
        copy.wait()
    padded = stage.shape[2]
    token_count = held.shape[1]
    width = held.shape[2]
    wide = width // chunks
    local_experts = gate.shape[0]
    capacity = group // local_experts

    def span(chunk):
        return pl.ds(chunk * wide, wide)

    def mark_hop(source, way, target):
        return pltpu.make_async_remote_copy(
            src_ref=marks.at[source],
            dst_ref=marks.at[source],
            send_sem=mark_send.at[source, way],
            recv_sem=mark_recv.at[source],
            device_id={"sp": target},
            device_id_type=MESH,
        )

    def row_hop(source, chunk, way, target):
        block = held.at[source, :, span(chunk)]
        return pltpu.make_async_remote_copy(
            src_ref=block,
            dst_ref=block,
            send_sem=row_send.at[source, chunk, way],
            recv_sem=row_recv.at[source, chunk],
            device_id={"sp": target},
            device_id_type=MESH,
        )

    def to_cell(source, chunk, k):
        other = (cell + k) % per_plane
        return pltpu.make_async_remote_copy(
            src_ref=stage.at[source, other, :, span(chunk)],
            dst_ref=inbox.at[source, tp, cell, :, span(chunk)],
            send_sem=cell_send.at[source, chunk, k],
            recv_sem=cell_recv.at[source, chunk, (per_plane - k) % per_plane],
            device_id={"sp": plane * per_plane + other},
            device_id_type=MESH,
        )

    def from_cell(source, chunk, k):
        return pltpu.make_async_remote_copy(
            src_ref=stage.at[source, cell, :, span(chunk)],
            dst_ref=inbox.at[source, tp, (cell + k) % per_plane, :, span(chunk)],
            send_sem=cell_send.at[source, chunk, k],
            recv_sem=cell_recv.at[source, chunk, k],
            device_id={"sp": sp},
            device_id_type=MESH,
        )

    def to_pair(source, chunk, k):
        block = inbox.at[source, tp, :, :, span(chunk)]
        return pltpu.make_async_remote_copy(
            src_ref=block,
            dst_ref=block,
            send_sem=pair_send.at[source, chunk, k - 1],
            recv_sem=pair_recv.at[source, chunk, k - 1],
            device_id={"tp": (tp + k) % tp_count},
            device_id_type=MESH,
        )

    def part_copy(source, chunk, k):
        other = (tp + k) % tp_count
        return pltpu.make_async_remote_copy(
            src_ref=result.at[source, other, :, :, span(chunk)],
            dst_ref=theirs.at[k - 1, source, :, :, span(chunk)],
            send_sem=part_send.at[source, chunk, k - 1],
            recv_sem=part_recv.at[source, chunk, k - 1],
            device_id={"tp": other},
            device_id_type=MESH,
        )

    def back_to(source, chunk, k):
        other = (cell + k) % per_plane
        return pltpu.make_async_remote_copy(
            src_ref=stage.at[source, other, :, span(chunk)],
            dst_ref=back.at[source, cell, :, span(chunk)],
            send_sem=back_send.at[source, chunk, k],
            recv_sem=back_recv.at[source, chunk, (per_plane - k) % per_plane],
            device_id={"sp": plane * per_plane + other},
            device_id_type=MESH,
        )

    def back_from(source, chunk, k):
        return pltpu.make_async_remote_copy(
            src_ref=stage.at[source, cell, :, span(chunk)],
            dst_ref=back.at[source, (cell + k) % per_plane, :, span(chunk)],
            send_sem=back_send.at[source, chunk, k],
            recv_sem=back_recv.at[source, chunk, k],
            device_id={"sp": sp},
            device_id_type=MESH,
        )

    def homeward(source, chunk, way, target):
        return pltpu.make_async_remote_copy(
            src_ref=leaving.at[source, :, span(chunk)],
            dst_ref=landed.at[way, source, :, span(chunk)],
            send_sem=far_send.at[source, chunk],
            recv_sem=far_recv.at[way, source, chunk],
            device_id={"sp": target},
            device_id_type=MESH,
        )

    def onward(source, act):
        @pl.when((source <= plane) & (plane < planes - 1))
        def _():
            act(0, sp + per_plane)

        @pl.when((source >= plane) & (plane > 0))
        def _():
            act(1, sp - per_plane)

    def forward(source, chunk):
        onward(source, lambda way, target: row_hop(source, chunk, way, target).start())

    def arrive(source):
        mark_hop(source, 0, sp).wait_recv()
        onward(source, lambda way, target: mark_hop(source, way, target).start())
        for chunk in range(chunks):
            row_hop(source, chunk, 0, sp).wait_recv()
            forward(source, chunk)

    def select(source):
        slots = marks[source]
        row = lax.broadcasted_iota(jnp.int32, (padded, token_count), 0)
        picks = []
        for k in list(range(1, per_plane)) + [0]:
            base = (plane * per_plane + (cell + k) % per_plane) * group
            wanted = jnp.where(row < group, row + base, -1).astype(jnp.float32)
            hit = slots[0:1, :] == wanted
            for choice in range(1, TOPK):
                hit = hit | (slots[choice : choice + 1, :] == wanted)
            picks.append((k, jnp.where(hit, 1.0, 0.0).astype(jnp.bfloat16)))
        for chunk in range(chunks):
            tokens = held[source, :, span(chunk)]
            for k, pick in picks:
                chosen = jnp.dot(pick, tokens, preferred_element_type=jnp.float32).astype(
                    jnp.bfloat16
                )
                if k == 0:
                    inbox[source, tp, cell, :, span(chunk)] = chosen
                else:
                    stage[source, (cell + k) % per_plane, :, span(chunk)] = chosen
                    to_cell(source, chunk, k).start()

    def finish(source):
        for chunk in range(chunks):
            for k in range(1, per_plane):
                from_cell(source, chunk, k).wait_recv()
            for k in range(1, tp_count):
                to_pair(source, chunk, k).start()

    def experts(source):
        for chunk in range(chunks):
            for k in range(1, tp_count):
                to_pair(source, chunk, k).wait_recv()
        done = 0
        for index in range(local_experts):
            begin = index * capacity // 16 * 16
            end = -(-((index + 1) * capacity) // 16) * 16
            block = (tp_count, per_plane, end - begin, width)
            tokens = inbox[source, :, :, begin:end, :].reshape(-1, width)
            gated = jnp.dot(tokens, gate[index], preferred_element_type=jnp.float32)
            hidden = silu(gated) * jnp.dot(
                tokens, up[index], preferred_element_type=jnp.float32
            )
            out = (
                jnp.dot(
                    hidden.astype(jnp.bfloat16), down[index], preferred_element_type=jnp.float32
                )
                .astype(jnp.bfloat16)
                .reshape(block)
            )
            both = max(0, done - begin)
            if both > 0:
                shape = (tp_count, per_plane, both, width)
                row = lax.broadcasted_iota(jnp.int32, shape, 2) + begin
                result[source, :, :, begin:done, :] = jnp.where(
                    row < index * capacity, result[source, :, :, begin:done, :], out[:, :, :both]
                )
            if end > begin + both:
                result[source, :, :, begin + both : end, :] = out[:, :, both:]
            done = max(done, end)
        for chunk in range(chunks):
            for k in range(1, tp_count):
                part_copy(source, chunk, k).start()

    def hand_back(source):
        for chunk in range(chunks):
            for k in range(1, per_plane):
                to_cell(source, chunk, k).wait_send()
            for k in range(1, tp_count):
                part_copy(source, chunk, k).wait_recv()
            for k in list(range(1, per_plane)) + [0]:
                other = (cell + k) % per_plane
                total = result[source, tp, other, :, span(chunk)].astype(jnp.float32)
                for i in range(tp_count - 1):
                    total += theirs[i, source, other, :, span(chunk)].astype(jnp.float32)
                if k == 0:
                    back[source, cell, :, span(chunk)] = total.astype(jnp.bfloat16)
                else:
                    stage[source, other, :, span(chunk)] = total.astype(jnp.bfloat16)
                    back_to(source, chunk, k).start()

    def gather_up(source, last):
        slots = marks[source]
        row = lax.broadcasted_iota(jnp.int32, (per_plane * padded, token_count), 0)
        block = lax.div(row, padded)
        inner = row - block * padded
        wanted = jnp.where(
            inner < group, inner + (plane * per_plane + block) * group, -1
        ).astype(jnp.float32)
        share = jnp.zeros(wanted.shape, jnp.float32)
        for choice in range(TOPK):
            share += jnp.where(
                slots[choice : choice + 1, :] == wanted,
                slots[TOPK + choice : TOPK + choice + 1, :],
                0.0,
            )
        coarse = share.astype(jnp.bfloat16)
        fine = (share - coarse.astype(jnp.float32)).astype(jnp.bfloat16)
        both = jnp.concatenate([coarse, fine], axis=1)
        if last:
            comes = [(0, plane > 0), (1, plane < planes - 1)]
        else:
            ahead = source > plane
            behind = source < plane
            comes = [(0, ahead & (plane > 0)), (1, behind & (plane < planes - 1))]
        for chunk in range(chunks):
            for k in range(1, per_plane):
                back_from(source, chunk, k).wait_recv()
            begin = chunk * wide
            for at in range(begin, begin + wide, 512):
                values = back[source, :, :, at : at + 512].reshape(per_plane * padded, 512)
                pieces = lax.dot_general(
                    both, values, (((0,), (0,)), ((), ())), preferred_element_type=jnp.float32
                )
                summed[:, at : at + 512] = pieces[:token_count] + pieces[token_count:]
            for way, exists in comes:

                @pl.when(exists)
                def _(way=way, chunk=chunk):
                    homeward(source, chunk, way, sp).wait_recv()
                    summed[:, span(chunk)] += landed[way, source, :, span(chunk)].astype(
                        jnp.float32
                    )

            if not last:
                leaving[source, :, span(chunk)] = summed[:, span(chunk)].astype(jnp.bfloat16)

                @pl.when(ahead)
                def _(chunk=chunk):
                    homeward(source, chunk, 0, sp + per_plane).start()

                @pl.when(behind)
                def _(chunk=chunk):
                    homeward(source, chunk, 1, sp - per_plane).start()

    onward(plane, lambda way, target: mark_hop(plane, way, target).start())
    for chunk in range(chunks):
        forward(plane, chunk)
    select(plane)
    for copy in weights[:3]:
        copy.wait()
    normed = held[plane]
    shared_hidden = silu(
        jnp.dot(normed, shared_gate[...], preferred_element_type=jnp.float32)
    ) * jnp.dot(normed, shared_up[...], preferred_element_type=jnp.float32)
    shared_out[...] = jnp.dot(
        shared_hidden.astype(jnp.bfloat16), shared_down[...], preferred_element_type=jnp.float32
    )
    for copy in weights[3:]:
        copy.wait()

    at_edge = (plane == 0) | (plane == planes - 1)
    first_out = jnp.where(plane == 0, 1, planes - 2)

    finish(plane)
    experts(plane)

    def process(source):
        finish(source)
        experts(source)
        hand_back(source)

    def each(distance, act):
        def one(side, carry):
            source = plane + (2 * side - 1) * distance

            @pl.when((source >= 0) & (source < planes))
            def _():
                act(source)

            return carry

        lax.fori_loop(0, 2, one, 0)

    def step(distance, carry):
        each(distance, arrive)
        each(distance, select)

        @pl.when(distance > 1)
        def _():
            each(distance - 1, process)

        return carry

    lax.fori_loop(1, planes, step, 0)

    @pl.when(at_edge & (planes > 2))
    def _():
        gather_up(first_out, False)

    each(planes - 1, process)
    hand_back(plane)

    def chain(index, carry):
        low, high = carry
        use_high = (low < 0) | (
            (high < planes)
            & (2 * high + plane <= 2 * (planes - 1 - low) + (planes - 1 - plane))
        )
        source = jnp.where(use_high, high, low)

        @pl.when(jnp.logical_not(at_edge & (index == 0) & (planes > 2)))
        def _():
            gather_up(source, False)

        return jnp.where(use_high, low, low - 1), jnp.where(use_high, high + 1, high)

    lax.fori_loop(0, planes - 1, chain, (plane - 1, plane + 1))
    gather_up(plane, True)
    layer_ref[...] = (
        mixed_ref[...].astype(jnp.float32)
        + rms_scale(shared_out[...] + summed[...], gain_ref[...])
    ).astype(jnp.bfloat16)

    def drain(source, carry):
        onward(source, lambda way, target: mark_hop(source, way, target).wait_send())
        for chunk in range(chunks):
            onward(
                source, lambda way, target: row_hop(source, chunk, way, target).wait_send()
            )
            for k in range(1, per_plane):
                back_to(source, chunk, k).wait_send()
            for k in range(1, tp_count):
                to_pair(source, chunk, k).wait_send()
                part_copy(source, chunk, k).wait_send()

            @pl.when(source != plane)
            def _():
                homeward(source, chunk, 0, sp).wait_send()

        return carry

    lax.fori_loop(0, planes, drain, 0)


def expert_rows(
    dims,
    group,
    normed,
    slot_index,
    route_weights,
    routed_weights,
    shared_weights,
    mixed,
    gain,
):
    planes, rows, columns, tp_count = dims
    per_plane = rows * columns
    token_count, width = normed.shape
    padded = -(-group // 16) * 16
    slots = slot_index.reshape(token_count, TOPK).astype(jnp.float32)
    slots = jnp.concatenate([slots, route_weights], axis=1).T
    hbm = pl.BlockSpec(memory_space=pl.ANY)
    vmem = pl.BlockSpec(memory_space=pltpu.VMEM)
    dma = pltpu.SemaphoreType.DMA
    chunks = math.gcd(width // 512, 4)
    pairs = max(1, tp_count - 1)
    weights = list(routed_weights) + list(shared_weights)
    block = (planes, per_plane, padded, width)
    inbox = (planes, tp_count, per_plane, padded, width)
    return pl.pallas_call(
        functools.partial(expert_kernel, dims, group, chunks),
        out_shape=jax.ShapeDtypeStruct((token_count, width), jnp.bfloat16),
        in_specs=[hbm] * (2 + len(weights)) + [vmem, vmem],
        out_specs=vmem,
        scratch_shapes=[
            pltpu.VMEM((planes, 2 * TOPK, token_count), jnp.float32),
            pltpu.VMEM((token_count, width), jnp.float32),
            pltpu.VMEM((token_count, width), jnp.float32),
            pltpu.VMEM((planes, token_count, width), jnp.bfloat16),
            pltpu.VMEM(block, jnp.bfloat16),
            pltpu.VMEM(inbox, jnp.bfloat16),
            pltpu.VMEM(inbox, jnp.bfloat16),
            pltpu.VMEM((pairs,) + block, jnp.bfloat16),
            pltpu.VMEM(block, jnp.bfloat16),
            pltpu.VMEM((planes, token_count, width), jnp.bfloat16),
            pltpu.VMEM((2, planes, token_count, width), jnp.bfloat16),
        ]
        + [pltpu.VMEM(weight.shape, jnp.bfloat16) for weight in weights]
        + [
            dma((2,)),
            dma((len(weights),)),
            dma((planes, chunks)),
            dma((planes,)),
            dma((planes, chunks, 2)),
            dma((planes, 2)),
            dma((planes, chunks, per_plane)),
            dma((planes, chunks, per_plane)),
            dma((planes, chunks, pairs)),
            dma((planes, chunks, pairs)),
            dma((planes, chunks, pairs)),
            dma((planes, chunks, pairs)),
            dma((planes, chunks, per_plane)),
            dma((planes, chunks, per_plane)),
            dma((2, planes, chunks)),
            dma((planes, chunks)),
        ],
        compiler_params=pltpu.CompilerParams(
            collective_id=1, has_side_effects=True, vmem_limit_bytes=60 * 1024 * 1024
        ),
        name="expert_layer",
    )(normed, slots, *weights, mixed, gain.reshape(1, -1))


def shards(
    queries_narrow,
    keys_narrow,
    values_narrow,
    queries_wide,
    keys_wide,
    values_wide,
    lambda_narrow,
    lambda_wide,
    gain_narrow,
    gain_wide,
    out_narrow,
    out_wide,
    stream,
    gain_mix,
    gain_ffn,
    gain_post,
    shared_gate,
    shared_up,
    shared_down,
    expert_gate,
    expert_up,
    expert_down,
    expert_ids,
    route_weights,
):
    sp_count = lax.axis_size("sp")
    narrow_rows, wide_rows = attended_rows(
        sp_count,
        lax.axis_size("tp"),
        queries_narrow,
        keys_narrow,
        values_narrow,
        queries_wide,
        keys_wide,
        values_wide,
        lambda_narrow,
        lambda_wide,
        gain_narrow,
        gain_wide,
    )
    projected = jnp.dot(narrow_rows, out_narrow, preferred_element_type=jnp.float32) + jnp.dot(
        wide_rows, out_wide, preferred_element_type=jnp.float32
    )
    mixed_rows = (stream.astype(jnp.float32) + rms_scale(projected, gain_mix)).astype(jnp.bfloat16)
    normed = rms_scale(mixed_rows.astype(jnp.float32), gain_ffn).astype(jnp.bfloat16)
    row_count = normed.shape[0]
    tp_count = lax.axis_size("tp")
    local_experts = expert_gate.shape[0]
    experts_all = local_experts * sp_count
    capacity = max(2, 3 * row_count * TOPK // (2 * experts_all))
    chosen = (
        expert_ids[:, :, None] == jnp.arange(experts_all, dtype=jnp.int32)[None, None, :]
    ).astype(jnp.float32)
    named = jnp.sum(chosen, axis=1)
    order = jnp.arange(row_count, dtype=jnp.int32)
    earlier = jnp.dot(
        (order[None, :] < order[:, None]).astype(jnp.bfloat16),
        named.astype(jnp.bfloat16),
        preferred_element_type=jnp.float32,
    )
    slot_rank = jnp.sum(chosen * earlier[:, None, :], axis=2).astype(jnp.int32)
    slot_index = expert_ids * capacity + slot_rank
    group = local_experts * capacity
    dims = plane_shape(sp_count) + (tp_count,)
    return expert_rows(
        dims,
        group,
        normed,
        slot_index,
        route_weights,
        (expert_gate, expert_up, expert_down),
        (shared_gate, shared_up, shared_down),
        mixed_rows,
        gain_post,
    )


def solution(mesh):
    return jax.shard_map(
        shards,
        mesh=mesh,
        in_specs=(
            P("sp", "tp"),
            P("sp", "tp"),
            P("sp", "tp"),
            P("sp", "tp"),
            P("sp", "tp"),
            P("sp", "tp"),
            P("tp"),
            P("tp"),
            P(),
            P(),
            P(),
            P(),
            P(("sp", "tp"), None),
            P(),
            P(),
            P(),
            P(),
            P(),
            P(),
            P("sp", None, "tp"),
            P("sp", None, "tp"),
            P("sp", "tp", None),
            P(("sp", "tp"), None),
            P(("sp", "tp"), None),
        ),
        out_specs=P(("sp", "tp"), None),
        check_vma=False,
    )
```

```python
import functools
import math

import jax
import jax.numpy as jnp
from jax import lax
from jax.experimental import pallas as pl
from jax.experimental.pallas import tpu as pltpu
from jax.sharding import PartitionSpec as P

D = 2048
DN = 64
VN = 128
DW = 128
VW = 256
TOPK = 4


EPS = 1e-06


def rms_scale(values, gain_row):
    return values * lax.rsqrt(jnp.mean(values * values, axis=-1, keepdims=True) + EPS) * gain_row


MESH = pl.DeviceIdType.MESH
LOG2E = math.log2(math.e)
MASKED = -1e30


def plane_shape(sp_count):
    bits = sp_count.bit_length() - 1
    if 1 << bits != sp_count:
        return sp_count, 1, 1
    columns = 1 << (bits // 3 if bits % 3 == 0 else (bits - bits // 2) // 2)
    rows = columns
    return sp_count // (rows * columns), rows, columns


def attend_kernel(
    dims,
    qn_ref,
    kn_ref,
    vn_ref,
    qw_ref,
    kw_ref,
    vw_ref,
    lamn_ref,
    lamw_ref,
    gainn_ref,
    gainw_ref,
    outn_ref,
    outw_ref,
    kv,
    own,
    raw_n,
    raw_w,
    maps_n,
    att_n,
    att_w,
    row_max,
    row_sum,
    acc_n,
    acc_w,
    lam,
    lam_own,
    load_sem,
    query_sem,
    query_recv,
    recv_sem,
    swap_sem,
    whole_sem,
    up_sem,
    peer_sem,
    pair_sem,
    relay_sem,
    out_send,
    out_recv,
    lam_sem,
):
    planes, rows, columns, _tp_count = dims
    per_plane = rows * columns
    pairs = columns // 2
    grid = rows * pairs
    sp = lax.axis_index("sp")
    tp = lax.axis_index("tp")
    plane = sp // per_plane
    cell = sp % per_plane
    y = cell // columns
    x = cell % columns
    side = x % 2
    across = cell + 1 - 2 * side
    across_sp = plane * per_plane + across
    query_cell = cell - side + tp
    queries = qn_ref.shape[0]
    half_rows = queries // 2
    at_home = side == tp
    away = side != tp

    weights = [lamn_ref[head] for head in range(lamn_ref.shape[0])]
    weights += [lamw_ref[head] for head in range(lamw_ref.shape[0])]
    lam_own[...] = jnp.zeros_like(lam_own)
    for index, weight in enumerate(weights):
        lam_own[index : index + 1, :] = jnp.full((1, lam_own.shape[1]), weight)

    def loads(into):
        copies = []
        begin = 0
        for index, ref in enumerate((kn_ref, vn_ref, kw_ref, vw_ref)):
            width = ref.shape[1]
            copies.append(
                pltpu.make_async_copy(ref, into.at[:, pl.ds(begin, width)], load_sem.at[index])
            )
            begin += width
        return copies

    moved = ((qn_ref, raw_n), (qw_ref, raw_w))

    def query_load(index):
        source, target = moved[index]
        return pltpu.make_async_copy(source, target, query_sem.at[index])

    def query_swap(index):
        source, target = moved[index]
        return pltpu.make_async_remote_copy(
            src_ref=source,
            dst_ref=target,
            send_sem=query_sem.at[index],
            recv_sem=query_recv.at[index],
            device_id={"sp": across_sp, "tp": 1 - tp},
            device_id_type=MESH,
        )

    @pl.when(at_home)
    def _():
        for copy in loads(kv.at[0, cell]) + [query_load(0), query_load(1)]:
            copy.start()

    @pl.when(away)
    def _():
        for copy in loads(own):
            copy.start()

    def peer(k):
        place = (y * pairs + x // 2 + k) % grid
        return place // pairs * columns + place % pairs * 2 + side

    barrier = pltpu.get_barrier_semaphore()

    def greet(device):
        pl.semaphore_signal(barrier, inc=1, device_id=device, device_id_type=MESH)

    for k in range(1, grid):
        greet({"sp": plane * per_plane + peer(k)})
    greet({"tp": 1 - tp})
    for core in range(2):
        greet({"sp": across_sp, "tp": core})

    @pl.when(plane > 0)
    def _():
        greet({"sp": sp - per_plane})

    @pl.when(plane < planes - 1)
    def _():
        greet({"sp": sp + per_plane})

    below = (plane > 0).astype(jnp.int32)
    above = (plane < planes - 1).astype(jnp.int32)
    pl.semaphore_wait(barrier, grid - 1 + 3 + below + above)

    def piece(depth, block, half):
        return kv.at[depth, block, pl.ds(pl.multiple_of(half * half_rows, half_rows), half_rows), :]

    def remote(source, depth, block, half, device, send):
        return pltpu.make_async_remote_copy(
            src_ref=source,
            dst_ref=piece(depth, block, half),
            send_sem=send,
            recv_sem=recv_sem.at[depth, block, half],
            device_id=device,
            device_id_type=MESH,
        )

    def arrived(depth, block, half):
        remote(
            piece(depth, block, half), depth, block, half, {"sp": sp}, up_sem.at[0, 0]
        ).wait_recv()

    def swap_copies():
        return [
            remote(
                own.at[pl.ds(core * half_rows, half_rows), :],
                0,
                cell,
                core,
                {"sp": across_sp, "tp": core},
                swap_sem.at[core],
            )
            for core in range(2)
        ]

    def whole_copies():
        return [
            remote(piece(0, cell, half), 0, cell, half, {"tp": 1 - tp}, whole_sem.at[half])
            for half in range(2)
        ]

    def up_copy(depth, which):
        block = cell if which == 0 else across
        return remote(
            piece(depth, block, tp),
            depth + 1,
            block,
            tp,
            {"sp": sp + per_plane},
            up_sem.at[depth, which],
        )

    def peer_copies(depth, which):
        block = cell if which == 0 else across
        return [
            remote(
                piece(depth, block, tp),
                depth,
                block,
                tp,
                {"sp": plane * per_plane + peer(k)},
                peer_sem.at[depth, which, k],
            )
            for k in range(1, grid)
        ]

    def pair_copy(depth, which):
        block = cell if which == 0 else across
        return remote(
            piece(depth, block, tp), depth, block, tp, {"tp": 1 - tp}, pair_sem.at[depth, which]
        )

    def relay_copy(depth, which, k):
        block = peer(k)
        if which == 1:
            block = block + 1 - 2 * side
        return remote(
            piece(depth, block, tp), depth, block, tp, {"tp": 1 - tp}, relay_sem.at[depth, which, k]
        )

    def spread(depth, which):
        @pl.when(plane < planes - 1)
        def _():
            up_copy(depth, which).start()

        for copy in peer_copies(depth, which):
            copy.start()

    def line(depth):
        for which, block in enumerate((cell, across)):
            arrived(depth, block, tp)
            spread(depth, which)
            pair_copy(depth, which).start()

    def relay(depth):
        for which in range(2):
            for k in range(1, grid):
                block = peer(k) if which == 0 else peer(k) + 1 - 2 * side
                arrived(depth, block, tp)
                relay_copy(depth, which, k).start()

    def finish(depth):
        for k in range(1, grid):
            arrived(depth, peer(k), 1 - tp)
            arrived(depth, peer(k) + 1 - 2 * side, 1 - tp)

    lam_copy = pltpu.make_async_remote_copy(
        src_ref=lam_own,
        dst_ref=lam,
        send_sem=lam_sem.at[0],
        recv_sem=lam_sem.at[1],
        device_id={"tp": 1 - tp},
        device_id_type=MESH,
    )

    @pl.when(at_home)
    def _():
        for copy in loads(kv.at[0, cell]):
            copy.wait()
        for copy in whole_copies():
            copy.start()
        lam_copy.start()
        lam[...] = lam_own[...]

    @pl.when(away)
    def _():
        for copy in loads(own):
            copy.wait()
        for copy in swap_copies() + [query_swap(0), query_swap(1)]:
            copy.start()
        arrived(0, cell, tp)

    spread(0, 0)
    row_max[...] = jnp.full_like(row_max, MASKED)
    row_sum[...] = jnp.zeros_like(row_sum)
    acc_n[...] = jnp.zeros_like(acc_n)
    acc_w[...] = jnp.zeros_like(acc_w)
    heads_n = maps_n.shape[0]
    width_k = kn_ref.shape[1]
    heads_w = qw_ref.shape[1] // kw_ref.shape[1]
    value_n = vn_ref.shape[1]
    begin_kw = width_k + value_n
    map_w = kw_ref.shape[1] // 2
    begin_vw = begin_kw + 2 * map_w
    value_w = vw_ref.shape[1]
    chunk = math.gcd(per_plane, 4)
    key_rows = chunk * queries

    def tile(query, key, value, factor, mask, state, acc, slot):
        scores = lax.dot_general(
            query, key, (((1,), (1,)), ((), ())), preferred_element_type=jnp.float32
        )
        if mask is not None:
            scores = jnp.where(mask, scores, MASKED)
        before = row_max[state][:, :1]
        now = jnp.maximum(before, jnp.max(scores, axis=1, keepdims=True))
        weights = jnp.exp2((scores - now) * factor)
        decay = jnp.exp2((before - now) * factor)
        total = row_sum[state][:, :1] * decay + jnp.sum(weights, axis=1, keepdims=True)
        acc[slot] = acc[slot] * decay + jnp.dot(
            weights.astype(jnp.bfloat16), value, preferred_element_type=jnp.float32
        )
        row_max[state] = jnp.broadcast_to(now, row_max.shape[1:])
        row_sum[state] = jnp.broadcast_to(total, row_sum.shape[1:])

    def attend(depth, masked, group):
        def part(at):
            def columns_of(begin, width):
                return kv[depth, pl.ds(at, chunk), :, begin : begin + width].reshape(
                    key_rows, width
                )

            mask = None
            if masked:
                query_pos = query_cell * queries + lax.broadcasted_iota(
                    jnp.int32, (queries, key_rows), 0
                )
                key_pos = at * queries + lax.broadcasted_iota(jnp.int32, (queries, key_rows), 1)
                mask = key_pos <= query_pos

            def narrow(head, carry):
                key = columns_of(0, width_k)
                value = columns_of(width_k, value_n)
                for which in range(2):
                    index = head * 2 + which
                    tile(
                        maps_n[head, which],
                        key,
                        value,
                        DN**-0.5 * LOG2E,
                        mask,
                        index,
                        acc_n,
                        index,
                    )
                return carry

            def wide(head, carry):
                value = columns_of(begin_vw, value_w)
                for which in range(2):
                    index = head * 2 + which
                    tile(
                        raw_w[:, pl.ds(pl.multiple_of(index * map_w, map_w), map_w)],
                        columns_of(begin_kw + which * map_w, map_w),
                        value,
                        DW**-0.5 * LOG2E,
                        mask,
                        2 * heads_n + index,
                        acc_w,
                        index,
                    )
                return carry

            if group == 0:
                lax.fori_loop(0, heads_n, narrow, 0)
            else:
                lax.fori_loop(0, heads_w, wide, 0)

        if per_plane == chunk:
            part(0)
        else:

            def step(at, carry):
                part(at * chunk)
                return carry

            lax.fori_loop(0, per_plane // chunk, step, 0)

    def close(first, second, weight, gain):
        head = first - weight * second
        scale = lax.rsqrt(jnp.mean(head * head, axis=1, keepdims=True) + EPS)
        return (head * scale * gain).astype(jnp.bfloat16)

    share = outn_ref.shape[0]
    home_sp = plane * per_plane + query_cell

    def out_copies(kind, core):
        att, out = ((att_n, outn_ref), (att_w, outw_ref))[kind]
        width = att.shape[1]
        return pltpu.make_async_remote_copy(
            src_ref=att.at[pl.ds(pl.multiple_of(core * share, share), share), :],
            dst_ref=out.at[:, pl.ds(pl.multiple_of(side * width, width), width)],
            send_sem=out_send.at[kind, core],
            recv_sem=out_recv.at[kind, side],
            device_id={"sp": home_sp, "tp": core},
            device_id_type=MESH,
        )

    def send_out(kind, act):
        @pl.when(at_home)
        def _():
            act(out_copies(kind, 1 - tp))

        @pl.when(away)
        def _():
            for core in range(2):
                act(out_copies(kind, core))

    def keep(kind):
        att, out = ((att_n, outn_ref), (att_w, outw_ref))[kind]
        width = att.shape[1]

        @pl.when(at_home)
        def _():
            out[:, pl.ds(pl.multiple_of(side * width, width), width)] = att[
                pl.ds(pl.multiple_of(tp * share, share), share), :
            ]

    def start(copy):
        copy.start()

    def wait_send(copy):
        copy.wait_send()

    def out_arrived(kind, group):
        att, out = ((att_n, outn_ref), (att_w, outw_ref))[kind]
        width = att.shape[1]
        block = out.at[:, pl.ds(pl.multiple_of(group * width, width), width)]
        pltpu.make_async_remote_copy(
            src_ref=block,
            dst_ref=block,
            send_sem=out_send.at[kind, 0],
            recv_sem=out_recv.at[kind, group],
            device_id={"sp": sp},
            device_id_type=MESH,
        ).wait_recv()

    def close_narrow():
        for head in range(heads_n):
            maps = [acc_n[2 * head + k] / row_sum[2 * head + k][:, :1] for k in range(2)]
            att_n[:, head * value_n : (head + 1) * value_n] = close(
                maps[0], maps[1], lam[head : head + 1, :1], gainn_ref[...]
            )
        send_out(0, start)

    arrived(0, across, tp)
    spread(0, 1)
    pair_copy(0, 1).start()
    relay(0)

    @pl.when(plane > 0)
    def _():
        line(1)

    def query_wait(index):
        @pl.when(at_home)
        def _():
            query_load(index).wait()

        @pl.when(away)
        def _():
            query_swap(index).wait()

    query_wait(0)

    for head in range(heads_n):
        both = raw_n[:, head * width_k : (head + 1) * width_k]
        lane = lax.broadcasted_iota(jnp.int32, both.shape, 1)
        zero = jnp.zeros_like(both)
        maps_n[head, 0] = jnp.where(lane < DN, both, zero)
        maps_n[head, 1] = jnp.where(lane < DN, zero, both)

    @pl.when(away)
    def _():
        arrived(0, cell, 1 - tp)
        lam_copy.wait_recv()

    arrived(0, across, 1 - tp)
    finish(0)
    attend(0, True, 0)

    @pl.when(plane == 0)
    def _():
        close_narrow()

    query_wait(1)
    attend(0, True, 1)

    def depth_step(depth, carry):
        relay(depth)

        @pl.when(depth < plane)
        def _():
            line(depth + 1)

        arrived(depth, cell, 1 - tp)
        arrived(depth, across, 1 - tp)
        finish(depth)
        attend(depth, False, 0)

        @pl.when(depth == plane)
        def _():
            close_narrow()

        attend(depth, False, 1)
        return carry

    lax.fori_loop(1, plane + 1, depth_step, 0)

    for head in range(heads_w):
        maps = [
            acc_w[2 * head + k] / row_sum[2 * (heads_n + head) + k][:, :1] for k in range(2)
        ]
        att_w[:, head * value_w : (head + 1) * value_w] = close(
            maps[0], maps[1], lam[heads_n + head : heads_n + head + 1, :1], gainw_ref[...]
        )
    send_out(1, start)
    keep(0)
    keep(1)

    @pl.when(at_home)
    def _():
        for copy in whole_copies():
            copy.wait_send()
        lam_copy.wait_send()

    @pl.when(away)
    def _():
        for copy in swap_copies():
            copy.wait_send()

    def drain_line(depth, which):
        @pl.when(plane < planes - 1)
        def _():
            up_copy(depth, which).wait_send()

        for copy in peer_copies(depth, which):
            copy.wait_send()
        for k in range(1, grid):
            relay_copy(depth, which, k).wait_send()

    def drain(depth, carry):
        for which in range(2):
            drain_line(depth, which)
            pair_copy(depth, which).wait_send()
        return carry

    drain_line(0, 0)
    drain_line(0, 1)
    pair_copy(0, 1).wait_send()
    lax.fori_loop(1, plane + 1, drain, 0)
    for kind in range(2):
        out_arrived(kind, 1 - side)

        @pl.when(away)
        def _(kind=kind):
            out_arrived(kind, side)

        send_out(kind, wait_send)


def attended_rows(
    sp_count,
    tp_count,
    queries_narrow,
    keys_narrow,
    values_narrow,
    queries_wide,
    keys_wide,
    values_wide,
    lambda_narrow,
    lambda_wide,
    gain_narrow,
    gain_wide,
):
    planes, rows, columns = plane_shape(sp_count)
    count = queries_narrow.shape[0]
    heads_n = queries_narrow.shape[1] // (2 * DN)
    heads_w = queries_wide.shape[1] // (2 * DW)
    width = (
        keys_narrow.shape[1] + values_narrow.shape[1] + keys_wide.shape[1] + values_wide.shape[1]
    )
    per_plane = rows * columns
    grid = per_plane // 2
    tiles = 2 * (heads_n + heads_w)
    share = count // tp_count
    vmem = pl.BlockSpec(memory_space=pltpu.VMEM)
    smem = pl.BlockSpec(memory_space=pltpu.SMEM)
    lambdas = (-(-(heads_n + heads_w) // 8) * 8, 128)
    hbm = pl.BlockSpec(memory_space=pl.ANY)
    dma = pltpu.SemaphoreType.DMA
    return pl.pallas_call(
        functools.partial(attend_kernel, (planes, rows, columns, tp_count)),
        out_shape=[
            jax.ShapeDtypeStruct((share, tp_count * heads_n * VN), jnp.bfloat16),
            jax.ShapeDtypeStruct((share, tp_count * heads_w * VW), jnp.bfloat16),
        ],
        in_specs=[hbm, hbm, hbm, hbm, hbm, hbm, smem, smem, vmem, vmem],
        out_specs=[vmem, vmem],
        scratch_shapes=[
            pltpu.VMEM((planes, per_plane, count, width), jnp.bfloat16),
            pltpu.VMEM((count, width), jnp.bfloat16),
            pltpu.VMEM(queries_narrow.shape, jnp.bfloat16),
            pltpu.VMEM(queries_wide.shape, jnp.bfloat16),
            pltpu.VMEM((heads_n, 2, count, 2 * DN), jnp.bfloat16),
            pltpu.VMEM((count, heads_n * VN), jnp.bfloat16),
            pltpu.VMEM((count, heads_w * VW), jnp.bfloat16),
            pltpu.VMEM((tiles, count, 128), jnp.float32),
            pltpu.VMEM((tiles, count, 128), jnp.float32),
            pltpu.VMEM((2 * heads_n, count, VN), jnp.float32),
            pltpu.VMEM((2 * heads_w, count, VW), jnp.float32),
            pltpu.VMEM(lambdas, jnp.float32),
            pltpu.VMEM(lambdas, jnp.float32),
            dma((4,)),
            dma((2,)),
            dma((2,)),
            dma((planes, per_plane, 2)),
            dma((2,)),
            dma((2,)),
            dma((planes, 2)),
            dma((planes, 2, grid)),
            dma((planes, 2)),
            dma((planes, 2, grid)),
            dma((2, 2)),
            dma((2, 2)),
            dma((2,)),
        ],
        compiler_params=pltpu.CompilerParams(
            collective_id=0, has_side_effects=True, vmem_limit_bytes=56 * 1024 * 1024
        ),
        name="gather_attend",
    )(
        queries_narrow,
        keys_narrow,
        values_narrow,
        queries_wide,
        keys_wide,
        values_wide,
        lambda_narrow,
        lambda_wide,
        gain_narrow.reshape(1, -1),
        gain_wide.reshape(1, -1),
    )


def plane_greeting(planes, rows, columns, tp_count):
    per_plane = rows * columns
    sp = lax.axis_index("sp")
    tp = lax.axis_index("tp")
    plane = sp // per_plane
    cell = sp % per_plane
    barrier = pltpu.get_barrier_semaphore()
    for k in range(1, per_plane):
        pl.semaphore_signal(
            barrier,
            inc=1,
            device_id={"sp": plane * per_plane + (cell + k) % per_plane},
            device_id_type=MESH,
        )
    for k in range(1, planes):
        pl.semaphore_signal(
            barrier,
            inc=1,
            device_id={"sp": (plane + k) % planes * per_plane + cell},
            device_id_type=MESH,
        )
    for k in range(1, tp_count):
        pl.semaphore_signal(
            barrier, inc=1, device_id={"tp": (tp + k) % tp_count}, device_id_type=MESH
        )
    pl.semaphore_wait(barrier, per_plane - 1 + planes - 1 + tp_count - 1)
    return plane, cell, sp, tp


def silu(values):
    return values / (1.0 + jnp.exp(-values))


def expert_kernel(
    dims,
    group,
    chunks,
    normed_ref,
    slots_ref,
    gate_ref,
    up_ref,
    down_ref,
    shared_gate_ref,
    shared_up_ref,
    shared_down_ref,
    mixed_ref,
    gain_ref,
    layer_ref,
    marks,
    shared_out,
    summed,
    held,
    stage,
    inbox,
    result,
    theirs,
    back,
    leaving,
    landed,
    gate,
    up,
    down,
    shared_gate,
    shared_up,
    shared_down,
    load_sem,
    weight_sem,
    row_recv,
    mark_recv,
    row_send,
    mark_send,
    cell_recv,
    cell_send,
    pair_recv,
    pair_send,
    part_recv,
    part_send,
    back_recv,
    back_send,
    far_recv,
    far_send,
):
    planes, rows, columns, tp_count = dims
    per_plane = rows * columns
    mine = lax.axis_index("sp") // per_plane
    loads = [
        pltpu.make_async_copy(normed_ref, held.at[mine], load_sem.at[0]),
        pltpu.make_async_copy(slots_ref, marks.at[mine], load_sem.at[1]),
    ]
    weights = [
        pltpu.make_async_copy(source, target, weight_sem.at[index])
        for index, (source, target) in enumerate(
            (
                (shared_gate_ref, shared_gate),
                (shared_up_ref, shared_up),
                (shared_down_ref, shared_down),
                (gate_ref, gate),
                (up_ref, up),
                (down_ref, down),
            )
        )
    ]
    for copy in loads + weights:
        copy.start()
    plane, cell, sp, tp = plane_greeting(planes, rows, columns, tp_count)
    for copy in loads:
        copy.wait()
    padded = stage.shape[2]
    token_count = held.shape[1]
    width = held.shape[2]
    wide = width // chunks
    local_experts = gate.shape[0]
    capacity = group // local_experts

    def span(chunk):
        return pl.ds(chunk * wide, wide)

    def mark_hop(source, way, target):
        return pltpu.make_async_remote_copy(
            src_ref=marks.at[source],
            dst_ref=marks.at[source],
            send_sem=mark_send.at[source, way],
            recv_sem=mark_recv.at[source],
            device_id={"sp": target},
            device_id_type=MESH,
        )

    def row_hop(source, chunk, way, target):
        block = held.at[source, :, span(chunk)]
        return pltpu.make_async_remote_copy(
            src_ref=block,
            dst_ref=block,
            send_sem=row_send.at[source, chunk, way],
            recv_sem=row_recv.at[source, chunk],
            device_id={"sp": target},
            device_id_type=MESH,
        )

    def to_cell(source, chunk, k):
        other = (cell + k) % per_plane
        return pltpu.make_async_remote_copy(
            src_ref=stage.at[source, other, :, span(chunk)],
            dst_ref=inbox.at[source, tp, cell, :, span(chunk)],
            send_sem=cell_send.at[source, chunk, k],
            recv_sem=cell_recv.at[source, chunk, (per_plane - k) % per_plane],
            device_id={"sp": plane * per_plane + other},
            device_id_type=MESH,
        )

    def from_cell(source, chunk, k):
        return pltpu.make_async_remote_copy(
            src_ref=stage.at[source, cell, :, span(chunk)],
            dst_ref=inbox.at[source, tp, (cell + k) % per_plane, :, span(chunk)],
            send_sem=cell_send.at[source, chunk, k],
            recv_sem=cell_recv.at[source, chunk, k],
            device_id={"sp": sp},
            device_id_type=MESH,
        )

    def to_pair(source, chunk, k):
        block = inbox.at[source, tp, :, :, span(chunk)]
        return pltpu.make_async_remote_copy(
            src_ref=block,
            dst_ref=block,
            send_sem=pair_send.at[source, chunk, k - 1],
            recv_sem=pair_recv.at[source, chunk, k - 1],
            device_id={"tp": (tp + k) % tp_count},
            device_id_type=MESH,
        )

    def part_copy(source, chunk, k):
        other = (tp + k) % tp_count
        return pltpu.make_async_remote_copy(
            src_ref=result.at[source, other, :, :, span(chunk)],
            dst_ref=theirs.at[k - 1, source, :, :, span(chunk)],
            send_sem=part_send.at[source, chunk, k - 1],
            recv_sem=part_recv.at[source, chunk, k - 1],
            device_id={"tp": other},
            device_id_type=MESH,
        )

    def back_to(source, chunk, k):
        other = (cell + k) % per_plane
        return pltpu.make_async_remote_copy(
            src_ref=stage.at[source, other, :, span(chunk)],
            dst_ref=back.at[source, cell, :, span(chunk)],
            send_sem=back_send.at[source, chunk, k],
            recv_sem=back_recv.at[source, chunk, (per_plane - k) % per_plane],
            device_id={"sp": plane * per_plane + other},
            device_id_type=MESH,
        )

    def back_from(source, chunk, k):
        return pltpu.make_async_remote_copy(
            src_ref=stage.at[source, cell, :, span(chunk)],
            dst_ref=back.at[source, (cell + k) % per_plane, :, span(chunk)],
            send_sem=back_send.at[source, chunk, k],
            recv_sem=back_recv.at[source, chunk, k],
            device_id={"sp": sp},
            device_id_type=MESH,
        )

    def homeward(source, chunk, way, target):
        return pltpu.make_async_remote_copy(
            src_ref=leaving.at[source, :, span(chunk)],
            dst_ref=landed.at[way, source, :, span(chunk)],
            send_sem=far_send.at[source, chunk],
            recv_sem=far_recv.at[way, source, chunk],
            device_id={"sp": target},
            device_id_type=MESH,
        )

    def onward(source, act):
        @pl.when((source <= plane) & (plane < planes - 1))
        def _():
            act(0, sp + per_plane)

        @pl.when((source >= plane) & (plane > 0))
        def _():
            act(1, sp - per_plane)

    def forward(source, chunk):
        onward(source, lambda way, target: row_hop(source, chunk, way, target).start())

    def arrive(source):
        mark_hop(source, 0, sp).wait_recv()
        onward(source, lambda way, target: mark_hop(source, way, target).start())
        for chunk in range(chunks):
            row_hop(source, chunk, 0, sp).wait_recv()
            forward(source, chunk)

    def select(source):
        slots = marks[source]
        row = lax.broadcasted_iota(jnp.int32, (padded, token_count), 0)
        picks = []
        for k in list(range(1, per_plane)) + [0]:
            base = (plane * per_plane + (cell + k) % per_plane) * group
            wanted = jnp.where(row < group, row + base, -1).astype(jnp.float32)
            hit = slots[0:1, :] == wanted
            for choice in range(1, TOPK):
                hit = hit | (slots[choice : choice + 1, :] == wanted)
            picks.append((k, jnp.where(hit, 1.0, 0.0).astype(jnp.bfloat16)))
        for chunk in range(chunks):
            tokens = held[source, :, span(chunk)]
            for k, pick in picks:
                chosen = jnp.dot(pick, tokens, preferred_element_type=jnp.float32).astype(
                    jnp.bfloat16
                )
                if k == 0:
                    inbox[source, tp, cell, :, span(chunk)] = chosen
                else:
                    stage[source, (cell + k) % per_plane, :, span(chunk)] = chosen
                    to_cell(source, chunk, k).start()

    def finish(source):
        for chunk in range(chunks):
            for k in range(1, per_plane):
                from_cell(source, chunk, k).wait_recv()
            for k in range(1, tp_count):
                to_pair(source, chunk, k).start()

    def experts(source):
        for chunk in range(chunks):
            for k in range(1, tp_count):
                to_pair(source, chunk, k).wait_recv()
        done = 0
        for index in range(local_experts):
            begin = index * capacity // 16 * 16
            end = -(-((index + 1) * capacity) // 16) * 16
            block = (tp_count, per_plane, end - begin, width)
            tokens = inbox[source, :, :, begin:end, :].reshape(-1, width)
            gated = jnp.dot(tokens, gate[index], preferred_element_type=jnp.float32)
            hidden = silu(gated) * jnp.dot(
                tokens, up[index], preferred_element_type=jnp.float32
            )
            out = (
                jnp.dot(
                    hidden.astype(jnp.bfloat16), down[index], preferred_element_type=jnp.float32
                )
                .astype(jnp.bfloat16)
                .reshape(block)
            )
            both = max(0, done - begin)
            if both > 0:
                shape = (tp_count, per_plane, both, width)
                row = lax.broadcasted_iota(jnp.int32, shape, 2) + begin
                result[source, :, :, begin:done, :] = jnp.where(
                    row < index * capacity, result[source, :, :, begin:done, :], out[:, :, :both]
                )
            if end > begin + both:
                result[source, :, :, begin + both : end, :] = out[:, :, both:]
            done = max(done, end)
        for chunk in range(chunks):
            for k in range(1, tp_count):
                part_copy(source, chunk, k).start()

    def hand_back(source):
        for chunk in range(chunks):
            for k in range(1, per_plane):
                to_cell(source, chunk, k).wait_send()
            for k in range(1, tp_count):
                part_copy(source, chunk, k).wait_recv()
            for k in list(range(1, per_plane)) + [0]:
                other = (cell + k) % per_plane
                total = result[source, tp, other, :, span(chunk)].astype(jnp.float32)
                for i in range(tp_count - 1):
                    total += theirs[i, source, other, :, span(chunk)].astype(jnp.float32)
                if k == 0:
                    back[source, cell, :, span(chunk)] = total.astype(jnp.bfloat16)
                else:
                    stage[source, other, :, span(chunk)] = total.astype(jnp.bfloat16)
                    back_to(source, chunk, k).start()

    def gather_up(source, last):
        slots = marks[source]
        row = lax.broadcasted_iota(jnp.int32, (per_plane * padded, token_count), 0)
        block = lax.div(row, padded)
        inner = row - block * padded
        wanted = jnp.where(
            inner < group, inner + (plane * per_plane + block) * group, -1
        ).astype(jnp.float32)
        share = jnp.zeros(wanted.shape, jnp.float32)
        for choice in range(TOPK):
            share += jnp.where(
                slots[choice : choice + 1, :] == wanted,
                slots[TOPK + choice : TOPK + choice + 1, :],
                0.0,
            )
        coarse = share.astype(jnp.bfloat16)
        fine = (share - coarse.astype(jnp.float32)).astype(jnp.bfloat16)
        both = jnp.concatenate([coarse, fine], axis=1)
        if last:
            comes = [(0, plane > 0), (1, plane < planes - 1)]
        else:
            ahead = source > plane
            behind = source < plane
            comes = [(0, ahead & (plane > 0)), (1, behind & (plane < planes - 1))]
        for chunk in range(chunks):
            for k in range(1, per_plane):
                back_from(source, chunk, k).wait_recv()
            begin = chunk * wide
            for at in range(begin, begin + wide, 512):
                values = back[source, :, :, at : at + 512].reshape(per_plane * padded, 512)
                pieces = lax.dot_general(
                    both, values, (((0,), (0,)), ((), ())), preferred_element_type=jnp.float32
                )
                summed[:, at : at + 512] = pieces[:token_count] + pieces[token_count:]
            for way, exists in comes:

                @pl.when(exists)
                def _(way=way, chunk=chunk):
                    homeward(source, chunk, way, sp).wait_recv()
                    summed[:, span(chunk)] += landed[way, source, :, span(chunk)].astype(
                        jnp.float32
                    )

            if not last:
                leaving[source, :, span(chunk)] = summed[:, span(chunk)].astype(jnp.bfloat16)

                @pl.when(ahead)
                def _(chunk=chunk):
                    homeward(source, chunk, 0, sp + per_plane).start()

                @pl.when(behind)
                def _(chunk=chunk):
                    homeward(source, chunk, 1, sp - per_plane).start()

    onward(plane, lambda way, target: mark_hop(plane, way, target).start())
    for chunk in range(chunks):
        forward(plane, chunk)
    select(plane)
    for copy in weights[:3]:
        copy.wait()
    normed = held[plane]
    shared_hidden = silu(
        jnp.dot(normed, shared_gate[...], preferred_element_type=jnp.float32)
    ) * jnp.dot(normed, shared_up[...], preferred_element_type=jnp.float32)
    shared_out[...] = jnp.dot(
        shared_hidden.astype(jnp.bfloat16), shared_down[...], preferred_element_type=jnp.float32
    )
    for copy in weights[3:]:
        copy.wait()

    at_edge = (plane == 0) | (plane == planes - 1)
    first_out = jnp.where(plane == 0, 1, planes - 2)

    finish(plane)
    experts(plane)

    def process(source):
        finish(source)
        experts(source)
        hand_back(source)

    def each(distance, act):
        def one(side, carry):
            source = plane + (2 * side - 1) * distance

            @pl.when((source >= 0) & (source < planes))
            def _():
                act(source)

            return carry

        lax.fori_loop(0, 2, one, 0)

    def step(distance, carry):
        each(distance, arrive)
        each(distance, select)

        @pl.when(at_edge & (planes > 2) & (distance == planes - 1))
        def _():
            gather_up(first_out, False)

        @pl.when(distance > 1)
        def _():
            each(distance - 1, process)

        return carry

    lax.fori_loop(1, planes, step, 0)

    each(planes - 1, process)
    hand_back(plane)

    def chain(index, carry):
        low, high = carry
        use_high = (low < 0) | (
            (high < planes)
            & (2 * high + plane <= 2 * (planes - 1 - low) + (planes - 1 - plane))
        )
        source = jnp.where(use_high, high, low)

        @pl.when(jnp.logical_not(at_edge & (index == 0) & (planes > 2)))
        def _():
            gather_up(source, False)

        return jnp.where(use_high, low, low - 1), jnp.where(use_high, high + 1, high)

    lax.fori_loop(0, planes - 1, chain, (plane - 1, plane + 1))
    gather_up(plane, True)
    layer_ref[...] = (
        mixed_ref[...].astype(jnp.float32)
        + rms_scale(shared_out[...] + summed[...], gain_ref[...])
    ).astype(jnp.bfloat16)

    def drain(source, carry):
        onward(source, lambda way, target: mark_hop(source, way, target).wait_send())
        for chunk in range(chunks):
            onward(
                source, lambda way, target: row_hop(source, chunk, way, target).wait_send()
            )
            for k in range(1, per_plane):
                back_to(source, chunk, k).wait_send()
            for k in range(1, tp_count):
                to_pair(source, chunk, k).wait_send()
                part_copy(source, chunk, k).wait_send()

            @pl.when(source != plane)
            def _():
                homeward(source, chunk, 0, sp).wait_send()

        return carry

    lax.fori_loop(0, planes, drain, 0)


def expert_rows(
    dims,
    group,
    normed,
    slot_index,
    route_weights,
    routed_weights,
    shared_weights,
    mixed,
    gain,
):
    planes, rows, columns, tp_count = dims
    per_plane = rows * columns
    token_count, width = normed.shape
    padded = -(-group // 16) * 16
    slots = slot_index.reshape(token_count, TOPK).astype(jnp.float32)
    slots = jnp.concatenate([slots, route_weights], axis=1).T
    hbm = pl.BlockSpec(memory_space=pl.ANY)
    vmem = pl.BlockSpec(memory_space=pltpu.VMEM)
    dma = pltpu.SemaphoreType.DMA
    chunks = math.gcd(width // 512, 4)
    pairs = max(1, tp_count - 1)
    weights = list(routed_weights) + list(shared_weights)
    block = (planes, per_plane, padded, width)
    inbox = (planes, tp_count, per_plane, padded, width)
    return pl.pallas_call(
        functools.partial(expert_kernel, dims, group, chunks),
        out_shape=jax.ShapeDtypeStruct((token_count, width), jnp.bfloat16),
        in_specs=[hbm] * (2 + len(weights)) + [vmem, vmem],
        out_specs=vmem,
        scratch_shapes=[
            pltpu.VMEM((planes, 2 * TOPK, token_count), jnp.float32),
            pltpu.VMEM((token_count, width), jnp.float32),
            pltpu.VMEM((token_count, width), jnp.float32),
            pltpu.VMEM((planes, token_count, width), jnp.bfloat16),
            pltpu.VMEM(block, jnp.bfloat16),
            pltpu.VMEM(inbox, jnp.bfloat16),
            pltpu.VMEM(inbox, jnp.bfloat16),
            pltpu.VMEM((pairs,) + block, jnp.bfloat16),
            pltpu.VMEM(block, jnp.bfloat16),
            pltpu.VMEM((planes, token_count, width), jnp.bfloat16),
            pltpu.VMEM((2, planes, token_count, width), jnp.bfloat16),
        ]
        + [pltpu.VMEM(weight.shape, jnp.bfloat16) for weight in weights]
        + [
            dma((2,)),
            dma((len(weights),)),
            dma((planes, chunks)),
            dma((planes,)),
            dma((planes, chunks, 2)),
            dma((planes, 2)),
            dma((planes, chunks, per_plane)),
            dma((planes, chunks, per_plane)),
            dma((planes, chunks, pairs)),
            dma((planes, chunks, pairs)),
            dma((planes, chunks, pairs)),
            dma((planes, chunks, pairs)),
            dma((planes, chunks, per_plane)),
            dma((planes, chunks, per_plane)),
            dma((2, planes, chunks)),
            dma((planes, chunks)),
        ],
        compiler_params=pltpu.CompilerParams(
            collective_id=1, has_side_effects=True, vmem_limit_bytes=60 * 1024 * 1024
        ),
        name="expert_layer",
    )(normed, slots, *weights, mixed, gain.reshape(1, -1))


def shards(
    queries_narrow,
    keys_narrow,
    values_narrow,
    queries_wide,
    keys_wide,
    values_wide,
    lambda_narrow,
    lambda_wide,
    gain_narrow,
    gain_wide,
    out_narrow,
    out_wide,
    stream,
    gain_mix,
    gain_ffn,
    gain_post,
    shared_gate,
    shared_up,
    shared_down,
    expert_gate,
    expert_up,
    expert_down,
    expert_ids,
    route_weights,
):
    sp_count = lax.axis_size("sp")
    narrow_rows, wide_rows = attended_rows(
        sp_count,
        lax.axis_size("tp"),
        queries_narrow,
        keys_narrow,
        values_narrow,
        queries_wide,
        keys_wide,
        values_wide,
        lambda_narrow,
        lambda_wide,
        gain_narrow,
        gain_wide,
    )
    projected = jnp.dot(narrow_rows, out_narrow, preferred_element_type=jnp.float32) + jnp.dot(
        wide_rows, out_wide, preferred_element_type=jnp.float32
    )
    mixed_rows = (stream.astype(jnp.float32) + rms_scale(projected, gain_mix)).astype(jnp.bfloat16)
    normed = rms_scale(mixed_rows.astype(jnp.float32), gain_ffn).astype(jnp.bfloat16)
    row_count = normed.shape[0]
    tp_count = lax.axis_size("tp")
    local_experts = expert_gate.shape[0]
    experts_all = local_experts * sp_count
    capacity = max(2, 3 * row_count * TOPK // (2 * experts_all))
    chosen = (
        expert_ids[:, :, None] == jnp.arange(experts_all, dtype=jnp.int32)[None, None, :]
    ).astype(jnp.float32)
    named = jnp.sum(chosen, axis=1)
    order = jnp.arange(row_count, dtype=jnp.int32)
    earlier = jnp.dot(
        (order[None, :] < order[:, None]).astype(jnp.bfloat16),
        named.astype(jnp.bfloat16),
        preferred_element_type=jnp.float32,
    )
    slot_rank = jnp.sum(chosen * earlier[:, None, :], axis=2).astype(jnp.int32)
    slot_index = expert_ids * capacity + slot_rank
    group = local_experts * capacity
    dims = plane_shape(sp_count) + (tp_count,)
    return expert_rows(
        dims,
        group,
        normed,
        slot_index,
        route_weights,
        (expert_gate, expert_up, expert_down),
        (shared_gate, shared_up, shared_down),
        mixed_rows,
        gain_post,
    )


def solution(mesh):
    return jax.shard_map(
        shards,
        mesh=mesh,
        in_specs=(
            P("sp", "tp"),
            P("sp", "tp"),
            P("sp", "tp"),
            P("sp", "tp"),
            P("sp", "tp"),
            P("sp", "tp"),
            P("tp"),
            P("tp"),
            P(),
            P(),
            P(),
            P(),
            P(("sp", "tp"), None),
            P(),
            P(),
            P(),
            P(),
            P(),
            P(),
            P("sp", None, "tp"),
            P("sp", None, "tp"),
            P("sp", "tp", None),
            P(("sp", "tp"), None),
            P(("sp", "tp"), None),
        ),
        out_specs=P(("sp", "tp"), None),
        check_vma=False,
    )
```

```python
import functools
import math

import jax
import jax.numpy as jnp
from jax import lax
from jax.experimental import pallas as pl
from jax.experimental.pallas import tpu as pltpu
from jax.sharding import PartitionSpec as P

D = 2048
DN = 64
VN = 128
DW = 128
VW = 256
TOPK = 4


EPS = 1e-06


def rms_scale(values, gain_row):
    return values * lax.rsqrt(jnp.mean(values * values, axis=-1, keepdims=True) + EPS) * gain_row


MESH = pl.DeviceIdType.MESH
LOG2E = math.log2(math.e)
MASKED = -1e30


def plane_shape(sp_count):
    bits = sp_count.bit_length() - 1
    if 1 << bits != sp_count:
        return sp_count, 1, 1
    columns = 1 << (bits // 3 if bits % 3 == 0 else (bits - bits // 2) // 2)
    rows = columns
    return sp_count // (rows * columns), rows, columns


def attend_kernel(
    dims,
    qn_ref,
    kn_ref,
    vn_ref,
    qw_ref,
    kw_ref,
    vw_ref,
    lamn_ref,
    lamw_ref,
    gainn_ref,
    gainw_ref,
    outn_ref,
    outw_ref,
    kv,
    own,
    raw_n,
    raw_w,
    maps_n,
    att_n,
    att_w,
    row_max,
    row_sum,
    acc_n,
    acc_w,
    lam,
    lam_own,
    load_sem,
    query_sem,
    query_recv,
    recv_sem,
    swap_sem,
    whole_sem,
    up_sem,
    peer_sem,
    pair_sem,
    relay_sem,
    out_send,
    out_recv,
    lam_sem,
):
    planes, rows, columns, _tp_count = dims
    per_plane = rows * columns
    pairs = columns // 2
    grid = rows * pairs
    sp = lax.axis_index("sp")
    tp = lax.axis_index("tp")
    plane = sp // per_plane
    cell = sp % per_plane
    y = cell // columns
    x = cell % columns
    side = x % 2
    across = cell + 1 - 2 * side
    across_sp = plane * per_plane + across
    query_cell = cell - side + tp
    queries = qn_ref.shape[0]
    half_rows = queries // 2
    at_home = side == tp
    away = side != tp

    weights = [lamn_ref[head] for head in range(lamn_ref.shape[0])]
    weights += [lamw_ref[head] for head in range(lamw_ref.shape[0])]
    lam_own[...] = jnp.zeros_like(lam_own)
    for index, weight in enumerate(weights):
        lam_own[index : index + 1, :] = jnp.full((1, lam_own.shape[1]), weight)

    def loads(into):
        copies = []
        begin = 0
        for index, ref in enumerate((kn_ref, vn_ref, kw_ref, vw_ref)):
            width = ref.shape[1]
            copies.append(
                pltpu.make_async_copy(ref, into.at[:, pl.ds(begin, width)], load_sem.at[index])
            )
            begin += width
        return copies

    moved = ((qn_ref, raw_n), (qw_ref, raw_w))

    def query_load(index):
        source, target = moved[index]
        return pltpu.make_async_copy(source, target, query_sem.at[index])

    def query_swap(index):
        source, target = moved[index]
        return pltpu.make_async_remote_copy(
            src_ref=source,
            dst_ref=target,
            send_sem=query_sem.at[index],
            recv_sem=query_recv.at[index],
            device_id={"sp": across_sp, "tp": 1 - tp},
            device_id_type=MESH,
        )

    @pl.when(at_home)
    def _():
        for copy in loads(kv.at[0, cell]) + [query_load(0), query_load(1)]:
            copy.start()

    @pl.when(away)
    def _():
        for copy in loads(own):
            copy.start()

    def peer(k):
        place = (y * pairs + x // 2 + k) % grid
        return place // pairs * columns + place % pairs * 2 + side

    barrier = pltpu.get_barrier_semaphore()

    def greet(device):
        pl.semaphore_signal(barrier, inc=1, device_id=device, device_id_type=MESH)

    for k in range(1, grid):
        greet({"sp": plane * per_plane + peer(k)})
    greet({"tp": 1 - tp})
    for core in range(2):
        greet({"sp": across_sp, "tp": core})

    @pl.when(plane > 0)
    def _():
        greet({"sp": sp - per_plane})

    @pl.when(plane < planes - 1)
    def _():
        greet({"sp": sp + per_plane})

    below = (plane > 0).astype(jnp.int32)
    above = (plane < planes - 1).astype(jnp.int32)
    pl.semaphore_wait(barrier, grid - 1 + 3 + below + above)

    def piece(depth, block, half):
        return kv.at[depth, block, pl.ds(pl.multiple_of(half * half_rows, half_rows), half_rows), :]

    def remote(source, depth, block, half, device, send):
        return pltpu.make_async_remote_copy(
            src_ref=source,
            dst_ref=piece(depth, block, half),
            send_sem=send,
            recv_sem=recv_sem.at[depth, block, half],
            device_id=device,
            device_id_type=MESH,
        )

    def arrived(depth, block, half):
        remote(
            piece(depth, block, half), depth, block, half, {"sp": sp}, up_sem.at[0, 0]
        ).wait_recv()

    def swap_copies():
        return [
            remote(
                own.at[pl.ds(core * half_rows, half_rows), :],
                0,
                cell,
                core,
                {"sp": across_sp, "tp": core},
                swap_sem.at[core],
            )
            for core in range(2)
        ]

    def whole_copies():
        return [
            remote(piece(0, cell, half), 0, cell, half, {"tp": 1 - tp}, whole_sem.at[half])
            for half in range(2)
        ]

    def up_copy(depth, which):
        block = cell if which == 0 else across
        return remote(
            piece(depth, block, tp),
            depth + 1,
            block,
            tp,
            {"sp": sp + per_plane},
            up_sem.at[depth, which],
        )

    def peer_copies(depth, which):
        block = cell if which == 0 else across
        return [
            remote(
                piece(depth, block, tp),
                depth,
                block,
                tp,
                {"sp": plane * per_plane + peer(k)},
                peer_sem.at[depth, which, k],
            )
            for k in range(1, grid)
        ]

    def pair_copy(depth, which):
        block = cell if which == 0 else across
        return remote(
            piece(depth, block, tp), depth, block, tp, {"tp": 1 - tp}, pair_sem.at[depth, which]
        )

    def relay_copy(depth, which, k):
        block = peer(k)
        if which == 1:
            block = block + 1 - 2 * side
        return remote(
            piece(depth, block, tp), depth, block, tp, {"tp": 1 - tp}, relay_sem.at[depth, which, k]
        )

    def spread(depth, which):
        @pl.when(plane < planes - 1)
        def _():
            up_copy(depth, which).start()

        for copy in peer_copies(depth, which):
            copy.start()

    def line(depth):
        for which, block in enumerate((cell, across)):
            arrived(depth, block, tp)
            spread(depth, which)
            pair_copy(depth, which).start()

    def relay(depth):
        for which in range(2):
            for k in range(1, grid):
                block = peer(k) if which == 0 else peer(k) + 1 - 2 * side
                arrived(depth, block, tp)
                relay_copy(depth, which, k).start()

    def finish(depth):
        for k in range(1, grid):
            arrived(depth, peer(k), 1 - tp)
            arrived(depth, peer(k) + 1 - 2 * side, 1 - tp)

    lam_copy = pltpu.make_async_remote_copy(
        src_ref=lam_own,
        dst_ref=lam,
        send_sem=lam_sem.at[0],
        recv_sem=lam_sem.at[1],
        device_id={"tp": 1 - tp},
        device_id_type=MESH,
    )

    @pl.when(at_home)
    def _():
        for copy in loads(kv.at[0, cell]):
            copy.wait()
        for copy in whole_copies():
            copy.start()
        lam_copy.start()
        lam[...] = lam_own[...]

    @pl.when(away)
    def _():
        for copy in loads(own):
            copy.wait()
        for copy in swap_copies() + [query_swap(0), query_swap(1)]:
            copy.start()
        arrived(0, cell, tp)

    spread(0, 0)
    row_max[...] = jnp.full_like(row_max, MASKED)
    row_sum[...] = jnp.zeros_like(row_sum)
    acc_n[...] = jnp.zeros_like(acc_n)
    acc_w[...] = jnp.zeros_like(acc_w)
    heads_n = maps_n.shape[0]
    width_k = kn_ref.shape[1]
    heads_w = qw_ref.shape[1] // kw_ref.shape[1]
    value_n = vn_ref.shape[1]
    begin_kw = width_k + value_n
    map_w = kw_ref.shape[1] // 2
    begin_vw = begin_kw + 2 * map_w
    value_w = vw_ref.shape[1]
    chunk = math.gcd(per_plane, 4)
    key_rows = chunk * queries

    def tile(query, key, value, factor, mask, state, acc, slot):
        scores = lax.dot_general(
            query, key, (((1,), (1,)), ((), ())), preferred_element_type=jnp.float32
        )
        if mask is not None:
            scores = jnp.where(mask, scores, MASKED)
        before = row_max[state][:, :1]
        now = jnp.maximum(before, jnp.max(scores, axis=1, keepdims=True))
        weights = jnp.exp2((scores - now) * factor)
        decay = jnp.exp2((before - now) * factor)
        total = row_sum[state][:, :1] * decay + jnp.sum(weights, axis=1, keepdims=True)
        acc[slot] = acc[slot] * decay + jnp.dot(
            weights.astype(jnp.bfloat16), value, preferred_element_type=jnp.float32
        )
        row_max[state] = jnp.broadcast_to(now, row_max.shape[1:])
        row_sum[state] = jnp.broadcast_to(total, row_sum.shape[1:])

    def attend(depth, masked, group):
        def part(at):
            def columns_of(begin, width):
                return kv[depth, pl.ds(at, chunk), :, begin : begin + width].reshape(
                    key_rows, width
                )

            mask = None
            if masked:
                query_pos = query_cell * queries + lax.broadcasted_iota(
                    jnp.int32, (queries, key_rows), 0
                )
                key_pos = at * queries + lax.broadcasted_iota(jnp.int32, (queries, key_rows), 1)
                mask = key_pos <= query_pos

            def narrow(head, carry):
                key = columns_of(0, width_k)
                value = columns_of(width_k, value_n)
                for which in range(2):
                    index = head * 2 + which
                    tile(
                        maps_n[head, which],
                        key,
                        value,
                        DN**-0.5 * LOG2E,
                        mask,
                        index,
                        acc_n,
                        index,
                    )
                return carry

            def wide(head, carry):
                value = columns_of(begin_vw, value_w)
                for which in range(2):
                    index = head * 2 + which
                    tile(
                        raw_w[:, pl.ds(pl.multiple_of(index * map_w, map_w), map_w)],
                        columns_of(begin_kw + which * map_w, map_w),
                        value,
                        DW**-0.5 * LOG2E,
                        mask,
                        2 * heads_n + index,
                        acc_w,
                        index,
                    )
                return carry

            if group == 0:
                lax.fori_loop(0, heads_n, narrow, 0)
            else:
                lax.fori_loop(0, heads_w, wide, 0)

        if per_plane == chunk:
            part(0)
        else:

            def step(at, carry):
                part(at * chunk)
                return carry

            lax.fori_loop(0, per_plane // chunk, step, 0)

    def close(first, second, weight, gain):
        head = first - weight * second
        scale = lax.rsqrt(jnp.mean(head * head, axis=1, keepdims=True) + EPS)
        return (head * scale * gain).astype(jnp.bfloat16)

    share = outn_ref.shape[0]
    home_sp = plane * per_plane + query_cell

    def out_copies(kind, core):
        att, out = ((att_n, outn_ref), (att_w, outw_ref))[kind]
        width = att.shape[1]
        return pltpu.make_async_remote_copy(
            src_ref=att.at[pl.ds(pl.multiple_of(core * share, share), share), :],
            dst_ref=out.at[:, pl.ds(pl.multiple_of(side * width, width), width)],
            send_sem=out_send.at[kind, core],
            recv_sem=out_recv.at[kind, side],
            device_id={"sp": home_sp, "tp": core},
            device_id_type=MESH,
        )

    def send_out(kind, act):
        @pl.when(at_home)
        def _():
            act(out_copies(kind, 1 - tp))

        @pl.when(away)
        def _():
            for core in range(2):
                act(out_copies(kind, core))

    def keep(kind):
        att, out = ((att_n, outn_ref), (att_w, outw_ref))[kind]
        width = att.shape[1]

        @pl.when(at_home)
        def _():
            out[:, pl.ds(pl.multiple_of(side * width, width), width)] = att[
                pl.ds(pl.multiple_of(tp * share, share), share), :
            ]

    def start(copy):
        copy.start()

    def wait_send(copy):
        copy.wait_send()

    def out_arrived(kind, group):
        att, out = ((att_n, outn_ref), (att_w, outw_ref))[kind]
        width = att.shape[1]
        block = out.at[:, pl.ds(pl.multiple_of(group * width, width), width)]
        pltpu.make_async_remote_copy(
            src_ref=block,
            dst_ref=block,
            send_sem=out_send.at[kind, 0],
            recv_sem=out_recv.at[kind, group],
            device_id={"sp": sp},
            device_id_type=MESH,
        ).wait_recv()

    def close_narrow():
        for head in range(heads_n):
            maps = [acc_n[2 * head + k] / row_sum[2 * head + k][:, :1] for k in range(2)]
            att_n[:, head * value_n : (head + 1) * value_n] = close(
                maps[0], maps[1], lam[head : head + 1, :1], gainn_ref[...]
            )
        send_out(0, start)

    arrived(0, across, tp)
    spread(0, 1)
    pair_copy(0, 1).start()
    relay(0)

    @pl.when(plane > 0)
    def _():
        line(1)

    def query_wait(index):
        @pl.when(at_home)
        def _():
            query_load(index).wait()

        @pl.when(away)
        def _():
            query_swap(index).wait()

    query_wait(0)

    for head in range(heads_n):
        both = raw_n[:, head * width_k : (head + 1) * width_k]
        lane = lax.broadcasted_iota(jnp.int32, both.shape, 1)
        zero = jnp.zeros_like(both)
        maps_n[head, 0] = jnp.where(lane < DN, both, zero)
        maps_n[head, 1] = jnp.where(lane < DN, zero, both)

    @pl.when(away)
    def _():
        arrived(0, cell, 1 - tp)
        lam_copy.wait_recv()

    arrived(0, across, 1 - tp)
    finish(0)
    attend(0, True, 0)

    @pl.when(plane == 0)
    def _():
        close_narrow()

    query_wait(1)
    attend(0, True, 1)

    def depth_step(depth, carry):
        relay(depth)

        @pl.when(depth < plane)
        def _():
            line(depth + 1)

        arrived(depth, cell, 1 - tp)
        arrived(depth, across, 1 - tp)
        finish(depth)
        attend(depth, False, 0)

        @pl.when(depth == plane)
        def _():
            close_narrow()

        attend(depth, False, 1)
        return carry

    lax.fori_loop(1, plane + 1, depth_step, 0)

    for head in range(heads_w):
        maps = [
            acc_w[2 * head + k] / row_sum[2 * (heads_n + head) + k][:, :1] for k in range(2)
        ]
        att_w[:, head * value_w : (head + 1) * value_w] = close(
            maps[0], maps[1], lam[heads_n + head : heads_n + head + 1, :1], gainw_ref[...]
        )
    send_out(1, start)
    keep(0)
    keep(1)

    @pl.when(at_home)
    def _():
        for copy in whole_copies():
            copy.wait_send()
        lam_copy.wait_send()

    @pl.when(away)
    def _():
        for copy in swap_copies():
            copy.wait_send()

    def drain_line(depth, which):
        @pl.when(plane < planes - 1)
        def _():
            up_copy(depth, which).wait_send()

        for copy in peer_copies(depth, which):
            copy.wait_send()
        for k in range(1, grid):
            relay_copy(depth, which, k).wait_send()

    def drain(depth, carry):
        for which in range(2):
            drain_line(depth, which)
            pair_copy(depth, which).wait_send()
        return carry

    drain_line(0, 0)
    drain_line(0, 1)
    pair_copy(0, 1).wait_send()
    lax.fori_loop(1, plane + 1, drain, 0)
    for kind in range(2):
        out_arrived(kind, 1 - side)

        @pl.when(away)
        def _(kind=kind):
            out_arrived(kind, side)

        send_out(kind, wait_send)


def attended_rows(
    sp_count,
    tp_count,
    queries_narrow,
    keys_narrow,
    values_narrow,
    queries_wide,
    keys_wide,
    values_wide,
    lambda_narrow,
    lambda_wide,
    gain_narrow,
    gain_wide,
):
    planes, rows, columns = plane_shape(sp_count)
    count = queries_narrow.shape[0]
    heads_n = queries_narrow.shape[1] // (2 * DN)
    heads_w = queries_wide.shape[1] // (2 * DW)
    width = (
        keys_narrow.shape[1] + values_narrow.shape[1] + keys_wide.shape[1] + values_wide.shape[1]
    )
    per_plane = rows * columns
    grid = per_plane // 2
    tiles = 2 * (heads_n + heads_w)
    share = count // tp_count
    vmem = pl.BlockSpec(memory_space=pltpu.VMEM)
    smem = pl.BlockSpec(memory_space=pltpu.SMEM)
    lambdas = (-(-(heads_n + heads_w) // 8) * 8, 128)
    hbm = pl.BlockSpec(memory_space=pl.ANY)
    dma = pltpu.SemaphoreType.DMA
    return pl.pallas_call(
        functools.partial(attend_kernel, (planes, rows, columns, tp_count)),
        out_shape=[
            jax.ShapeDtypeStruct((share, tp_count * heads_n * VN), jnp.bfloat16),
            jax.ShapeDtypeStruct((share, tp_count * heads_w * VW), jnp.bfloat16),
        ],
        in_specs=[hbm, hbm, hbm, hbm, hbm, hbm, smem, smem, vmem, vmem],
        out_specs=[vmem, vmem],
        scratch_shapes=[
            pltpu.VMEM((planes, per_plane, count, width), jnp.bfloat16),
            pltpu.VMEM((count, width), jnp.bfloat16),
            pltpu.VMEM(queries_narrow.shape, jnp.bfloat16),
            pltpu.VMEM(queries_wide.shape, jnp.bfloat16),
            pltpu.VMEM((heads_n, 2, count, 2 * DN), jnp.bfloat16),
            pltpu.VMEM((count, heads_n * VN), jnp.bfloat16),
            pltpu.VMEM((count, heads_w * VW), jnp.bfloat16),
            pltpu.VMEM((tiles, count, 128), jnp.float32),
            pltpu.VMEM((tiles, count, 128), jnp.float32),
            pltpu.VMEM((2 * heads_n, count, VN), jnp.float32),
            pltpu.VMEM((2 * heads_w, count, VW), jnp.float32),
            pltpu.VMEM(lambdas, jnp.float32),
            pltpu.VMEM(lambdas, jnp.float32),
            dma((4,)),
            dma((2,)),
            dma((2,)),
            dma((planes, per_plane, 2)),
            dma((2,)),
            dma((2,)),
            dma((planes, 2)),
            dma((planes, 2, grid)),
            dma((planes, 2)),
            dma((planes, 2, grid)),
            dma((2, 2)),
            dma((2, 2)),
            dma((2,)),
        ],
        compiler_params=pltpu.CompilerParams(
            collective_id=0, has_side_effects=True, vmem_limit_bytes=56 * 1024 * 1024
        ),
        name="gather_attend",
    )(
        queries_narrow,
        keys_narrow,
        values_narrow,
        queries_wide,
        keys_wide,
        values_wide,
        lambda_narrow,
        lambda_wide,
        gain_narrow.reshape(1, -1),
        gain_wide.reshape(1, -1),
    )


def plane_greeting(planes, rows, columns, tp_count):
    per_plane = rows * columns
    sp = lax.axis_index("sp")
    tp = lax.axis_index("tp")
    plane = sp // per_plane
    cell = sp % per_plane
    barrier = pltpu.get_barrier_semaphore()
    for k in range(1, per_plane):
        pl.semaphore_signal(
            barrier,
            inc=1,
            device_id={"sp": plane * per_plane + (cell + k) % per_plane},
            device_id_type=MESH,
        )
    for k in range(1, planes):
        pl.semaphore_signal(
            barrier,
            inc=1,
            device_id={"sp": (plane + k) % planes * per_plane + cell},
            device_id_type=MESH,
        )
    for k in range(1, tp_count):
        pl.semaphore_signal(
            barrier, inc=1, device_id={"tp": (tp + k) % tp_count}, device_id_type=MESH
        )
    pl.semaphore_wait(barrier, per_plane - 1 + planes - 1 + tp_count - 1)
    return plane, cell, sp, tp


def silu(values):
    return values / (1.0 + jnp.exp(-values))


def expert_kernel(
    dims,
    group,
    chunks,
    normed_ref,
    slots_ref,
    gate_ref,
    up_ref,
    down_ref,
    shared_gate_ref,
    shared_up_ref,
    shared_down_ref,
    mixed_ref,
    gain_ref,
    layer_ref,
    marks,
    shared_out,
    summed,
    held,
    stage,
    inbox,
    result,
    theirs,
    back,
    leaving,
    landed,
    gate,
    up,
    down,
    shared_gate,
    shared_up,
    shared_down,
    load_sem,
    weight_sem,
    row_recv,
    mark_recv,
    row_send,
    mark_send,
    cell_recv,
    cell_send,
    pair_recv,
    pair_send,
    part_recv,
    part_send,
    back_recv,
    back_send,
    far_recv,
    far_send,
):
    planes, rows, columns, tp_count = dims
    per_plane = rows * columns
    mine = lax.axis_index("sp") // per_plane
    loads = [
        pltpu.make_async_copy(normed_ref, held.at[mine], load_sem.at[0]),
        pltpu.make_async_copy(slots_ref, marks.at[mine], load_sem.at[1]),
    ]
    weights = [
        pltpu.make_async_copy(source, target, weight_sem.at[index])
        for index, (source, target) in enumerate(
            (
                (shared_gate_ref, shared_gate),
                (shared_up_ref, shared_up),
                (shared_down_ref, shared_down),
                (gate_ref, gate),
                (up_ref, up),
                (down_ref, down),
            )
        )
    ]
    for copy in loads + weights:
        copy.start()
    plane, cell, sp, tp = plane_greeting(planes, rows, columns, tp_count)
    for copy in loads:
        copy.wait()
    padded = stage.shape[2]
    token_count = held.shape[1]
    width = held.shape[2]
    wide = width // chunks
    local_experts = gate.shape[0]
    capacity = group // local_experts

    def span(chunk):
        return pl.ds(chunk * wide, wide)

    def mark_hop(source, way, target):
        return pltpu.make_async_remote_copy(
            src_ref=marks.at[source],
            dst_ref=marks.at[source],
            send_sem=mark_send.at[source, way],
            recv_sem=mark_recv.at[source],
            device_id={"sp": target},
            device_id_type=MESH,
        )

    def row_hop(source, chunk, way, target):
        block = held.at[source, :, span(chunk)]
        return pltpu.make_async_remote_copy(
            src_ref=block,
            dst_ref=block,
            send_sem=row_send.at[source, chunk, way],
            recv_sem=row_recv.at[source, chunk],
            device_id={"sp": target},
            device_id_type=MESH,
        )

    def to_cell(source, chunk, k):
        other = (cell + k) % per_plane
        return pltpu.make_async_remote_copy(
            src_ref=stage.at[source, other, :, span(chunk)],
            dst_ref=inbox.at[source, tp, cell, :, span(chunk)],
            send_sem=cell_send.at[source, chunk, k],
            recv_sem=cell_recv.at[source, chunk, (per_plane - k) % per_plane],
            device_id={"sp": plane * per_plane + other},
            device_id_type=MESH,
        )

    def from_cell(source, chunk, k):
        return pltpu.make_async_remote_copy(
            src_ref=stage.at[source, cell, :, span(chunk)],
            dst_ref=inbox.at[source, tp, (cell + k) % per_plane, :, span(chunk)],
            send_sem=cell_send.at[source, chunk, k],
            recv_sem=cell_recv.at[source, chunk, k],
            device_id={"sp": sp},
            device_id_type=MESH,
        )

    def to_pair(source, chunk, k):
        block = inbox.at[source, tp, :, :, span(chunk)]
        return pltpu.make_async_remote_copy(
            src_ref=block,
            dst_ref=block,
            send_sem=pair_send.at[source, chunk, k - 1],
            recv_sem=pair_recv.at[source, chunk, k - 1],
            device_id={"tp": (tp + k) % tp_count},
            device_id_type=MESH,
        )

    def part_copy(source, chunk, k):
        other = (tp + k) % tp_count
        return pltpu.make_async_remote_copy(
            src_ref=result.at[source, other, :, :, span(chunk)],
            dst_ref=theirs.at[k - 1, source, :, :, span(chunk)],
            send_sem=part_send.at[source, chunk, k - 1],
            recv_sem=part_recv.at[source, chunk, k - 1],
            device_id={"tp": other},
            device_id_type=MESH,
        )

    def back_to(source, chunk, k):
        other = (cell + k) % per_plane
        return pltpu.make_async_remote_copy(
            src_ref=stage.at[source, other, :, span(chunk)],
            dst_ref=back.at[source, cell, :, span(chunk)],
            send_sem=back_send.at[source, chunk, k],
            recv_sem=back_recv.at[source, chunk, (per_plane - k) % per_plane],
            device_id={"sp": plane * per_plane + other},
            device_id_type=MESH,
        )

    def back_from(source, chunk, k):
        return pltpu.make_async_remote_copy(
            src_ref=stage.at[source, cell, :, span(chunk)],
            dst_ref=back.at[source, (cell + k) % per_plane, :, span(chunk)],
            send_sem=back_send.at[source, chunk, k],
            recv_sem=back_recv.at[source, chunk, k],
            device_id={"sp": sp},
            device_id_type=MESH,
        )

    def homeward(source, chunk, way, target):
        return pltpu.make_async_remote_copy(
            src_ref=leaving.at[source, :, span(chunk)],
            dst_ref=landed.at[way, source, :, span(chunk)],
            send_sem=far_send.at[source, chunk],
            recv_sem=far_recv.at[way, source, chunk],
            device_id={"sp": target},
            device_id_type=MESH,
        )

    def onward(source, act):
        @pl.when((source <= plane) & (plane < planes - 1))
        def _():
            act(0, sp + per_plane)

        @pl.when((source >= plane) & (plane > 0))
        def _():
            act(1, sp - per_plane)

    def forward(source, chunk):
        onward(source, lambda way, target: row_hop(source, chunk, way, target).start())

    def arrive(source):
        mark_hop(source, 0, sp).wait_recv()
        onward(source, lambda way, target: mark_hop(source, way, target).start())
        for chunk in range(chunks):
            row_hop(source, chunk, 0, sp).wait_recv()
            forward(source, chunk)

    def select(source):
        slots = marks[source]
        row = lax.broadcasted_iota(jnp.int32, (padded, token_count), 0)
        picks = []
        for k in list(range(1, per_plane)) + [0]:
            base = (plane * per_plane + (cell + k) % per_plane) * group
            wanted = jnp.where(row < group, row + base, -1).astype(jnp.float32)
            hit = slots[0:1, :] == wanted
            for choice in range(1, TOPK):
                hit = hit | (slots[choice : choice + 1, :] == wanted)
            picks.append((k, jnp.where(hit, 1.0, 0.0).astype(jnp.bfloat16)))
        for chunk in range(chunks):
            tokens = held[source, :, span(chunk)]
            for k, pick in picks:
                chosen = jnp.dot(pick, tokens, preferred_element_type=jnp.float32).astype(
                    jnp.bfloat16
                )
                if k == 0:
                    inbox[source, tp, cell, :, span(chunk)] = chosen
                else:
                    stage[source, (cell + k) % per_plane, :, span(chunk)] = chosen
                    to_cell(source, chunk, k).start()

    def finish(source):
        for chunk in range(chunks):
            for k in range(1, per_plane):
                from_cell(source, chunk, k).wait_recv()
            for k in range(1, tp_count):
                to_pair(source, chunk, k).start()

    def experts(source):
        for chunk in range(chunks):
            for k in range(1, tp_count):
                to_pair(source, chunk, k).wait_recv()
        done = 0
        for index in range(local_experts):
            begin = index * capacity // 16 * 16
            end = -(-((index + 1) * capacity) // 16) * 16
            block = (tp_count, per_plane, end - begin, width)
            tokens = inbox[source, :, :, begin:end, :].reshape(-1, width)
            gated = jnp.dot(tokens, gate[index], preferred_element_type=jnp.float32)
            hidden = silu(gated) * jnp.dot(
                tokens, up[index], preferred_element_type=jnp.float32
            )
            out = (
                jnp.dot(
                    hidden.astype(jnp.bfloat16), down[index], preferred_element_type=jnp.float32
                )
                .astype(jnp.bfloat16)
                .reshape(block)
            )
            both = max(0, done - begin)
            if both > 0:
                shape = (tp_count, per_plane, both, width)
                row = lax.broadcasted_iota(jnp.int32, shape, 2) + begin
                result[source, :, :, begin:done, :] = jnp.where(
                    row < index * capacity, result[source, :, :, begin:done, :], out[:, :, :both]
                )
            if end > begin + both:
                result[source, :, :, begin + both : end, :] = out[:, :, both:]
            done = max(done, end)
        for chunk in range(chunks):
            for k in range(1, tp_count):
                part_copy(source, chunk, k).start()

    def hand_back(source):
        for chunk in range(chunks):
            for k in range(1, per_plane):
                to_cell(source, chunk, k).wait_send()
            for k in range(1, tp_count):
                part_copy(source, chunk, k).wait_recv()
            for k in list(range(1, per_plane)) + [0]:
                other = (cell + k) % per_plane
                total = result[source, tp, other, :, span(chunk)].astype(jnp.float32)
                for i in range(tp_count - 1):
                    total += theirs[i, source, other, :, span(chunk)].astype(jnp.float32)
                if k == 0:
                    back[source, cell, :, span(chunk)] = total.astype(jnp.bfloat16)
                else:
                    stage[source, other, :, span(chunk)] = total.astype(jnp.bfloat16)
                    back_to(source, chunk, k).start()

    def gather_up(source, last):
        slots = marks[source]
        row = lax.broadcasted_iota(jnp.int32, (per_plane * padded, token_count), 0)
        block = lax.div(row, padded)
        inner = row - block * padded
        wanted = jnp.where(
            inner < group, inner + (plane * per_plane + block) * group, -1
        ).astype(jnp.float32)
        share = jnp.zeros(wanted.shape, jnp.float32)
        for choice in range(TOPK):
            share += jnp.where(
                slots[choice : choice + 1, :] == wanted,
                slots[TOPK + choice : TOPK + choice + 1, :],
                0.0,
            )
        coarse = share.astype(jnp.bfloat16)
        fine = (share - coarse.astype(jnp.float32)).astype(jnp.bfloat16)
        both = jnp.concatenate([coarse, fine], axis=1)
        if last:
            comes = [(0, plane > 0), (1, plane < planes - 1)]
        else:
            ahead = source > plane
            behind = source < plane
            comes = [(0, ahead & (plane > 0)), (1, behind & (plane < planes - 1))]
        for chunk in range(chunks):
            for k in range(1, per_plane):
                back_from(source, chunk, k).wait_recv()
            begin = chunk * wide
            for at in range(begin, begin + wide, 512):
                values = back[source, :, :, at : at + 512].reshape(per_plane * padded, 512)
                pieces = lax.dot_general(
                    both, values, (((0,), (0,)), ((), ())), preferred_element_type=jnp.float32
                )
                summed[:, at : at + 512] = pieces[:token_count] + pieces[token_count:]
            for way, exists in comes:

                @pl.when(exists)
                def _(way=way, chunk=chunk):
                    homeward(source, chunk, way, sp).wait_recv()
                    summed[:, span(chunk)] += landed[way, source, :, span(chunk)].astype(
                        jnp.float32
                    )

            if not last:
                leaving[source, :, span(chunk)] = summed[:, span(chunk)].astype(jnp.bfloat16)

                @pl.when(ahead)
                def _(chunk=chunk):
                    homeward(source, chunk, 0, sp + per_plane).start()

                @pl.when(behind)
                def _(chunk=chunk):
                    homeward(source, chunk, 1, sp - per_plane).start()

    onward(plane, lambda way, target: mark_hop(plane, way, target).start())
    for chunk in range(chunks):
        forward(plane, chunk)
    select(plane)
    for copy in weights[:3]:
        copy.wait()
    normed = held[plane]
    shared_hidden = silu(
        jnp.dot(normed, shared_gate[...], preferred_element_type=jnp.float32)
    ) * jnp.dot(normed, shared_up[...], preferred_element_type=jnp.float32)
    shared_out[...] = jnp.dot(
        shared_hidden.astype(jnp.bfloat16), shared_down[...], preferred_element_type=jnp.float32
    )
    for copy in weights[3:]:
        copy.wait()

    at_edge = (plane == 0) | (plane == planes - 1)
    first_out = jnp.where(plane == 0, 1, planes - 2)

    if planes == 1:
        finish(plane)
        experts(plane)

    def process(source):
        finish(source)
        experts(source)
        hand_back(source)

    def each(distance, act):
        def one(side, carry):
            source = plane + (2 * side - 1) * distance

            @pl.when((source >= 0) & (source < planes))
            def _():
                act(source)

            return carry

        lax.fori_loop(0, 2, one, 0)

    def step(distance, carry):
        each(distance, arrive)
        each(distance, select)

        @pl.when(at_edge & (planes > 2) & (distance == planes - 1))
        def _():
            gather_up(first_out, False)

        @pl.when(distance == 1)
        def _():
            finish(plane)
            experts(plane)

        @pl.when(distance > 1)
        def _():
            each(distance - 1, process)

        return carry

    lax.fori_loop(1, planes, step, 0)

    each(planes - 1, process)
    hand_back(plane)

    def chain(index, carry):
        low, high = carry
        use_high = (low < 0) | (
            (high < planes)
            & (2 * high + plane <= 2 * (planes - 1 - low) + (planes - 1 - plane))
        )
        source = jnp.where(use_high, high, low)

        @pl.when(jnp.logical_not(at_edge & (index == 0) & (planes > 2)))
        def _():
            gather_up(source, False)

        return jnp.where(use_high, low, low - 1), jnp.where(use_high, high + 1, high)

    lax.fori_loop(0, planes - 1, chain, (plane - 1, plane + 1))
    gather_up(plane, True)
    layer_ref[...] = (
        mixed_ref[...].astype(jnp.float32)
        + rms_scale(shared_out[...] + summed[...], gain_ref[...])
    ).astype(jnp.bfloat16)

    def drain(source, carry):
        onward(source, lambda way, target: mark_hop(source, way, target).wait_send())
        for chunk in range(chunks):
            onward(
                source, lambda way, target: row_hop(source, chunk, way, target).wait_send()
            )
            for k in range(1, per_plane):
                back_to(source, chunk, k).wait_send()
            for k in range(1, tp_count):
                to_pair(source, chunk, k).wait_send()
                part_copy(source, chunk, k).wait_send()

            @pl.when(source != plane)
            def _():
                homeward(source, chunk, 0, sp).wait_send()

        return carry

    lax.fori_loop(0, planes, drain, 0)


def expert_rows(
    dims,
    group,
    normed,
    slot_index,
    route_weights,
    routed_weights,
    shared_weights,
    mixed,
    gain,
):
    planes, rows, columns, tp_count = dims
    per_plane = rows * columns
    token_count, width = normed.shape
    padded = -(-group // 16) * 16
    slots = slot_index.reshape(token_count, TOPK).astype(jnp.float32)
    slots = jnp.concatenate([slots, route_weights], axis=1).T
    hbm = pl.BlockSpec(memory_space=pl.ANY)
    vmem = pl.BlockSpec(memory_space=pltpu.VMEM)
    dma = pltpu.SemaphoreType.DMA
    chunks = math.gcd(width // 512, 4)
    pairs = max(1, tp_count - 1)
    weights = list(routed_weights) + list(shared_weights)
    block = (planes, per_plane, padded, width)
    inbox = (planes, tp_count, per_plane, padded, width)
    return pl.pallas_call(
        functools.partial(expert_kernel, dims, group, chunks),
        out_shape=jax.ShapeDtypeStruct((token_count, width), jnp.bfloat16),
        in_specs=[hbm] * (2 + len(weights)) + [vmem, vmem],
        out_specs=vmem,
        scratch_shapes=[
            pltpu.VMEM((planes, 2 * TOPK, token_count), jnp.float32),
            pltpu.VMEM((token_count, width), jnp.float32),
            pltpu.VMEM((token_count, width), jnp.float32),
            pltpu.VMEM((planes, token_count, width), jnp.bfloat16),
            pltpu.VMEM(block, jnp.bfloat16),
            pltpu.VMEM(inbox, jnp.bfloat16),
            pltpu.VMEM(inbox, jnp.bfloat16),
            pltpu.VMEM((pairs,) + block, jnp.bfloat16),
            pltpu.VMEM(block, jnp.bfloat16),
            pltpu.VMEM((planes, token_count, width), jnp.bfloat16),
            pltpu.VMEM((2, planes, token_count, width), jnp.bfloat16),
        ]
        + [pltpu.VMEM(weight.shape, jnp.bfloat16) for weight in weights]
        + [
            dma((2,)),
            dma((len(weights),)),
            dma((planes, chunks)),
            dma((planes,)),
            dma((planes, chunks, 2)),
            dma((planes, 2)),
            dma((planes, chunks, per_plane)),
            dma((planes, chunks, per_plane)),
            dma((planes, chunks, pairs)),
            dma((planes, chunks, pairs)),
            dma((planes, chunks, pairs)),
            dma((planes, chunks, pairs)),
            dma((planes, chunks, per_plane)),
            dma((planes, chunks, per_plane)),
            dma((2, planes, chunks)),
            dma((planes, chunks)),
        ],
        compiler_params=pltpu.CompilerParams(
            collective_id=1, has_side_effects=True, vmem_limit_bytes=60 * 1024 * 1024
        ),
        name="expert_layer",
    )(normed, slots, *weights, mixed, gain.reshape(1, -1))


def shards(
    queries_narrow,
    keys_narrow,
    values_narrow,
    queries_wide,
    keys_wide,
    values_wide,
    lambda_narrow,
    lambda_wide,
    gain_narrow,
    gain_wide,
    out_narrow,
    out_wide,
    stream,
    gain_mix,
    gain_ffn,
    gain_post,
    shared_gate,
    shared_up,
    shared_down,
    expert_gate,
    expert_up,
    expert_down,
    expert_ids,
    route_weights,
):
    sp_count = lax.axis_size("sp")
    narrow_rows, wide_rows = attended_rows(
        sp_count,
        lax.axis_size("tp"),
        queries_narrow,
        keys_narrow,
        values_narrow,
        queries_wide,
        keys_wide,
        values_wide,
        lambda_narrow,
        lambda_wide,
        gain_narrow,
        gain_wide,
    )
    projected = jnp.dot(narrow_rows, out_narrow, preferred_element_type=jnp.float32) + jnp.dot(
        wide_rows, out_wide, preferred_element_type=jnp.float32
    )
    mixed_rows = (stream.astype(jnp.float32) + rms_scale(projected, gain_mix)).astype(jnp.bfloat16)
    normed = rms_scale(mixed_rows.astype(jnp.float32), gain_ffn).astype(jnp.bfloat16)
    row_count = normed.shape[0]
    tp_count = lax.axis_size("tp")
    local_experts = expert_gate.shape[0]
    experts_all = local_experts * sp_count
    capacity = max(2, 3 * row_count * TOPK // (2 * experts_all))
    chosen = (
        expert_ids[:, :, None] == jnp.arange(experts_all, dtype=jnp.int32)[None, None, :]
    ).astype(jnp.float32)
    named = jnp.sum(chosen, axis=1)
    order = jnp.arange(row_count, dtype=jnp.int32)
    earlier = jnp.dot(
        (order[None, :] < order[:, None]).astype(jnp.bfloat16),
        named.astype(jnp.bfloat16),
        preferred_element_type=jnp.float32,
    )
    slot_rank = jnp.sum(chosen * earlier[:, None, :], axis=2).astype(jnp.int32)
    slot_index = expert_ids * capacity + slot_rank
    group = local_experts * capacity
    dims = plane_shape(sp_count) + (tp_count,)
    return expert_rows(
        dims,
        group,
        normed,
        slot_index,
        route_weights,
        (expert_gate, expert_up, expert_down),
        (shared_gate, shared_up, shared_down),
        mixed_rows,
        gain_post,
    )


def solution(mesh):
    return jax.shard_map(
        shards,
        mesh=mesh,
        in_specs=(
            P("sp", "tp"),
            P("sp", "tp"),
            P("sp", "tp"),
            P("sp", "tp"),
            P("sp", "tp"),
            P("sp", "tp"),
            P("tp"),
            P("tp"),
            P(),
            P(),
            P(),
            P(),
            P(("sp", "tp"), None),
            P(),
            P(),
            P(),
            P(),
            P(),
            P(),
            P("sp", None, "tp"),
            P("sp", None, "tp"),
            P("sp", "tp", None),
            P(("sp", "tp"), None),
            P(("sp", "tp"), None),
        ),
        out_specs=P(("sp", "tp"), None),
        check_vma=False,
    )
```
